512 devices in a mesh: grp: 2 (over y), sp: 16 (over z), tp: 16 (over x, core).
Axes of the slice: x: 8, y: 2, z: 16, core: 2. Of those that a mesh axis runs over, the one named last changes fastest.
The devices are a block of a 8x8x16 slice.
Arguments:
- hidden_items: bfloat16 [4096, 4096], P(('grp', 'sp', 'tp')), parts along dimension 0, may hold values from -6 to 6
- sample_cond: bfloat16 [8192], P('grp'), parts along dimension 0, may hold values from -6 to 6
- prompt_items: bfloat16 [256, 4096], P(('grp', 'sp')), parts along dimension 0, may hold values from -6 to 6
- prompt_cond: bfloat16 [4096], replicated, may hold values from -6 to 6
- adjust_shifting: bfloat16 [4096, 4096], P('sp', 'tp'), may hold values from -0.125 to 0.125
- adjust_stretch: bfloat16 [4096, 4096], P('sp', 'tp'), may hold values from -0.125 to 0.125
- skip_valve: bfloat16 [4096, 4096], P('sp', 'tp'), may hold values from -0.125 to 0.125
- receiver_matrix: bfloat16 [4096, 2048], P(None, 'tp'), may hold values from -0.09375 to 0.09375
- address_matrix: bfloat16 [4096, 2048], P(None, 'tp'), may hold values from -0.09375 to 0.09375
- payload_matrix: bfloat16 [4096, 2048], P(None, 'tp'), may hold values from -0.09375 to 0.09375
- joint_lower_projector: bfloat16 [4096, 64], P('sp'), may hold values from -0.09375 to 0.09375
- fading_raise_matrix: bfloat16 [64, 2048], P(None, 'tp'), may hold values from -1.5 to 1.5
- step_raise_matrix: bfloat16 [64, 2048], P(None, 'tp'), may hold values from -1.5 to 1.5
- feature_fading: float32 [2048], P('tp'), may hold values from 0 to 0.1, as said below
- spike_logfade: float32 [4096, 32], P(('grp', 'sp'), 'tp'), parts along dimension 0, may hold values from 0 to 2
- group_standard_factor: float32 [2048], P('tp'), may hold values from 0.1 to 1.9
- emit_matrix: bfloat16 [2048, 4096], P('tp', 'sp'), may hold values from -0.125 to 0.125
Outputs:
- latent_out: bfloat16 [4096, 4096], P(('grp', 'sp', 'tp')), parts along dimension 0
The draws below stay inside these ranges and needn't reach their ends.
There are 2 independent parts, one for each index of `grp`. The reference program is written for one: setup_inputs(seed, part) draws one part's arguments, and reference() takes and returns one part's arrays. A program takes and returns all parts, laid end to end along the dimension named above; an argument that names none is the same for every part. Nothing has to cross between parts.
Inputs may be any that keep to these rules, and one draw needn't show every extreme that they name: `feature_fading`: per-token decay rate of each channel.
All inputs are finite; a program needn't handle non-finite values.
Results may differ from the reference program's by a relative error of at most 0.015.
Values may be sent and summed in bfloat16 or wider, within the bound.
No kernel may reach another device: no remote copies, remote signals or barrier semaphores. Data moves between devices by JAX's collectives and lax.ppermute only.
A program may use at most 64 MiB of HBM per device.

```python
import math
import jax
import jax.numpy as jnp
from jax import lax

D = 4096
ATTEND_GROUPS = 32
ATTEND_WIDTH = 64
RANK = 64
TOK_SP = 128
CTX = 128
HIDDEN_COUNT = 2048
A_WIDTH = 2048
N_TP = 16


def draw_feature_fading(key, part):
    key_one, another_address, further_address = jax.random.split(jax.random.fold_in(key, 11), 3)
    chain_len = HIDDEN_COUNT + CTX
    quick_heads = jax.random.randint(key_one, (ATTEND_GROUPS,), 0, 2) == 0
    fast_rate = jnp.exp(jax.random.uniform(another_address, (ATTEND_GROUPS, ATTEND_WIDTH), jnp.float32, math.log(0.035), math.log(0.09)))
    slow_rate = jnp.exp(jax.random.uniform(further_address, (ATTEND_GROUPS, ATTEND_WIDTH), jnp.float32, math.log(0.2), math.log(1.0))) / chain_len
    return jnp.where(quick_heads[:, None], fast_rate, slow_rate).reshape(ATTEND_GROUPS * ATTEND_WIDTH).astype(jnp.float32)


def draw_spike_logfade(key, part):
    key_one, another_address, further_address = jax.random.split(jax.random.fold_in(key, 23), 3)
    chain_len = HIDDEN_COUNT + CTX
    block_count = HIDDEN_COUNT // TOK_SP
    levels = jnp.exp(jax.random.uniform(key_one, (block_count, 1, ATTEND_GROUPS), jnp.float32, math.log(0.1), math.log(1.0))) / chain_len
    drawn_answer = jnp.broadcast_to(levels, (block_count, TOK_SP, ATTEND_GROUPS)).reshape(HIDDEN_COUNT, ATTEND_GROUPS)
    spike_places = jax.random.randint(another_address, (2, ATTEND_GROUPS), 0, HIDDEN_COUNT)
    spike_span = -jnp.log(jax.random.uniform(further_address, (2, ATTEND_GROUPS), jnp.float32, 0.5, 0.8))
    agreement_marks = jnp.arange(HIDDEN_COUNT)[:, None, None] == spike_places[None]
    spike_present = jnp.sum(jnp.where(agreement_marks, spike_span[None], 0.0), axis=1)
    return (drawn_answer + spike_present).astype(jnp.float32)


def block_levels(stream_key, dims, cuts, least, high):
    def one(dim, shards_of):
        steps = jax.random.uniform(jax.random.fold_in(jax.random.fold_in(stream_key, 6), dim), (shards_of,), jnp.float32, least / len(cuts), high / len(cuts))
        return jnp.repeat(jnp.exp(steps), dims[dim] // shards_of).reshape((-1,) + (1,) * (len(dims) - dim - 1))

    level = one(*cuts[0])
    for cut in cuts[1:]:
        level = level * one(*cut)
    return level


def bell_draw(key, dims, deviation, bound, cuts=(), kind=jnp.bfloat16):
    array = jax.random.normal(key, dims, jnp.float32) * deviation
    if len(cuts) > 0:
        array = block_levels(key, dims, cuts, -0.22, 0.18) * array
    return jnp.clip(array, min=-bound, max=bound).astype(kind)


def setup_inputs(seed: int = 0, part: int = 0) -> dict:
    keys = jax.random.split(jax.random.key(seed), 18)
    part_splits = jax.random.split(jax.random.fold_in(keys[17], part), 18)
    return {
        "hidden_items": bell_draw(part_splits[0], (HIDDEN_COUNT, D), 1.0, 6.0, ((0, 256),)),
        "sample_cond": bell_draw(part_splits[1], (D,), 1.0, 6.0),
        "prompt_items": bell_draw(part_splits[2], (CTX, D), 1.0, 6.0, ((0, 16),)),
        "prompt_cond": bell_draw(keys[3], (D,), 1.0, 6.0),
        "adjust_shifting": bell_draw(keys[4], (D, D), (D // 2) ** -0.5, 0.125, ((0, 16), (1, 16))),
        "adjust_stretch": bell_draw(keys[5], (D, D), (D // 2) ** -0.5, 0.125, ((0, 16), (1, 16))),
        "skip_valve": bell_draw(keys[6], (D, D), (D // 2) ** -0.5, 0.125, ((0, 16), (1, 16))),
        "receiver_matrix": bell_draw(keys[7], (D, A_WIDTH), D ** -0.5, 0.09375, ((1, 16),)),
        "address_matrix": bell_draw(keys[8], (D, A_WIDTH), D ** -0.5, 0.09375, ((1, 16),)),
        "payload_matrix": bell_draw(keys[9], (D, A_WIDTH), D ** -0.5, 0.09375, ((1, 16),)),
        "joint_lower_projector": bell_draw(keys[10], (D, RANK), D ** -0.5, 0.09375, ((0, 16),)),
        "fading_raise_matrix": bell_draw(keys[11], (RANK, A_WIDTH), 0.25, 1.5, ((1, 16),)),
        "step_raise_matrix": bell_draw(keys[12], (RANK, A_WIDTH), (RANK // 4) ** -0.5, 1.5, ((1, 16),)),
        "feature_fading": draw_feature_fading(jax.random.fold_in(keys[17], 71), part),
        "spike_logfade": draw_spike_logfade(jax.random.fold_in(jax.random.fold_in(keys[17], part), 71), part),
        "group_standard_factor": jnp.clip(1.0 + 0.18 * jax.random.normal(keys[15], (A_WIDTH,), jnp.float32), 0.1, 1.9),
        "emit_matrix": bell_draw(keys[16], (A_WIDTH, D), A_WIDTH ** -0.5, 0.125, ((0, 16), (1, 16))),
    }


EXACT_MODE = lax.Precision.HIGHEST
rate_shift = 5.0

def stored(value):
    return lax.optimization_barrier(value.astype(jnp.bfloat16))

def product(left, right):
    return jnp.dot(left, right, preferred_element_type=jnp.float32)

def modulate(rows, shifts, scales):
    values = rows.astype(jnp.float32)
    centre = lax.optimization_barrier(jnp.mean(values, -1, keepdims=True))
    spread = lax.optimization_barrier(jnp.mean(jnp.square(values - centre), -1, keepdims=True))
    normed = (values - centre) * lax.rsqrt(spread + 1e-05)
    return (normed * (1.0 + scales) + shifts).astype(jnp.bfloat16)

def head_inputs(u_rows, address_matrix, payload_matrix, joint_lower_projector, fading_raise_matrix, step_raise_matrix, feature_fading, surplus_entries):
    row_count = u_rows.shape[0]
    key_rows = stored(product(u_rows, address_matrix))
    value_rows = stored(product(u_rows, payload_matrix))
    low_rows = stored(product(u_rows, joint_lower_projector))
    squashed = jnp.tanh(low_rows.astype(jnp.float32)).astype(jnp.bfloat16)
    logdecay = -feature_fading * jax.nn.sigmoid(product(squashed, fading_raise_matrix)) - surplus_entries
    learned = jax.nn.sigmoid(product(squashed, step_raise_matrix) - rate_shift)
    key_heads = key_rows.astype(jnp.float32).reshape(row_count, ATTEND_GROUPS, ATTEND_WIDTH)
    unit_keys = key_heads * lax.rsqrt(lax.optimization_barrier(jnp.sum(key_heads * key_heads, -1, keepdims=True)) + 1e-06)
    removal = unit_keys * learned.reshape(row_count, ATTEND_GROUPS, ATTEND_WIDTH)
    retain = jnp.exp(logdecay).reshape(row_count, ATTEND_GROUPS, ATTEND_WIDTH)
    value_heads = value_rows.astype(jnp.float32).reshape(row_count, ATTEND_GROUPS, ATTEND_WIDTH)
    return (retain, key_heads, value_heads, unit_keys, removal)

def advance(carried, inputs):
    retain, key_heads, value_heads, unit_keys, removal = inputs
    probed = jnp.einsum('hvk,hk->hv', carried, unit_keys, precision=EXACT_MODE)
    return carried * retain[:, None, :] - probed[:, :, None] * removal[:, None, :] + value_heads[:, :, None] * key_heads[:, None, :]

def step_plain(carried, inputs):
    return (advance(carried, inputs), jnp.zeros((), jnp.float32))

def step_read(carried, inputs):
    carried = advance(carried, inputs[:5])
    return (carried, jnp.einsum('hvk,hk->hv', carried, inputs[5], precision=EXACT_MODE))

def reference(hidden_items, sample_cond, prompt_items, prompt_cond, adjust_shifting, adjust_stretch, skip_valve, receiver_matrix, address_matrix, payload_matrix, joint_lower_projector, fading_raise_matrix, step_raise_matrix, feature_fading, spike_logfade, group_standard_factor, emit_matrix):
    activated = jax.nn.silu(jnp.stack([sample_cond, prompt_cond]).astype(jnp.float32)).astype(jnp.bfloat16)
    shifts = product(activated, adjust_shifting)
    scales = product(activated, adjust_stretch)
    gates = product(activated[:1], skip_valve)[0]
    u_latent = modulate(hidden_items, shifts[0], scales[0])
    u_context = modulate(prompt_items, shifts[1], scales[1])
    query_heads = stored(product(u_latent, receiver_matrix)).astype(jnp.float32).reshape(HIDDEN_COUNT, ATTEND_GROUPS, ATTEND_WIDTH)
    surplus_entries = jnp.repeat(spike_logfade, ATTEND_WIDTH, axis=1)
    latent_parts = head_inputs(u_latent, address_matrix, payload_matrix, joint_lower_projector, fading_raise_matrix, step_raise_matrix, feature_fading, surplus_entries)
    context_parts = head_inputs(u_context, address_matrix, payload_matrix, joint_lower_projector, fading_raise_matrix, step_raise_matrix, feature_fading, 0.0)
    zeroed = jnp.zeros((ATTEND_GROUPS, ATTEND_WIDTH, ATTEND_WIDTH), jnp.float32)
    ctx_forward, _ = lax.scan(step_plain, zeroed, context_parts)
    ctx_backward, _ = lax.scan(step_plain, zeroed, context_parts, reverse=True)
    _, forward = lax.scan(step_read, ctx_forward, latent_parts + (query_heads,))
    _, backward = lax.scan(step_read, ctx_backward, latent_parts + (query_heads,), reverse=True)
    combined = forward + backward
    centre = lax.optimization_barrier(jnp.mean(combined, -1, keepdims=True))
    spread = lax.optimization_barrier(jnp.mean(jnp.square(combined - centre), -1, keepdims=True))
    normed = (combined - centre) * lax.rsqrt(spread + 0.00064) * group_standard_factor.reshape(ATTEND_GROUPS, ATTEND_WIDTH)
    normed = normed.reshape(HIDDEN_COUNT, ATTEND_GROUPS * ATTEND_WIDTH).astype(jnp.bfloat16)
    stride = ATTEND_GROUPS * ATTEND_WIDTH // N_TP
    mixed_sum = jnp.zeros((HIDDEN_COUNT, D), jnp.float32)
    for number in range(N_TP):
        portion = product(normed[:, number * stride:(number + 1) * stride], emit_matrix[number * stride:(number + 1) * stride])
        mixed_sum = mixed_sum + lax.optimization_barrier(portion.astype(jnp.bfloat16)).astype(jnp.float32)
    return (hidden_items.astype(jnp.float32) + gates * mixed_sum).astype(jnp.bfloat16)
```

```python
import jax
import jax.numpy as jnp
from jax import lax
from jax.experimental import pallas as pl
from jax.experimental.pallas import tpu as pltpu
from jax.sharding import PartitionSpec as P

HEAD = 64
EPS_ROW = 1e-05
EPS_HEAD = 0.00064
EPS_KEY = 1e-06
RATE_SHIFT = 5.0
NEVER = -1e30
BF16, F32 = jnp.bfloat16, jnp.float32

VMEM = pl.BlockSpec(memory_space=pltpu.VMEM)
SMEM = pl.BlockSpec(memory_space=pltpu.SMEM)


def call(body, outs, *args, flops=0, scalars=0, scratch=()):
    many = isinstance(outs, list)
    shapes = [jax.ShapeDtypeStruct(s, d) for s, d in (outs if many else [outs])]
    got = pl.pallas_call(
        body,
        out_shape=shapes,
        in_specs=[SMEM] * scalars + [VMEM] * (len(args) - scalars),
        out_specs=[VMEM] * len(shapes),
        scratch_shapes=list(scratch),
        compiler_params=pltpu.CompilerParams(vmem_limit_bytes=48 * 1024 * 1024),
        cost_estimate=pl.CostEstimate(
            flops=flops, transcendentals=0, bytes_accessed=sum(a.size * a.dtype.itemsize for a in args)
        ),
    )(*args)
    return got if many else got[0]


def dot(left, right, dims=((1,), (0,))):
    return lax.dot_general(
        left.astype(BF16), right.astype(BF16), (dims, ((), ())), preferred_element_type=F32
    )


def iota(shape, dim):
    return lax.broadcasted_iota(jnp.int32, shape, dim)


def partials_kernel(place, sample, prompt, shifting, stretch, valve, out):
    peers, rows, _ = out.shape
    mine = iota(sample.shape, 0) == place[0]

    def own(cond):
        return jnp.sum(jnp.where(mine, cond[...].astype(F32), 0.0), axis=0, keepdims=True)

    row = iota((rows, sample.shape[1]), 0)
    first, second = jax.nn.silu(own(sample)), jax.nn.silu(own(prompt))

    def at(k, both):
        left = jnp.where(row == k, first, 0.0)
        return jnp.where(row == k + 1, second, left) if both else left

    total = dot(at(0, True), shifting[...]) + dot(at(2, True), stretch[...])
    total = total + dot(at(4, False), valve[...])
    out[...] = jnp.broadcast_to(total[None], out.shape)


def sum_kernel(parts, out):
    total = parts[0]
    for k in range(1, parts.shape[0]):
        total = total + parts[k]
    out[...] = jnp.broadcast_to(total[None], out.shape)


def rows_kernel(latent, context, vectors, wq, wk, wv, u, q, k, v):
    count, width = latent.shape
    extra = context.shape[0]
    lane = vectors.shape[2]

    def moments(ref):
        total = jnp.zeros((ref.shape[0], lane), F32)
        for c in range(0, width, lane):
            total = total + ref[:, c : c + lane].astype(F32)
        centre = jnp.sum(total, -1, keepdims=True) * (1.0 / width)
        total = jnp.zeros((ref.shape[0], lane), F32)
        for c in range(0, width, lane):
            off = ref[:, c : c + lane].astype(F32) - centre
            total = total + off * off
        spread = jnp.sum(total, -1, keepdims=True) * (1.0 / width)
        return centre, lax.rsqrt(spread + EPS_ROW)

    lat, ctx = moments(latent), moments(context)
    pad = jnp.zeros((u.shape[0] - count - extra, lane), F32)
    for t in range(width // lane):
        cols = slice(t * lane, (t + 1) * lane)

        def one(ref, stats, i):
            normed = (ref[:, cols].astype(F32) - stats[0]) * stats[1]
            return normed * (1.0 + vectors[t, 2 + i : 3 + i, :]) + vectors[t, i : i + 1, :]

        u[:count, cols] = one(latent, lat, 0).astype(BF16)
        u[count:, cols] = jnp.concatenate([one(context, ctx, 1), pad], axis=0).astype(BF16)
    q[...] = dot(u[:count], wq[...]).astype(BF16)
    k[...] = dot(u[...], wk[...]).astype(BF16)
    v[...] = dot(u[...], wv[...]).astype(BF16)


def low_kernel(u, pieces, k, v, low, payload, down):
    _, blocks, rows, lane = pieces.shape
    span = pieces.shape[0] * rows
    for s in range(blocks):
        piece = pieces[:, s].astype(F32).reshape(span, lane)
        down[2 * s * span : (2 * s + 1) * span] = piece.astype(BF16)
        down[(2 * s + 1) * span : (2 * s + 2) * span] = pltpu.roll(piece, HEAD, 1).astype(BF16)
    result = dot(u[...], down[...])
    result = jnp.where(iota(result.shape, 1) < HEAD, result, 0.0)
    count = low.shape[0]
    low[...] = result[:count].astype(BF16)
    extra = payload.shape[1]
    for at, part in enumerate((k[count:].astype(F32), v[count:].astype(F32), result[count:])):
        part = part[:extra].astype(BF16)
        payload[:, :, at * lane : (at + 1) * lane] = jnp.broadcast_to(part[None], (payload.shape[0], extra, lane))


def inverse(mixing, row, col, upper):
    size = mixing[0].shape[0]
    eye = (row == col).astype(F32)
    width = 1
    found = None
    while width < size:
        here, there = (col, row) if upper else (row, col)
        shared = (row // (2 * width)) == (col // (2 * width))
        corner = shared & ((here // width) % 2 == 1) & ((there // width) % 2 == 0)
        parts = [jnp.where(corner, m, 0.0) for m in mixing]
        if found is None:
            found = [eye - p for p in parts]
        else:
            lefts = [dot(p, f) for p, f in zip(parts, found)]
            found = [f - dot(f, g) for f, g in zip(found, lefts)]
        width *= 2
    return found


def block_terms(k, v, low, fading, step, rates, spikes=None, q=None):
    count, lanes = k.shape
    row, col = iota((count, lanes), 0), iota((count, lanes), 1)
    heads = lanes // HEAD
    owns = [(col // HEAD) == h for h in range(heads)]

    squashed = jnp.tanh(low.astype(F32)).astype(BF16)
    feature = -rates * jax.nn.sigmoid(dot(squashed, fading))
    learned = jax.nn.sigmoid(dot(squashed, step) - RATE_SHIFT)
    key = k.astype(F32)
    norms = jnp.zeros_like(key)
    for own in owns:
        total = jnp.sum(jnp.where(own, key * key, 0.0), -1, keepdims=True)
        norms = jnp.where(own, lax.rsqrt(total + EPS_KEY), norms)
    unit = key * norms
    removal = unit * learned

    upto = (row >= col).astype(F32)

    def running(part):
        return lax.dot_general(
            upto, part, (((1,), (0,)), ((), ())), preferred_element_type=F32, precision=lax.Precision.HIGHEST
        )

    after = running(feature)
    before = after - feature
    grow, shrink = jnp.exp(after), jnp.exp(-after)
    grow_x, shrink_x = jnp.exp(before), jnp.exp(-before)
    end = after[count - 1 : count]
    if spikes is None:
        b_end = b_after = b_before = None
    else:
        jump = jnp.zeros_like(key)
        for h, own in enumerate(owns):
            jump = jnp.where(own, -spikes[:, h : h + 1], jump)
        b_after = running(jump)
        b_before = b_after - jump
        b_end = b_after[count - 1 : count]
        across_after, across_before = b_after.T, b_before.T

    def pair(h, upper, strict):
        inside = ((col > row) if strict else (col >= row)) if upper else ((col < row) if strict else (col <= row))
        if spikes is None:
            return inside.astype(F32)
        at = h * HEAD
        down_after, down_before = b_after[:, at : at + 1], b_before[:, at : at + 1]
        side_after, side_before = across_after[at : at + 1], across_before[at : at + 1]
        if upper:
            power = side_before - (down_after if strict else down_before)
        else:
            power = (down_before if strict else down_after) - side_after
        return jnp.where(inside, jnp.exp(jnp.where(inside, power, NEVER)), 0.0)

    def scaled(tensor, power):
        return tensor if spikes is None else tensor * jnp.exp(power)

    probes = (unit * grow_x, unit * shrink)
    removals = (removal * shrink, removal * grow_x)
    keys = (key * shrink, key * grow_x)
    asks = None if q is None else (q.astype(F32) * grow, q.astype(F32) * shrink_x)

    scores = []
    for d in range(2):
        right = jnp.concatenate([removals[d], keys[d]], axis=0)
        for own in owns:
            left = jnp.where(own, probes[d], 0.0)
            if q is not None:
                left = jnp.concatenate([left, jnp.where(own, asks[d], 0.0)], axis=0)
            scores.append(dot(left, right, ((1,), (1,))))
    chains = [(d, h) for d in range(2) for h in range(heads)]
    masks = {(d, h): pair(h, d == 1, True) for d, h in chains}
    mixing = {c: scores[n][:count, :count] * masks[c] for n, c in enumerate(chains)}
    seen = {c: dot(scores[n][:count, count:] * masks[c], v) for n, c in enumerate(chains)}
    solved = {}
    for d in range(2):
        found = inverse([mixing[d, h] for h in range(heads)], row, col, d == 1)
        for h in range(heads):
            solved[d, h] = found[h]

    whole = jnp.exp(end)
    starts = (
        scaled(probes[0], b_before),
        scaled(probes[1] * whole, None if spikes is None else b_end - b_after),
    )

    def gathered(parts):
        total = parts[0]
        for own, part in zip(owns[1:], parts[1:]):
            total = jnp.where(own, part, total)
        return total

    results = []
    for d in range(2):
        x, y = [], []
        for h in range(heads):
            both = dot(solved[d, h], jnp.concatenate([starts[d], seen[d, h]], axis=1))
            x.append(both[:, :lanes])
            y.append(both[:, lanes:])
        x, y = gathered(x), gathered(y)
        if d == 0:
            weigh = whole if spikes is None else whole * jnp.exp(b_end - b_after)
        else:
            weigh = jnp.ones_like(whole) if spikes is None else jnp.exp(b_before)
        last_keys, last_removals = keys[d] * weigh, removals[d] * weigh
        offset = dot(
            jnp.concatenate([v.astype(F32), -y], axis=0),
            jnp.concatenate([last_keys, last_removals], axis=0),
            ((0,), (0,)),
        )
        if q is None:
            results.append((None, offset, None, None))
            continue
        decay = whole if spikes is None else jnp.exp(end + b_end)
        factor = jnp.where(row == col, decay, 0.0) - dot(x, last_removals, ((0,), (0,)))
        if d == 0:
            query = scaled(asks[0], b_after)
        else:
            query = scaled(asks[1] * whole, None if spikes is None else b_end - b_before)
        wx, base = [], []
        for h in range(heads):
            n = chains.index((d, h))
            mask = pair(h, d == 1, False)
            reads = scores[n][count:] * jnp.concatenate([mask, mask], axis=1)
            both = dot(reads[:, :count], jnp.concatenate([x, y], axis=1))
            wx.append(both[:, :lanes])
            base.append(dot(reads[:, count:], v) - both[:, lanes:])
        results.append((factor, offset, query - gathered(wx), gathered(base)))
    return results


def same_head(shape):
    return (iota(shape, 0) // HEAD) == (iota(shape, 1) // HEAD)


def maps_kernel(place, q, k, v, low, fading, step, rates, spikes, sent, asked, base):
    count = q.shape[0]
    ahead, behind = block_terms(
        k[:count], v[:count], low[:, :HEAD], fading[...], step[...], rates[...], spikes[...], q[...]
    )
    same = same_head(ahead[0].shape)
    packed = [
        jnp.where(same, factor, pltpu.roll(offset, HEAD, 0)).astype(BF16)
        for factor, offset in (ahead[:2], behind[:2])
    ]
    for j in range(sent.shape[0]):
        sent[j] = jnp.where(place[0] < j, packed[0], packed[1])
    asked[0], asked[1] = ahead[2].astype(BF16), behind[2].astype(BF16)
    base[...] = ahead[3] + behind[3]


def context_kernel(got, fading, step, rates, state):
    blocks, extra, lanes = got.shape[0], got.shape[1], got.shape[2] // 3
    parts = [
        got[:, :, n * lanes : (n + 1) * lanes].astype(F32).reshape(blocks * extra, lanes).astype(BF16)
        for n in range(3)
    ]
    ahead, behind = block_terms(parts[0], parts[1], parts[2][:, :HEAD], fading[...], step[...], rates[...])
    same = same_head(ahead[1].shape)
    state[0], state[1] = jnp.where(same, ahead[1], 0.0), jnp.where(same, behind[1], 0.0)


def read_kernel(place, maps, state, asked, base, gains, emit, keep, give):
    peers, size, _ = maps.shape
    same = same_head((size, size))
    me, core = place[0], place[1]
    states = [state[0], state[1]]
    for n in range(peers - 1):
        for d, j, reached in ((0, n, n < me), (1, peers - 1 - n, peers - 1 - n > me)):
            packed = maps[j].astype(F32)
            factor = jnp.where(same, packed, 0.0)
            offset = jnp.where(same, pltpu.roll(packed, HEAD, 0), 0.0)
            states[d] = jnp.where(reached, dot(states[d], factor) + offset, states[d])
    out = base[...]
    for d in range(2):
        out = out + dot(asked[d], states[d], ((1,), (1,)))
    first = iota(out.shape, 1) < HEAD

    def mean(value):
        left = jnp.sum(jnp.where(first, value, 0.0), -1, keepdims=True)
        right = jnp.sum(jnp.where(first, 0.0, value), -1, keepdims=True)
        return jnp.where(first, left, right) * (1.0 / HEAD)

    out = out - mean(out)
    normed = out * lax.rsqrt(mean(out * out) + EPS_HEAD) * gains[...]
    chips, rows, width = keep.shape
    split = normed.reshape(chips, 2, rows, size)
    even, odd = split[:, 0].reshape(chips * rows, size), split[:, 1].reshape(chips * rows, size)
    mine = jnp.where(core == 0, even, odd)
    other = jnp.where(core == 0, odd, even)
    left = jnp.concatenate([mine, other], axis=0).astype(BF16)
    lane = emit.shape[2]
    for s in range(emit.shape[0]):
        part = dot(left, emit[s]).reshape(2, chips, rows, lane).astype(BF16)
        keep[:, :, s * lane : (s + 1) * lane] = part[0]
        give[:, :, s * lane : (s + 1) * lane] = part[1]


def last_kernel(parts, hidden, vectors, out):
    lane = vectors.shape[2]
    for t in range(vectors.shape[0]):
        cols = slice(t * lane, (t + 1) * lane)
        total = parts[0, :, cols].astype(F32)
        for n in range(1, parts.shape[0]):
            total = total + parts[n, :, cols].astype(F32)
        out[:, cols] = (hidden[:, cols].astype(F32) + vectors[t, 4:5, :] * total).astype(BF16)


def exchange(blocks, axis, groups=None):
    return lax.all_to_all(blocks, axis, 0, 0, tiled=True, axis_index_groups=groups)


def spread(shard, axis):
    return exchange(jnp.broadcast_to(shard[None], (lax.axis_size(axis), *shard.shape)), axis)


def shards(
    hidden_items,
    sample_cond,
    prompt_items,
    prompt_cond,
    adjust_shifting,
    adjust_stretch,
    skip_valve,
    receiver_matrix,
    address_matrix,
    payload_matrix,
    joint_lower_projector,
    fading_raise_matrix,
    step_raise_matrix,
    feature_fading,
    spike_logfade,
    group_standard_factor,
    emit_matrix,
):
    n_sp, n_tp = lax.axis_size("sp"), lax.axis_size("tp")
    me, tp = lax.axis_index("sp"), lax.axis_index("tp")
    rows, width = hidden_items.shape
    extra = prompt_items.shape[0]
    count = rows * n_tp
    lanes = receiver_matrix.shape[1]
    span, chunk = adjust_shifting.shape
    place = jnp.stack([me, tp % 2]).astype(jnp.int32)

    parts = call(
        partials_kernel,
        ((n_sp, 8, chunk), F32),
        place,
        sample_cond.reshape(-1, span),
        prompt_cond.reshape(-1, span),
        adjust_shifting,
        adjust_stretch,
        skip_valve,
        scalars=1,
        flops=8 * span * chunk * 6,
    )
    parts = exchange(parts, "sp")
    latent = spread(hidden_items, "tp").reshape(count, width)
    half = joint_lower_projector.shape[0] // 2
    packed = jnp.concatenate([joint_lower_projector[:half], joint_lower_projector[half:]], axis=1)
    piece = half // n_tp
    pieces = spread(lax.dynamic_slice_in_dim(packed, tp * piece, piece, 0), "sp")
    emit = spread(emit_matrix, "sp")

    vectors = exchange(call(sum_kernel, ((n_tp, 8, chunk), F32), parts), "tp")
    pieces = spread(pieces, "tp")

    padded = count + -(-extra // 16) * 16
    u, q, k, v = call(
        rows_kernel,
        [((padded, width), BF16), ((count, lanes), BF16), ((padded, lanes), BF16), ((padded, lanes), BF16)],
        latent,
        prompt_items,
        vectors,
        receiver_matrix,
        address_matrix,
        payload_matrix,
        flops=2 * padded * width * lanes * 3,
    )
    low, payload = call(
        low_kernel,
        [((count, lanes), BF16), ((n_sp, extra, 3 * lanes), BF16)],
        u,
        pieces,
        k,
        v,
        flops=2 * padded * width * lanes,
        scratch=[pltpu.VMEM((width, lanes), BF16)],
    )
    ctx = exchange(payload, "sp")
    rates = feature_fading.reshape(1, lanes)
    sent, asked, base = call(
        maps_kernel,
        [((n_sp, lanes, lanes), BF16), ((2, count, lanes), BF16), ((count, lanes), F32)],
        place,
        q,
        k,
        v,
        low,
        fading_raise_matrix,
        step_raise_matrix,
        rates,
        spike_logfade,
        scalars=1,
        flops=2 * 128**3 * 100,
    )
    maps = exchange(sent, "sp")
    state = call(
        context_kernel,
        ((2, lanes, lanes), F32),
        ctx,
        fading_raise_matrix,
        step_raise_matrix,
        rates,
        flops=2 * 128**3 * 80,
    )
    chips = n_tp // 2
    keep, give = call(
        read_kernel,
        [((chips, rows, width), BF16)] * 2,
        place,
        maps,
        state,
        asked,
        base,
        group_standard_factor.reshape(1, lanes),
        emit,
        scalars=1,
        flops=2 * count * lanes * width,
    )
    given = lax.ppermute(give, "tp", [(i, i ^ 1) for i in range(n_tp)])
    both = (keep.astype(F32) + given.astype(F32)).astype(BF16)
    final = exchange(both, "tp", [[2 * i + c for i in range(chips)] for c in range(2)])
    return call(last_kernel, ((rows, width), BF16), final, hidden_items, vectors)


def solution(mesh):
    placed = (
        P(("grp", "sp", "tp"), None),
        P("grp"),
        P(("grp", "sp"), None),
        P(),
        P("sp", "tp"),
        P("sp", "tp"),
        P("sp", "tp"),
        P(None, "tp"),
        P(None, "tp"),
        P(None, "tp"),
        P("sp", None),
        P(None, "tp"),
        P(None, "tp"),
        P("tp"),
        P(("grp", "sp"), "tp"),
        P("tp"),
        P("tp", "sp"),
    )
    return jax.shard_map(
        shards, mesh=mesh, in_specs=placed, out_specs=P(("grp", "sp", "tp"), None), check_vma=False
    )
```

```python
import math

import jax
import jax.numpy as jnp
from jax import lax
from jax.experimental import pallas as pl
from jax.experimental.pallas import tpu as pltpu
from jax.sharding import PartitionSpec as P


HEAD = 64
EPS_ROW = 1e-05
EPS_HEAD = 0.00064
EPS_KEY = 1e-06
RATE_SHIFT = 5.0
NEVER = -1e30
BF16, F32 = jnp.bfloat16, jnp.float32

VMEM = pl.BlockSpec(memory_space=pltpu.VMEM)
SMEM = pl.BlockSpec(memory_space=pltpu.SMEM)
ANY = pl.BlockSpec(memory_space=pl.ANY)


def call(body, outs, *args, flops=0, scalars=0, scratch=(), fetched=0):
    many = isinstance(outs, list)
    shapes = [jax.ShapeDtypeStruct(s, d) for s, d in (outs if many else [outs])]
    got = pl.pallas_call(
        body,
        out_shape=shapes,
        in_specs=[SMEM] * scalars + [VMEM] * (len(args) - scalars - fetched) + [ANY] * fetched,
        out_specs=[VMEM] * len(shapes),
        scratch_shapes=list(scratch),
        compiler_params=pltpu.CompilerParams(vmem_limit_bytes=48 * 1024 * 1024),
        cost_estimate=pl.CostEstimate(
            flops=flops, transcendentals=0, bytes_accessed=sum(a.size * a.dtype.itemsize for a in args)
        ),
    )(*args)
    return got if many else got[0]


def dot(left, right, dims=((1,), (0,))):
    return lax.dot_general(
        left.astype(BF16), right.astype(BF16), (dims, ((), ())), preferred_element_type=F32
    )


def iota(shape, dim):
    return lax.broadcasted_iota(jnp.int32, shape, dim)


def partials_kernel(place, sample, prompt, lower, shifting, stretch, valve, out, held, sems):
    copies = [
        pltpu.make_async_copy(ref, held.at[n], sems.at[n]) for n, ref in enumerate((shifting, stretch, valve))
    ]
    for copy in copies:
        copy.start()
    _, rows, _ = out.shape
    chunk = held.shape[2]
    wide = chunk // sample.shape[1]
    line = iota(sample.shape, 0)

    def own(cond):
        full = cond[...].astype(F32)
        cut = [
            jnp.sum(jnp.where(line == place[0] * wide + n, full, 0.0), axis=0, keepdims=True) for n in range(wide)
        ]
        return jax.nn.silu(jnp.concatenate(cut, axis=1))

    row = iota((rows, chunk), 0)
    first, second = own(sample), own(prompt)

    def at(k, both):
        left = jnp.where(row == k, first, 0.0)
        return jnp.where(row == k + 1, second, left) if both else left

    half = lower.shape[0] // 2
    blocks = lower[...].astype(F32).reshape(2 * half // rows, rows, lower.shape[1])
    number = iota(blocks.shape, 0)
    halves = [
        jnp.sum(jnp.where(number == place[2] + n * (half // rows), blocks, 0.0), axis=0) for n in range(2)
    ]
    piece = jnp.concatenate(halves, axis=1)
    for copy in copies:
        copy.wait()
    total = dot(at(0, True), held[0]) + dot(at(2, True), held[1]) + dot(at(4, False), held[2])
    out[...] = jnp.broadcast_to(jnp.concatenate([total, piece], axis=1)[None], out.shape)


def sum_kernel(parts, out):
    chunk = parts.shape[2] - out.shape[3]
    lanes = out.shape[3]
    total = parts[0, :, :chunk]
    for k in range(1, parts.shape[0]):
        total = total + parts[k, :, :chunk]
    high = total.astype(BF16)
    rest = (total - high.astype(F32)).astype(BF16)
    blocks = [parts[k, :, chunk:].astype(BF16) for k in range(parts.shape[0])]
    for value in (high, rest):
        blocks += [value[:, n : n + lanes] for n in range(0, chunk, lanes)]
    for p in range(out.shape[0]):
        for n, block in enumerate(blocks):
            out[p, n] = block


def by_core(core, own, other):
    return jnp.where(core == 0, own, other), jnp.where(core == 0, other, own)


def placed_rows(value, tp, held):
    count = held.shape[0]
    for n in range(count):
        held[tp ^ mask_of(n, count)] = value[n * held.shape[1] : (n + 1) * held.shape[1]]
    return held[...].reshape(count * held.shape[1], held.shape[2])


def mask_of(n, count):
    half = count // 2
    bits = half.bit_length() - 1
    inner = n % half
    mask = sum(((inner >> b) & 1) << (bits - b) for b in range(bits))
    return mask | (n // half)


def rows_kernel(place, near, far, context, mine, theirs, wq, wk, wv, u, q, k, v, vectors, held, moved, sems):
    copies = [pltpu.make_async_copy(ref, held.at[n], sems.at[n]) for n, ref in enumerate((wq, wk, wv))]
    for copy in copies:
        copy.start()
    half, width = near.shape
    count, extra = 2 * half, context.shape[0]
    lane = vectors.shape[2]
    lanes = mine.shape[3]
    spans = lane // lanes
    first = mine.shape[1] - 2 * spans
    for x in range(mine.shape[0]):
        found = []
        for ref in (mine, theirs):
            cut = [ref[x, first + n].astype(F32) + ref[x, first + spans + n].astype(F32) for n in range(spans)]
            found.append(jnp.concatenate(cut, axis=1))
        vectors[2 * x], vectors[2 * x + 1] = by_core(place[1], *found)

    def moments(ref):
        total = jnp.zeros((ref.shape[0], lane), F32)
        for c in range(0, width, lane):
            total = total + ref[:, c : c + lane].astype(F32)
        centre = jnp.sum(total, -1, keepdims=True) * (1.0 / width)
        total = jnp.zeros((ref.shape[0], lane), F32)
        for c in range(0, width, lane):
            off = ref[:, c : c + lane].astype(F32) - centre
            total = total + off * off
        spread = jnp.sum(total, -1, keepdims=True) * (1.0 / width)
        return centre, lax.rsqrt(spread + EPS_ROW)

    stats = [moments(ref) for ref in (near, far, context)]
    pad = jnp.zeros((u.shape[0] - count - extra, lane), F32)
    for t in range(width // lane):
        cols = slice(t * lane, (t + 1) * lane)

        def one(n, ref, i):
            normed = (ref[:, cols].astype(F32) - stats[n][0]) * stats[n][1]
            return normed * (1.0 + vectors[t, 2 + i : 3 + i, :]) + vectors[t, i : i + 1, :]

        u[:half, cols] = one(0, near, 0).astype(BF16)
        u[half:count, cols] = one(1, far, 0).astype(BF16)
        u[count:, cols] = jnp.concatenate([one(2, context, 1), pad], axis=0).astype(BF16)
    for copy in copies:
        copy.wait()
    q[...] = placed_rows(dot(u[:count], held[0]), place[2], moved).astype(BF16)
    for out, n in ((k, 1), (v, 2)):
        found = dot(u[...], held[n])
        out[:count] = placed_rows(found[:count], place[2], moved).astype(BF16)
        out[count:] = found[count:].astype(BF16)


def low_kernel(place, u, mine, theirs, k, v, low, payload, down, moved):
    lane = mine.shape[3]
    blocks = down.shape[0] // (2 * lane)
    for s in range(blocks):
        even, odd = by_core(place[1], mine[:, s].astype(F32), theirs[:, s].astype(F32))
        piece = jnp.stack([even, odd], axis=1).reshape(lane, lane)
        down[2 * s * lane : (2 * s + 1) * lane] = piece.astype(BF16)
        down[(2 * s + 1) * lane : (2 * s + 2) * lane] = pltpu.roll(piece, HEAD, 1).astype(BF16)
    result = dot(u[...], down[...])
    result = jnp.where(iota(result.shape, 1) < HEAD, result, 0.0)
    count, extra = low.shape[0], payload.shape[0]
    low[...] = placed_rows(result[:count], place[2], moved).astype(BF16)
    for at, part in enumerate((k[count:].astype(F32), v[count:].astype(F32), result[count:])):
        payload[:, at * lane : (at + 1) * lane] = part[:extra].astype(BF16)


def inverse(mixing, row, col, upper):
    size = mixing[0].shape[0]
    eye = (row == col).astype(F32)
    width = 1
    found = None
    while width < size:
        here, there = (col, row) if upper else (row, col)
        shared = (row // (2 * width)) == (col // (2 * width))
        corner = shared & ((here // width) % 2 == 1) & ((there // width) % 2 == 0)
        parts = [jnp.where(corner, m, 0.0) for m in mixing]
        if found is None:
            found = [eye - p for p in parts]
        else:
            lefts = [dot(p, f) for p, f in zip(parts, found)]
            found = [f - dot(f, g) for f, g in zip(found, lefts)]
        width *= 2
    return found


def block_terms(k, v, low, fading, step, rates, spikes=None, q=None):
    count, lanes = k.shape
    row, col = iota((count, lanes), 0), iota((count, lanes), 1)
    heads = lanes // HEAD
    owns = [(col // HEAD) == h for h in range(heads)]

    squashed = jnp.tanh(low.astype(F32)).astype(BF16)
    feature = -rates * jax.nn.sigmoid(dot(squashed, fading))
    learned = jax.nn.sigmoid(dot(squashed, step) - RATE_SHIFT)
    key = k.astype(F32)
    norms = jnp.zeros_like(key)
    for own in owns:
        total = jnp.sum(jnp.where(own, key * key, 0.0), -1, keepdims=True)
        norms = jnp.where(own, lax.rsqrt(total + EPS_KEY), norms)
    unit = key * norms
    removal = unit * learned

    upto = (row >= col).astype(F32)

    def running(part):
        return lax.dot_general(
            upto, part, (((1,), (0,)), ((), ())), preferred_element_type=F32, precision=lax.Precision.HIGHEST
        )

    after = running(feature)
    before = after - feature
    grow, shrink = jnp.exp(after), jnp.exp(-after)
    grow_x, shrink_x = jnp.exp(before), jnp.exp(-before)
    end = after[count - 1 : count]
    if spikes is None:
        b_end = b_after = b_before = None
    else:
        jump = jnp.zeros_like(key)
        for h, own in enumerate(owns):
            jump = jnp.where(own, -spikes[:, h : h + 1], jump)
        b_after = running(jump)
        b_before = b_after - jump
        b_end = b_after[count - 1 : count]
        across_after, across_before = b_after.T, b_before.T

    def pair(h, upper, strict):
        inside = ((col > row) if strict else (col >= row)) if upper else ((col < row) if strict else (col <= row))
        if spikes is None:
            return inside.astype(F32)
        at = h * HEAD
        down_after, down_before = b_after[:, at : at + 1], b_before[:, at : at + 1]
        side_after, side_before = across_after[at : at + 1], across_before[at : at + 1]
        if upper:
            power = side_before - (down_after if strict else down_before)
        else:
            power = (down_before if strict else down_after) - side_after
        return jnp.where(inside, jnp.exp(jnp.where(inside, power, NEVER)), 0.0)

    def scaled(tensor, power):
        return tensor if spikes is None else tensor * jnp.exp(power)

    probes = (unit * grow_x, unit * shrink)
    removals = (removal * shrink, removal * grow_x)
    keys = (key * shrink, key * grow_x)
    asks = None if q is None else (q.astype(F32) * grow, q.astype(F32) * shrink_x)

    scores = []
    for d in range(2):
        right = jnp.concatenate([removals[d], keys[d]], axis=0)
        for own in owns:
            left = jnp.where(own, probes[d], 0.0)
            if q is not None:
                left = jnp.concatenate([left, jnp.where(own, asks[d], 0.0)], axis=0)
            scores.append(dot(left, right, ((1,), (1,))))
    chains = [(d, h) for d in range(2) for h in range(heads)]
    masks = {(d, h): pair(h, d == 1, True) for d, h in chains}
    mixing = {c: scores[n][:count, :count] * masks[c] for n, c in enumerate(chains)}
    seen = {c: dot(scores[n][:count, count:] * masks[c], v) for n, c in enumerate(chains)}
    solved = {}
    for d in range(2):
        found = inverse([mixing[d, h] for h in range(heads)], row, col, d == 1)
        for h in range(heads):
            solved[d, h] = found[h]

    whole = jnp.exp(end)
    starts = (
        scaled(probes[0], b_before),
        scaled(probes[1] * whole, None if spikes is None else b_end - b_after),
    )

    def gathered(parts):
        total = parts[0]
        for own, part in zip(owns[1:], parts[1:]):
            total = jnp.where(own, part, total)
        return total

    results = []
    for d in range(2):
        x, y = [], []
        for h in range(heads):
            both = dot(solved[d, h], jnp.concatenate([starts[d], seen[d, h]], axis=1))
            x.append(both[:, :lanes])
            y.append(both[:, lanes:])
        x, y = gathered(x), gathered(y)
        if d == 0:
            weigh = whole if spikes is None else whole * jnp.exp(b_end - b_after)
        else:
            weigh = jnp.ones_like(whole) if spikes is None else jnp.exp(b_before)
        last_keys, last_removals = keys[d] * weigh, removals[d] * weigh
        offset = dot(
            jnp.concatenate([v.astype(F32), -y], axis=0),
            jnp.concatenate([last_keys, last_removals], axis=0),
            ((0,), (0,)),
        )
        if q is None:
            results.append((None, offset, None, None))
            continue
        decay = whole if spikes is None else jnp.exp(end + b_end)
        factor = jnp.where(row == col, decay, 0.0) - dot(x, last_removals, ((0,), (0,)))
        if d == 0:
            query = scaled(asks[0], b_after)
        else:
            query = scaled(asks[1] * whole, None if spikes is None else b_end - b_before)
        wx, base = [], []
        for h in range(heads):
            n = chains.index((d, h))
            mask = pair(h, d == 1, False)
            reads = scores[n][count:] * jnp.concatenate([mask, mask], axis=1)
            both = dot(reads[:, :count], jnp.concatenate([x, y], axis=1))
            wx.append(both[:, :lanes])
            base.append(dot(reads[:, count:], v) - both[:, lanes:])
        results.append((factor, offset, query - gathered(wx), gathered(base)))
    return results


def same_head(shape):
    return (iota(shape, 0) // HEAD) == (iota(shape, 1) // HEAD)


def maps_kernel(place, q, k, v, low, fading, step, rates, spikes, sent, asked, base):
    count = q.shape[0]
    ahead, behind = block_terms(
        k[:count], v[:count], low[:, :HEAD], fading[...], step[...], rates[...], spikes[...], q[...]
    )
    same = same_head(ahead[0].shape)
    packed = [
        jnp.where(same, factor, pltpu.roll(offset, HEAD, 0)).astype(BF16)
        for factor, offset in (ahead[:2], behind[:2])
    ]
    for j in range(sent.shape[0]):
        sent[j] = jnp.where(place[0] < j, packed[0], packed[1])
    asked[0], asked[1] = ahead[2].astype(BF16), behind[2].astype(BF16)
    base[...] = ahead[3] + behind[3]


def context_kernel(place, got, fading, step, rates, state, moved):
    blocks, extra, lanes = got.shape[0], got.shape[1], got.shape[2] // 3
    for n in range(blocks):
        moved[place[0] ^ n] = got[n].astype(F32)
    parts = [
        moved[:, :, n * lanes : (n + 1) * lanes].reshape(blocks * extra, lanes).astype(BF16) for n in range(3)
    ]
    ahead, behind = block_terms(parts[0], parts[1], parts[2][:, :HEAD], fading[...], step[...], rates[...])
    same = same_head(ahead[1].shape)
    state[0], state[1] = jnp.where(same, ahead[1], 0.0), jnp.where(same, behind[1], 0.0)


def read_kernel(place, maps, state, asked, base, gains, emit_0, emit_1, emit_2, emit_3, keep, give):
    peers, size, _ = maps.shape
    same = same_head((size, size))
    me, core = place[0], place[1]
    states = [state[0], state[1]]
    for n in range(peers - 1):
        for d, j, reached in ((0, n, n < me), (1, peers - 1 - n, peers - 1 - n > me)):
            packed = maps[j].astype(F32)
            factor = jnp.where(same, packed, 0.0)
            offset = jnp.where(same, pltpu.roll(packed, HEAD, 0), 0.0)
            states[d] = jnp.where(reached, dot(states[d], factor) + offset, states[d])
    out = base[...]
    for d in range(2):
        out = out + dot(asked[d], states[d], ((1,), (1,)))
    first = iota(out.shape, 1) < HEAD

    def mean(value):
        left = jnp.sum(jnp.where(first, value, 0.0), -1, keepdims=True)
        right = jnp.sum(jnp.where(first, 0.0, value), -1, keepdims=True)
        return jnp.where(first, left, right) * (1.0 / HEAD)

    out = out - mean(out)
    normed = out * lax.rsqrt(mean(out * out) + EPS_HEAD) * gains[...]
    chips, rows, _ = keep.shape
    split = normed.reshape(chips, 2, rows, size)
    even, odd = split[:, 0].reshape(chips * rows, size), split[:, 1].reshape(chips * rows, size)
    mine = jnp.where(core == 0, even, odd)
    other = jnp.where(core == 0, odd, even)
    left = jnp.concatenate([mine, other], axis=0).astype(BF16)
    lane = emit_0.shape[2]
    fours = emit_0.shape[0]
    for b, emit in enumerate((emit_0, emit_1, emit_2, emit_3)):
        for a in range(fours):
            block = fours * ((me // fours - a + fours) % fours) + (me - b + fours) % fours
            cols = pl.ds(pl.multiple_of(block * lane, lane), lane)
            part = dot(left, emit[a]).reshape(2, chips, rows, lane).astype(BF16)
            keep[:, :, cols] = part[0]
            give[:, :, cols] = part[1]


def last_kernel(parts, hidden, vectors, out):
    lane = vectors.shape[2]
    for t in range(vectors.shape[0]):
        cols = slice(t * lane, (t + 1) * lane)
        total = parts[0, :, cols].astype(F32)
        for n in range(1, parts.shape[0]):
            total = total + parts[n, :, cols].astype(F32)
        out[:, cols] = (hidden[:, cols].astype(F32) + vectors[t, 4:5, :] * total).astype(BF16)


def exchange(blocks, axis, groups=None):
    return lax.all_to_all(blocks, axis, 0, 0, tiled=True, axis_index_groups=groups)


def swapped(value, axis, bit):
    return lax.ppermute(value, axis, [(i, i ^ bit) for i in range(lax.axis_size(axis))])


def shards(
    hidden_items,
    sample_cond,
    prompt_items,
    prompt_cond,
    adjust_shifting,
    adjust_stretch,
    skip_valve,
    receiver_matrix,
    address_matrix,
    payload_matrix,
    joint_lower_projector,
    fading_raise_matrix,
    step_raise_matrix,
    feature_fading,
    spike_logfade,
    group_standard_factor,
    emit_matrix,
):
    n_sp, n_tp = lax.axis_size("sp"), lax.axis_size("tp")
    me, tp = lax.axis_index("sp"), lax.axis_index("tp")
    rows, width = hidden_items.shape
    extra = prompt_items.shape[0]
    count = rows * n_tp
    lanes = receiver_matrix.shape[1]
    span, chunk = adjust_shifting.shape
    chips = n_tp // 2
    same_core = [[2 * i + c for i in range(chips)] for c in range(2)]
    place = jnp.stack([me, tp % 2, tp]).astype(jnp.int32)

    parts = call(
        partials_kernel,
        ((n_sp, 8, chunk + lanes), F32),
        place,
        sample_cond.reshape(-1, lanes),
        prompt_cond.reshape(-1, lanes),
        joint_lower_projector,
        adjust_shifting,
        adjust_stretch,
        skip_valve,
        scalars=1,
        fetched=3,
        flops=8 * span * chunk * 6,
        scratch=[pltpu.VMEM((3, span, chunk), BF16), pltpu.SemaphoreType.DMA((3,))],
    )
    parts = exchange(parts, "sp")

    near, bit = hidden_items[None], n_tp // 2
    while bit > 1:
        near = jnp.concatenate([near, swapped(near, "tp", bit)], axis=0)
        bit //= 2
    far = swapped(near, "tp", 1)

    fours = math.isqrt(n_sp)
    emits = jnp.stack(
        [emit_matrix]
        + [lax.ppermute(emit_matrix, "sp", [(i, (i + fours * a) % n_sp) for i in range(n_sp)]) for a in range(1, fours)]
    )
    emits = [emits] + [
        lax.ppermute(emits, "sp", [(i, i // fours * fours + (i + b) % fours) for i in range(n_sp)])
        for b in range(1, fours)
    ]

    spans = chunk // lanes
    mine = call(sum_kernel, ((chips, n_sp + 2 * spans, 8, lanes), BF16), parts)
    mine = exchange(mine, "tp", same_core)
    theirs = swapped(mine, "tp", 1)

    padded = count + -(-extra // 16) * 16
    u, q, k, v, vectors = call(
        rows_kernel,
        [
            ((padded, width), BF16),
            ((count, lanes), BF16),
            ((padded, lanes), BF16),
            ((padded, lanes), BF16),
            ((n_tp, 8, chunk), F32),
        ],
        place,
        near.reshape(count // 2, width),
        far.reshape(count // 2, width),
        prompt_items,
        mine,
        theirs,
        receiver_matrix,
        address_matrix,
        payload_matrix,
        scalars=1,
        fetched=3,
        flops=2 * padded * width * lanes * 3,
        scratch=[
            pltpu.VMEM((3, width, lanes), BF16),
            pltpu.VMEM((n_tp, rows, lanes), F32),
            pltpu.SemaphoreType.DMA((3,)),
        ],
    )
    low, payload = call(
        low_kernel,
        [((count, lanes), BF16), ((extra, 3 * lanes), BF16)],
        place,
        u,
        mine,
        theirs,
        k,
        v,
        scalars=1,
        flops=2 * padded * width * lanes,
        scratch=[pltpu.VMEM((width, lanes), BF16), pltpu.VMEM((n_tp, rows, lanes), F32)],
    )
    ctx, bit = payload[None], 1
    while bit < n_sp:
        ctx = jnp.concatenate([ctx, swapped(ctx, "sp", bit)], axis=0)
        bit *= 2
    rates = feature_fading.reshape(1, lanes)
    sent, asked, base = call(
        maps_kernel,
        [((n_sp, lanes, lanes), BF16), ((2, count, lanes), BF16), ((count, lanes), F32)],
        place,
        q,
        k,
        v,
        low,
        fading_raise_matrix,
        step_raise_matrix,
        rates,
        spike_logfade,
        scalars=1,
        flops=2 * 128**3 * 100,
    )
    maps = exchange(sent, "sp")
    state = call(
        context_kernel,
        ((2, lanes, lanes), F32),
        place,
        ctx,
        fading_raise_matrix,
        step_raise_matrix,
        rates,
        scalars=1,
        flops=2 * 128**3 * 80,
        scratch=[pltpu.VMEM((n_sp, extra, 3 * lanes), F32)],
    )
    keep, give = call(
        read_kernel,
        [((chips, rows, width), BF16)] * 2,
        place,
        maps,
        state,
        asked,
        base,
        group_standard_factor.reshape(1, lanes),
        *emits,
        scalars=1,
        flops=2 * count * lanes * width,
    )
    given = swapped(give, "tp", 1)
    both = (keep.astype(F32) + given.astype(F32)).astype(BF16)
    final = exchange(both, "tp", same_core)
    return call(last_kernel, ((rows, width), BF16), final, hidden_items, vectors)


def solution(mesh):
    placed = (
        P(("grp", "sp", "tp"), None),
        P("grp"),
        P(("grp", "sp"), None),
        P(),
        P("sp", "tp"),
        P("sp", "tp"),
        P("sp", "tp"),
        P(None, "tp"),
        P(None, "tp"),
        P(None, "tp"),
        P("sp", None),
        P(None, "tp"),
        P(None, "tp"),
        P("tp"),
        P(("grp", "sp"), "tp"),
        P("tp"),
        P("tp", "sp"),
    )

    return jax.shard_map(shards, mesh=mesh, in_specs=placed, out_specs=P(("grp", "sp", "tp"), None), check_vma=False)
```

```python
import jax
import jax.numpy as jnp
from jax import lax
from jax.experimental import pallas as pl
from jax.experimental.pallas import tpu as pltpu
from jax.sharding import PartitionSpec as P


HEAD = 64
EPS_ROW = 1e-05
EPS_HEAD = 0.00064
EPS_KEY = 1e-06
RATE_SHIFT = 5.0
NEVER = -1e30
BF16, F32 = jnp.bfloat16, jnp.float32

VMEM = pl.BlockSpec(memory_space=pltpu.VMEM)
SMEM = pl.BlockSpec(memory_space=pltpu.SMEM)
HBM = pl.BlockSpec(memory_space=pltpu.HBM)


def call(body, outs, *args, flops=0, scalars=0, scratch=(), fetched=0):
    many = isinstance(outs, list)
    shapes = [jax.ShapeDtypeStruct(s, d) for s, d in (outs if many else [outs])]
    got = pl.pallas_call(
        body,
        out_shape=shapes,
        in_specs=[SMEM] * scalars + [VMEM] * (len(args) - scalars - fetched) + [HBM] * fetched,
        out_specs=[VMEM] * len(shapes),
        scratch_shapes=list(scratch),
        compiler_params=pltpu.CompilerParams(vmem_limit_bytes=48 * 1024 * 1024),
        cost_estimate=pl.CostEstimate(
            flops=flops, transcendentals=0, bytes_accessed=sum(a.size * a.dtype.itemsize for a in args)
        ),
    )(*args)
    return got if many else got[0]


def dot(left, right, dims=((1,), (0,))):
    return lax.dot_general(
        left.astype(BF16), right.astype(BF16), (dims, ((), ())), preferred_element_type=F32
    )


def iota(shape, dim):
    return lax.broadcasted_iota(jnp.int32, shape, dim)


def partials_kernel(place, sample, prompt, lower, shifting, stretch, valve, out, conds, low_rows, held, sems):
    pairs = [(sample, conds.at[0]), (prompt, conds.at[1]), (lower, low_rows)]
    pairs += [(ref, held.at[n]) for n, ref in enumerate((shifting, stretch, valve))]
    copies = [pltpu.make_async_copy(ref, to, sems.at[n]) for n, (ref, to) in enumerate(pairs)]
    for copy in copies:
        copy.start()
    for copy in copies[:3]:
        copy.wait()
    _, rows, _ = out.shape
    chunk = held.shape[2]
    wide = chunk // sample.shape[1]
    line = iota(sample.shape, 0)

    def own(n):
        full = conds[n].astype(F32)
        cut = [
            jnp.sum(jnp.where(line == place[0] * wide + n, full, 0.0), axis=0, keepdims=True) for n in range(wide)
        ]
        return jax.nn.silu(jnp.concatenate(cut, axis=1))

    row = iota((rows, chunk), 0)
    first, second = own(0), own(1)

    def at(k, both):
        left = jnp.where(row == k, first, 0.0)
        return jnp.where(row == k + 1, second, left) if both else left

    upright = low_rows[...].astype(F32).T
    count = upright.shape[0] // rows
    blocks = upright.reshape(count, rows, upright.shape[1])
    number = iota(blocks.shape, 0)
    halves = [
        jnp.sum(jnp.where(number == place[2] + n * (count // 2), blocks, 0.0), axis=0) for n in range(2)
    ]
    piece = jnp.concatenate(halves, axis=1)
    for copy in copies[3:]:
        copy.wait()
    total = dot(at(0, True), held[0]) + dot(at(2, True), held[1]) + dot(at(4, False), held[2])
    out[...] = jnp.broadcast_to(jnp.concatenate([total, piece], axis=1)[None], out.shape)


def sum_kernel(parts, out):
    chunk = parts.shape[2] - out.shape[3]
    lanes = out.shape[3]
    total = parts[0, :, :chunk]
    for k in range(1, parts.shape[0]):
        total = total + parts[k, :, :chunk]
    high = total.astype(BF16)
    rest = (total - high.astype(F32)).astype(BF16)
    blocks = [parts[k, :, chunk:].astype(BF16) for k in range(parts.shape[0])]
    for value in (high, rest):
        blocks += [value[:, n : n + lanes] for n in range(0, chunk, lanes)]
    for p in range(out.shape[0]):
        for n, block in enumerate(blocks):
            out[p, n] = block


def by_core(core, own, other):
    return jnp.where(core == 0, own, other), jnp.where(core == 0, other, own)


def moments(ref, lane):
    width = ref.shape[1]
    total = jnp.zeros((ref.shape[0], lane), F32)
    for c in range(0, width, lane):
        total = total + ref[:, c : c + lane].astype(F32)
    centre = jnp.sum(total, -1, keepdims=True) * (1.0 / width)
    total = jnp.zeros((ref.shape[0], lane), F32)
    for c in range(0, width, lane):
        off = ref[:, c : c + lane].astype(F32) - centre
        total = total + off * off
    spread = jnp.sum(total, -1, keepdims=True) * (1.0 / width)
    return centre, lax.rsqrt(spread + EPS_ROW)


def modulated(place, latent, context, mine, theirs, u, vectors, down):
    count, width = latent.shape
    extra = context.shape[0]
    lane, lanes = vectors.shape[2], mine.shape[3]
    spans = lane // lanes
    stats = [moments(ref, lane) for ref in (latent, context)]
    first = mine.shape[1] - 2 * spans
    for x in range(mine.shape[0]):
        found = []
        for ref in (mine, theirs):
            cut = [ref[x, first + n].astype(F32) + ref[x, first + spans + n].astype(F32) for n in range(spans)]
            found.append(jnp.concatenate(cut, axis=1))
        vectors[2 * x], vectors[2 * x + 1] = by_core(place[1], *found)
    pad = jnp.zeros((u.shape[0] - count - extra, lane), F32)
    for t in range(width // lane):
        cols = slice(t * lane, (t + 1) * lane)

        def one(n, ref, i):
            normed = (ref[:, cols].astype(F32) - stats[n][0]) * stats[n][1]
            return normed * (1.0 + vectors[t, 2 + i : 3 + i, :]) + vectors[t, i : i + 1, :]

        u[:count, cols] = one(0, latent, 0).astype(BF16)
        u[count:, cols] = jnp.concatenate([one(1, context, 1), pad], axis=0).astype(BF16)
    for s in range(down.shape[0] // (2 * lanes)):
        even, odd = by_core(place[1], mine[:, s].astype(F32), theirs[:, s].astype(F32))
        piece = jnp.stack([even, odd], axis=1).reshape(lanes, lanes)
        down[2 * s * lanes : (2 * s + 1) * lanes] = piece.astype(BF16)
        down[(2 * s + 1) * lanes : (2 * s + 2) * lanes] = pltpu.roll(piece, HEAD, 1).astype(BF16)


def inverse(mixing, row, col, upper):
    size = mixing[0].shape[0]
    eye = (row == col).astype(F32)
    width = 1
    found = None
    while width < size:
        here, there = (col, row) if upper else (row, col)
        shared = (row // (2 * width)) == (col // (2 * width))
        corner = shared & ((here // width) % 2 == 1) & ((there // width) % 2 == 0)
        parts = [jnp.where(corner, m, 0.0) for m in mixing]
        if found is None:
            found = [eye - p for p in parts]
        else:
            lefts = [dot(p, f) for p, f in zip(parts, found)]
            found = [f - dot(f, g) for f, g in zip(found, lefts)]
        width *= 2
    return found


def block_terms(k, v, low, fading, step, rates, spikes=None, q=None):
    count, lanes = k.shape
    row, col = iota((count, lanes), 0), iota((count, lanes), 1)
    heads = lanes // HEAD
    owns = [(col // HEAD) == h for h in range(heads)]

    squashed = jnp.tanh(low.astype(F32)).astype(BF16)
    feature = -rates * jax.nn.sigmoid(dot(squashed, fading))
    learned = jax.nn.sigmoid(dot(squashed, step) - RATE_SHIFT)
    key = k.astype(F32)
    norms = jnp.zeros_like(key)
    for own in owns:
        total = jnp.sum(jnp.where(own, key * key, 0.0), -1, keepdims=True)
        norms = jnp.where(own, lax.rsqrt(total + EPS_KEY), norms)
    unit = key * norms
    removal = unit * learned

    upto = (row >= col).astype(F32)

    def running(part):
        return lax.dot_general(
            upto, part, (((1,), (0,)), ((), ())), preferred_element_type=F32, precision=lax.Precision.HIGHEST
        )

    after = running(feature)
    before = after - feature
    grow, shrink = jnp.exp(after), jnp.exp(-after)
    grow_x, shrink_x = jnp.exp(before), jnp.exp(-before)
    end = after[count - 1 : count]
    if spikes is None:
        b_end = b_after = b_before = None
    else:
        across = jnp.zeros((lanes, count), F32)
        for h in range(heads):
            across = jnp.where(iota(across.shape, 0) // HEAD == h, -spikes[h : h + 1], across)
        jump = across.T
        b_after = running(jump)
        b_before = b_after - jump
        b_end = b_after[count - 1 : count]
        across_after, across_before = b_after.T, b_before.T

    def pair(h, upper, strict):
        inside = ((col > row) if strict else (col >= row)) if upper else ((col < row) if strict else (col <= row))
        if spikes is None:
            return inside.astype(F32)
        at = h * HEAD
        down_after, down_before = b_after[:, at : at + 1], b_before[:, at : at + 1]
        side_after, side_before = across_after[at : at + 1], across_before[at : at + 1]
        if upper:
            power = side_before - (down_after if strict else down_before)
        else:
            power = (down_before if strict else down_after) - side_after
        return jnp.where(inside, jnp.exp(jnp.where(inside, power, NEVER)), 0.0)

    def scaled(tensor, power):
        return tensor if spikes is None else tensor * jnp.exp(power)

    probes = (unit * grow_x, unit * shrink)
    removals = (removal * shrink, removal * grow_x)
    keys = (key * shrink, key * grow_x)
    asks = None if q is None else (q.astype(F32) * grow, q.astype(F32) * shrink_x)

    scores = []
    for d in range(2):
        right = jnp.concatenate([removals[d], keys[d]], axis=0)
        for own in owns:
            left = jnp.where(own, probes[d], 0.0)
            if q is not None:
                left = jnp.concatenate([left, jnp.where(own, asks[d], 0.0)], axis=0)
            scores.append(dot(left, right, ((1,), (1,))))
    chains = [(d, h) for d in range(2) for h in range(heads)]
    masks = {(d, h): pair(h, d == 1, True) for d, h in chains}
    mixing = {c: scores[n][:count, :count] * masks[c] for n, c in enumerate(chains)}
    seen = {c: dot(scores[n][:count, count:] * masks[c], v) for n, c in enumerate(chains)}
    solved = {}
    for d in range(2):
        found = inverse([mixing[d, h] for h in range(heads)], row, col, d == 1)
        for h in range(heads):
            solved[d, h] = found[h]

    whole = jnp.exp(end)
    starts = (
        scaled(probes[0], b_before),
        scaled(probes[1] * whole, None if spikes is None else b_end - b_after),
    )

    def gathered(parts):
        total = parts[0]
        for own, part in zip(owns[1:], parts[1:]):
            total = jnp.where(own, part, total)
        return total

    results = []
    for d in range(2):
        x, y = [], []
        for h in range(heads):
            both = dot(solved[d, h], jnp.concatenate([starts[d], seen[d, h]], axis=1))
            x.append(both[:, :lanes])
            y.append(both[:, lanes:])
        x, y = gathered(x), gathered(y)
        if d == 0:
            weigh = whole if spikes is None else whole * jnp.exp(b_end - b_after)
        else:
            weigh = jnp.ones_like(whole) if spikes is None else jnp.exp(b_before)
        last_keys, last_removals = keys[d] * weigh, removals[d] * weigh
        offset = dot(
            jnp.concatenate([v.astype(F32), -y], axis=0),
            jnp.concatenate([last_keys, last_removals], axis=0),
            ((0,), (0,)),
        )
        if q is None:
            results.append((None, offset, None, None))
            continue
        decay = whole if spikes is None else jnp.exp(end + b_end)
        factor = jnp.where(row == col, decay, 0.0) - dot(x, last_removals, ((0,), (0,)))
        if d == 0:
            query = scaled(asks[0], b_after)
        else:
            query = scaled(asks[1] * whole, None if spikes is None else b_end - b_before)
        wx, base = [], []
        for h in range(heads):
            n = chains.index((d, h))
            mask = pair(h, d == 1, False)
            reads = scores[n][count:] * jnp.concatenate([mask, mask], axis=1)
            both = dot(reads[:, :count], jnp.concatenate([x, y], axis=1))
            wx.append(both[:, :lanes])
            base.append(dot(reads[:, count:], v) - both[:, lanes:])
        results.append((factor, offset, query - gathered(wx), gathered(base)))
    return results


def same_head(shape):
    return (iota(shape, 0) // HEAD) == (iota(shape, 1) // HEAD)


def block_kernel(
    place, mine, theirs, latent_, context_, wq, wk, wv, fading_, step_, rates_, spikes_,
    sent, asked, base, vectors,
    latent, context, held, fading, step, rates, spikes, u, down, sems,
):
    pairs = [(latent_, latent), (context_, context)]
    pairs += [(ref, held.at[n]) for n, ref in enumerate((wq, wk, wv))]
    pairs += [(fading_, fading), (step_, step), (rates_, rates), (spikes_, spikes)]
    copies = [pltpu.make_async_copy(ref, to, sems.at[n]) for n, (ref, to) in enumerate(pairs)]
    for copy in copies:
        copy.start()
    for copy in copies[:2]:
        copy.wait()
    modulated(place, latent, context, mine, theirs, u, vectors, down)
    for copy in copies[2:]:
        copy.wait()
    count, extra = latent.shape[0], context.shape[0]
    q = dot(u[:count], held[0]).astype(BF16)
    k, v = dot(u[...], held[1]).astype(BF16), dot(u[...], held[2]).astype(BF16)
    low = dot(u[...], down[...])
    low = jnp.where(iota(low.shape, 1) < HEAD, low, 0.0).astype(BF16)
    ahead, behind = block_terms(
        k[:count], v[:count], low[:count, :HEAD], fading[...], step[...], rates[...], spikes[...], q
    )
    same = same_head(ahead[0].shape)
    packed = [
        jnp.where(same, factor, pltpu.roll(offset, HEAD, 0)).astype(BF16)
        for factor, offset in (ahead[:2], behind[:2])
    ]
    tail = [part[count:].astype(F32)[:extra] for part in (k, v, low)]
    tail = jnp.concatenate(tail + [jnp.zeros_like(tail[0])] * (-len(tail) % 2), axis=0).astype(BF16)
    size = packed[0].shape[0]
    for j in range(sent.shape[0]):
        sent[j, :size] = jnp.where(place[0] < j, packed[0], packed[1])
        sent[j, size:] = tail
    asked[0], asked[1] = ahead[2].astype(BF16), behind[2].astype(BF16)
    base[...] = ahead[3] + behind[3]


def read_kernel(
    place, maps, asked, base, fading_, step_, rates_, gains_, emit_,
    keep, give,
    fading, step, rates, gains, emit, sems,
):
    pairs = [(fading_, fading), (step_, step), (rates_, rates), (gains_, gains), (emit_, emit)]
    copies = [pltpu.make_async_copy(ref, to, sems.at[n]) for n, (ref, to) in enumerate(pairs)]
    for copy in copies:
        copy.start()
    peers, _, size = maps.shape
    extra = keep.shape[1]
    same = same_head((size, size))
    me, core = place[0], place[1]
    for copy in copies[:4]:
        copy.wait()
    parts = [
        jnp.concatenate([maps[j, size + n * extra : size + (n + 1) * extra].astype(F32) for j in range(peers)], axis=0)
        for n in range(3)
    ]
    parts = [part.astype(BF16) for part in parts]
    context = block_terms(parts[0], parts[1], parts[2][:, :HEAD], fading[...], step[...], rates[...])
    eye = (iota((size, size), 0) == iota((size, size), 1)).astype(F32)
    composed = [jnp.concatenate([eye, jnp.zeros_like(eye)], axis=0) for _ in range(2)]
    for n in range(peers - 1):
        for d, j, reached in ((0, n, n < me), (1, peers - 1 - n, peers - 1 - n > me)):
            packed = maps[j, :size].astype(F32)
            factor = jnp.where(same, packed, 0.0)
            offset = jnp.where(same, pltpu.roll(packed, HEAD, 0), 0.0)
            new = dot(composed[d], factor)
            new = jnp.concatenate([new[:size], new[size:] + offset], axis=0)
            composed[d] = jnp.where(reached, new, composed[d])
    out = base[...]
    for d in range(2):
        start = jnp.where(same, context[d][1], 0.0)
        state = dot(start, composed[d][:size]) + composed[d][size:]
        out = out + dot(asked[d], state, ((1,), (1,)))
    first = iota(out.shape, 1) < HEAD

    def mean(value):
        left = jnp.sum(jnp.where(first, value, 0.0), -1, keepdims=True)
        right = jnp.sum(jnp.where(first, 0.0, value), -1, keepdims=True)
        return jnp.where(first, left, right) * (1.0 / HEAD)

    out = out - mean(out)
    normed = out * lax.rsqrt(mean(out * out) + EPS_HEAD) * gains[...]
    chips, rows, _ = keep.shape
    split = normed.reshape(chips, 2, rows, size)
    even, odd = split[:, 0].reshape(chips * rows, size), split[:, 1].reshape(chips * rows, size)
    mine = jnp.where(core == 0, even, odd)
    other = jnp.where(core == 0, odd, even)
    left = jnp.concatenate([mine, other], axis=0).astype(BF16)
    copies[4].wait()
    lane = emit.shape[2]
    for s in range(emit.shape[0]):
        part = dot(left, emit[s]).reshape(2, chips, rows, lane).astype(BF16)
        keep[:, :, s * lane : (s + 1) * lane] = part[0]
        give[:, :, s * lane : (s + 1) * lane] = part[1]


def last_kernel(parts, hidden, vectors, out):
    lane = vectors.shape[2]
    for t in range(vectors.shape[0]):
        cols = slice(t * lane, (t + 1) * lane)
        total = parts[0, :, cols].astype(F32)
        for n in range(1, parts.shape[0]):
            total = total + parts[n, :, cols].astype(F32)
        out[:, cols] = (hidden[:, cols].astype(F32) + vectors[t, 4:5, :] * total).astype(BF16)


def exchange(blocks, axis, groups=None):
    return lax.all_to_all(blocks, axis, 0, 0, tiled=True, axis_index_groups=groups)


def swapped(value, axis, bit):
    return lax.ppermute(value, axis, [(i, i ^ bit) for i in range(lax.axis_size(axis))])


def shards(
    hidden_items,
    sample_cond,
    prompt_items,
    prompt_cond,
    adjust_shifting,
    adjust_stretch,
    skip_valve,
    receiver_matrix,
    address_matrix,
    payload_matrix,
    joint_lower_projector,
    fading_raise_matrix,
    step_raise_matrix,
    feature_fading,
    spike_logfade,
    group_standard_factor,
    emit_matrix,
):
    n_sp, n_tp = lax.axis_size("sp"), lax.axis_size("tp")
    me, tp = lax.axis_index("sp"), lax.axis_index("tp")
    rows, width = hidden_items.shape
    extra = prompt_items.shape[0]
    count = rows * n_tp
    lanes = receiver_matrix.shape[1]
    span, chunk = adjust_shifting.shape
    chips = n_tp // 2
    same_core = [[2 * i + c for i in range(chips)] for c in range(2)]
    place = jnp.stack([me, tp % 2, tp]).astype(jnp.int32)

    parts = call(
        partials_kernel,
        ((n_sp, 8, chunk + lanes), F32),
        place,
        sample_cond.reshape(-1, lanes),
        prompt_cond.reshape(-1, lanes),
        joint_lower_projector.T,
        adjust_shifting,
        adjust_stretch,
        skip_valve,
        scalars=1,
        fetched=6,
        flops=8 * span * chunk * 6,
        scratch=[
            pltpu.VMEM((2, width // lanes, lanes), BF16),
            pltpu.VMEM(joint_lower_projector.shape[::-1], BF16),
            pltpu.VMEM((3, span, chunk), BF16),
            pltpu.SemaphoreType.DMA((6,)),
        ],
    )
    latent = lax.all_gather(hidden_items, "tp", axis=0, tiled=True)
    emit = lax.all_gather(emit_matrix, "sp", axis=0)
    parts = exchange(parts, "sp")

    spans = chunk // lanes
    mine = call(sum_kernel, ((chips, n_sp + 2 * spans, 8, lanes), BF16), parts)
    mine = exchange(mine, "tp", same_core)
    theirs = swapped(mine, "tp", 1)

    padded = count + -(-extra // 16) * 16
    rates = feature_fading.reshape(1, lanes)
    small = [
        pltpu.VMEM(fading_raise_matrix.shape, BF16),
        pltpu.VMEM(step_raise_matrix.shape, BF16),
        pltpu.VMEM(rates.shape, F32),
    ]
    sent, asked, base, vectors = call(
        block_kernel,
        [
            ((n_sp, lanes + 4 * extra, lanes), BF16),
            ((2, count, lanes), BF16),
            ((count, lanes), F32),
            ((n_tp, 8, chunk), F32),
        ],
        place,
        mine,
        theirs,
        latent,
        prompt_items,
        receiver_matrix,
        address_matrix,
        payload_matrix,
        fading_raise_matrix,
        step_raise_matrix,
        rates,
        spike_logfade.T,
        scalars=1,
        fetched=9,
        flops=2 * padded * width * lanes * 4,
        scratch=[
            pltpu.VMEM((count, width), BF16),
            pltpu.VMEM((extra, width), BF16),
            pltpu.VMEM((3, width, lanes), BF16),
            *small,
            pltpu.VMEM(spike_logfade.shape[::-1], F32),
            pltpu.VMEM((padded, width), BF16),
            pltpu.VMEM((width, lanes), BF16),
            pltpu.SemaphoreType.DMA((9,)),
        ],
    )
    maps = exchange(sent, "sp")
    keep, give = call(
        read_kernel,
        [((chips, rows, width), BF16)] * 2,
        place,
        maps,
        asked,
        base,
        fading_raise_matrix,
        step_raise_matrix,
        rates,
        group_standard_factor.reshape(1, lanes),
        emit,
        scalars=1,
        fetched=5,
        flops=2 * count * lanes * width,
        scratch=[
            *small,
            pltpu.VMEM((1, lanes), F32),
            pltpu.VMEM((n_sp, *emit_matrix.shape), BF16),
            pltpu.SemaphoreType.DMA((5,)),
        ],
    )
    given = swapped(give, "tp", 1)
    both = (keep.astype(F32) + given.astype(F32)).astype(BF16)
    final = exchange(both, "tp", same_core)
    return call(last_kernel, ((rows, width), BF16), final, hidden_items, vectors)


def solution(mesh):
    placed = (
        P(("grp", "sp", "tp"), None),
        P("grp"),
        P(("grp", "sp"), None),
        P(),
        P("sp", "tp"),
        P("sp", "tp"),
        P("sp", "tp"),
        P(None, "tp"),
        P(None, "tp"),
        P(None, "tp"),
        P("sp", None),
        P(None, "tp"),
        P(None, "tp"),
        P("tp"),
        P(("grp", "sp"), "tp"),
        P("tp"),
        P("tp", "sp"),
    )

    return jax.shard_map(shards, mesh=mesh, in_specs=placed, out_specs=P(("grp", "sp", "tp"), None), check_vma=False)
```

```python
import jax
import jax.numpy as jnp
from jax import lax
from jax.experimental import pallas as pl
from jax.experimental.pallas import tpu as pltpu
from jax.sharding import PartitionSpec as P


HEAD = 64
EPS_ROW = 1e-05
EPS_HEAD = 0.00064
EPS_KEY = 1e-06
RATE_SHIFT = 5.0
NEVER = -1e30
SOME, ALL = 32 * 1024 * 1024, 63 * 1024 * 1024
BF16, F32 = jnp.bfloat16, jnp.float32

VMEM = pl.BlockSpec(memory_space=pltpu.VMEM)
SMEM = pl.BlockSpec(memory_space=pltpu.SMEM)
HBM = pl.BlockSpec(memory_space=pltpu.HBM)


def call(body, outs, *args, flops=0, scalars=0, scratch=(), fetched=0, room=SOME):
    many = isinstance(outs, list)
    shapes = [jax.ShapeDtypeStruct(s, d) for s, d in (outs if many else [outs])]
    got = pl.pallas_call(
        body,
        out_shape=shapes,
        in_specs=[SMEM] * scalars + [VMEM] * (len(args) - scalars - fetched) + [HBM] * fetched,
        out_specs=[VMEM] * len(shapes),
        scratch_shapes=list(scratch),
        compiler_params=pltpu.CompilerParams(vmem_limit_bytes=room),
        cost_estimate=pl.CostEstimate(
            flops=flops, transcendentals=0, bytes_accessed=sum(a.size * a.dtype.itemsize for a in args)
        ),
    )(*args)
    return got if many else got[0]


def dot(left, right, dims=((1,), (0,))):
    return lax.dot_general(
        left.astype(BF16), right.astype(BF16), (dims, ((), ())), preferred_element_type=F32
    )


def iota(shape, dim):
    return lax.broadcasted_iota(jnp.int32, shape, dim)


USED = 5


def packed_lines(total, lanes):
    high = total.astype(BF16).astype(F32)
    rest = total - high
    row = iota((total.shape[0], lanes), 0)
    last = rest[:, lanes:]
    free = total.shape[0] - USED
    return [
        jnp.where(row < USED, high[:, :lanes], pltpu.roll(last, USED, 0)).astype(BF16),
        jnp.where(row < USED, high[:, lanes:], pltpu.roll(last, USED - free, 0)).astype(BF16),
        rest[:, :lanes].astype(BF16),
    ]


def unpacked_lines(first, second, third):
    first, second, third = (part.astype(F32) for part in (first, second, third))
    count = first.shape[0]
    row = iota(first.shape, 0)
    free = count - USED
    last = jnp.where(row < free, pltpu.roll(first, count - USED, 0), pltpu.roll(second, count - USED + free, 0))
    return jnp.concatenate([first + third, second + last], axis=1)


def partials_kernel(place, sample, prompt, lower, shifting, stretch, valve, out, conds, low_rows, held, sems):
    pairs = [(sample, conds.at[0]), (prompt, conds.at[1]), (lower, low_rows)]
    pairs += [(ref, held.at[n]) for n, ref in enumerate((shifting, stretch, valve))]
    copies = [pltpu.make_async_copy(ref, to, sems.at[n]) for n, (ref, to) in enumerate(pairs)]
    for copy in copies:
        copy.start()
    for copy in copies[:3]:
        copy.wait()
    peers, _, rows, _ = out.shape
    chunk = held.shape[2]
    wide = chunk // sample.shape[1]
    line = iota(sample.shape, 0)

    def own(n):
        full = conds[n].astype(F32)
        cut = [
            jnp.sum(jnp.where(line == place[0] * wide + n, full, 0.0), axis=0, keepdims=True) for n in range(wide)
        ]
        return jax.nn.silu(jnp.concatenate(cut, axis=1))

    row = iota((rows, chunk), 0)
    first, second = own(0), own(1)

    def at(k, both):
        left = jnp.where(row == k, first, 0.0)
        return jnp.where(row == k + 1, second, left) if both else left

    upright = low_rows[...].astype(F32).T
    count = upright.shape[0] // rows
    blocks = upright.reshape(count, rows, upright.shape[1])
    number = iota(blocks.shape, 0)
    halves = [
        jnp.sum(jnp.where(number == place[2] + n * (count // 2), blocks, 0.0), axis=0) for n in range(2)
    ]
    piece = jnp.concatenate(halves, axis=1)
    for copy in copies[3:]:
        copy.wait()
    total = dot(at(0, True), held[0]) + dot(at(2, True), held[1]) + dot(at(4, False), held[2])
    for n, block in enumerate(packed_lines(total, out.shape[3]) + [piece.astype(BF16)]):
        for p in range(peers):
            out[p, n] = block


def sum_kernel(parts, out):
    lanes = out.shape[3]
    total = unpacked_lines(parts[0, 0], parts[0, 1], parts[0, 2])
    for k in range(1, parts.shape[0]):
        total = total + unpacked_lines(parts[k, 0], parts[k, 1], parts[k, 2])
    blocks = [parts[k, 3] for k in range(parts.shape[0])] + packed_lines(total, lanes)
    for p in range(out.shape[0]):
        for n, block in enumerate(blocks):
            out[p, n] = block


def by_core(core, own, other):
    return jnp.where(core == 0, own, other), jnp.where(core == 0, other, own)


def mask_of(n, count):
    half = count // 2
    bits = half.bit_length() - 1
    inner = n % half
    mask = sum(((inner >> b) & 1) << (bits - b) for b in range(bits))
    return mask | (n // half)


def placed_rows(value, tp, held):
    count, rows, lanes = held.shape
    for n in range(count):
        held[tp ^ mask_of(n, count)] = value[n * rows : (n + 1) * rows]
    return held[...].reshape(count * rows, lanes)


def moments(ref, lane):
    width = ref.shape[1]
    total = jnp.zeros((ref.shape[0], lane), F32)
    for c in range(0, width, lane):
        total = total + ref[:, c : c + lane].astype(F32)
    centre = jnp.sum(total, -1, keepdims=True) * (1.0 / width)
    total = jnp.zeros((ref.shape[0], lane), F32)
    for c in range(0, width, lane):
        off = ref[:, c : c + lane].astype(F32) - centre
        total = total + off * off
    spread = jnp.sum(total, -1, keepdims=True) * (1.0 / width)
    return centre, lax.rsqrt(spread + EPS_ROW)


def modulated(place, near, far, context, mine, theirs, u, vectors, down):
    half, width = near.shape
    count, extra = 2 * half, context.shape[0]
    lane, lanes = vectors.shape[2], mine.shape[3]
    stats = [moments(ref, lane) for ref in (near, far, context)]
    first = mine.shape[1] - 3
    for x in range(mine.shape[0]):
        found = [unpacked_lines(ref[x, first], ref[x, first + 1], ref[x, first + 2]) for ref in (mine, theirs)]
        vectors[2 * x], vectors[2 * x + 1] = by_core(place[1], *found)
    pad = jnp.zeros((u.shape[0] - count - extra, lane), F32)
    for t in range(width // lane):
        cols = slice(t * lane, (t + 1) * lane)

        def one(n, ref, i):
            normed = (ref[:, cols].astype(F32) - stats[n][0]) * stats[n][1]
            return normed * (1.0 + vectors[t, 2 + i : 3 + i, :]) + vectors[t, i : i + 1, :]

        u[:half, cols] = one(0, near, 0).astype(BF16)
        u[half:count, cols] = one(1, far, 0).astype(BF16)
        u[count:, cols] = jnp.concatenate([one(2, context, 1), pad], axis=0).astype(BF16)
    for s in range(down.shape[0] // (2 * lanes)):
        even, odd = by_core(place[1], mine[:, s].astype(F32), theirs[:, s].astype(F32))
        piece = jnp.stack([even, odd], axis=1).reshape(lanes, lanes)
        down[2 * s * lanes : (2 * s + 1) * lanes] = piece.astype(BF16)
        down[(2 * s + 1) * lanes : (2 * s + 2) * lanes] = pltpu.roll(piece, HEAD, 1).astype(BF16)


def inverse(mixing, row, col, upper):
    size = mixing[0].shape[0]
    eye = (row == col).astype(F32)
    width = 1
    found = None
    while width < size:
        here, there = (col, row) if upper else (row, col)
        shared = (row // (2 * width)) == (col // (2 * width))
        corner = shared & ((here // width) % 2 == 1) & ((there // width) % 2 == 0)
        parts = [jnp.where(corner, m, 0.0) for m in mixing]
        if found is None:
            found = [eye - p for p in parts]
        else:
            lefts = [dot(p, f) for p, f in zip(parts, found)]
            found = [f - dot(f, g) for f, g in zip(found, lefts)]
        width *= 2
    return found


def block_terms(k, v, low, fading, step, rates, spikes=None, q=None):
    count, lanes = k.shape
    row, col = iota((count, lanes), 0), iota((count, lanes), 1)
    heads = lanes // HEAD
    owns = [(col // HEAD) == h for h in range(heads)]

    squashed = jnp.tanh(low.astype(F32)).astype(BF16)
    feature = -rates * jax.nn.sigmoid(dot(squashed, fading))
    learned = jax.nn.sigmoid(dot(squashed, step) - RATE_SHIFT)
    key = k.astype(F32)
    norms = jnp.zeros_like(key)
    for own in owns:
        total = jnp.sum(jnp.where(own, key * key, 0.0), -1, keepdims=True)
        norms = jnp.where(own, lax.rsqrt(total + EPS_KEY), norms)
    unit = key * norms
    removal = unit * learned

    upto = (row >= col).astype(F32)

    def running(part):
        return lax.dot_general(
            upto, part, (((1,), (0,)), ((), ())), preferred_element_type=F32, precision=lax.Precision.HIGHEST
        )

    after = running(feature)
    before = after - feature
    grow, shrink = jnp.exp(after), jnp.exp(-after)
    grow_x, shrink_x = jnp.exp(before), jnp.exp(-before)
    end = after[count - 1 : count]
    if spikes is None:
        b_end = b_after = b_before = None
    else:
        across = jnp.zeros((lanes, count), F32)
        for h in range(heads):
            across = jnp.where(iota(across.shape, 0) // HEAD == h, -spikes[h : h + 1], across)
        jump = across.T
        b_after = running(jump)
        b_before = b_after - jump
        b_end = b_after[count - 1 : count]
        across_after, across_before = b_after.T, b_before.T

    def pair(h, upper, strict):
        inside = ((col > row) if strict else (col >= row)) if upper else ((col < row) if strict else (col <= row))
        if spikes is None:
            return inside.astype(F32)
        at = h * HEAD
        down_after, down_before = b_after[:, at : at + 1], b_before[:, at : at + 1]
        side_after, side_before = across_after[at : at + 1], across_before[at : at + 1]
        if upper:
            power = side_before - (down_after if strict else down_before)
        else:
            power = (down_before if strict else down_after) - side_after
        return jnp.where(inside, jnp.exp(jnp.where(inside, power, NEVER)), 0.0)

    def scaled(tensor, power):
        return tensor if spikes is None else tensor * jnp.exp(power)

    probes = (unit * grow_x, unit * shrink)
    removals = (removal * shrink, removal * grow_x)
    keys = (key * shrink, key * grow_x)
    asks = None if q is None else (q.astype(F32) * grow, q.astype(F32) * shrink_x)

    scores = []
    for d in range(2):
        right = jnp.concatenate([removals[d], keys[d]], axis=0)
        for own in owns:
            left = jnp.where(own, probes[d], 0.0)
            if q is not None:
                left = jnp.concatenate([left, jnp.where(own, asks[d], 0.0)], axis=0)
            scores.append(dot(left, right, ((1,), (1,))))
    chains = [(d, h) for d in range(2) for h in range(heads)]
    masks = {(d, h): pair(h, d == 1, True) for d, h in chains}
    mixing = {c: scores[n][:count, :count] * masks[c] for n, c in enumerate(chains)}
    seen = {c: dot(scores[n][:count, count:] * masks[c], v) for n, c in enumerate(chains)}
    solved = {}
    for d in range(2):
        found = inverse([mixing[d, h] for h in range(heads)], row, col, d == 1)
        for h in range(heads):
            solved[d, h] = found[h]

    whole = jnp.exp(end)
    starts = (
        scaled(probes[0], b_before),
        scaled(probes[1] * whole, None if spikes is None else b_end - b_after),
    )

    def gathered(parts):
        total = parts[0]
        for own, part in zip(owns[1:], parts[1:]):
            total = jnp.where(own, part, total)
        return total

    results = []
    for d in range(2):
        x, y = [], []
        for h in range(heads):
            both = dot(solved[d, h], jnp.concatenate([starts[d], seen[d, h]], axis=1))
            x.append(both[:, :lanes])
            y.append(both[:, lanes:])
        x, y = gathered(x), gathered(y)
        if d == 0:
            weigh = whole if spikes is None else whole * jnp.exp(b_end - b_after)
        else:
            weigh = jnp.ones_like(whole) if spikes is None else jnp.exp(b_before)
        last_keys, last_removals = keys[d] * weigh, removals[d] * weigh
        offset = dot(
            jnp.concatenate([v.astype(F32), -y], axis=0),
            jnp.concatenate([last_keys, last_removals], axis=0),
            ((0,), (0,)),
        )
        if q is None:
            results.append((None, offset, None, None))
            continue
        decay = whole if spikes is None else jnp.exp(end + b_end)
        factor = jnp.where(row == col, decay, 0.0) - dot(x, last_removals, ((0,), (0,)))
        if d == 0:
            query = scaled(asks[0], b_after)
        else:
            query = scaled(asks[1] * whole, None if spikes is None else b_end - b_before)
        wx, base = [], []
        for h in range(heads):
            n = chains.index((d, h))
            mask = pair(h, d == 1, False)
            reads = scores[n][count:] * jnp.concatenate([mask, mask], axis=1)
            both = dot(reads[:, :count], jnp.concatenate([x, y], axis=1))
            wx.append(both[:, :lanes])
            base.append(dot(reads[:, count:], v) - both[:, lanes:])
        results.append((factor, offset, query - gathered(wx), gathered(base)))
    return results


def same_head(shape):
    return (iota(shape, 0) // HEAD) == (iota(shape, 1) // HEAD)


def block_kernel(
    place, mine, theirs, near, far, context_, wq, wk, wv, fading_, step_, rates_, spikes_,
    sent, asked, base, vectors,
    context, held, fading, step, rates, spikes, u, down, moved_q, moved_k, moved_v, moved_low, sems,
):
    pairs = [(context_, context)]
    pairs += [(ref, held.at[n]) for n, ref in enumerate((wq, wk, wv))]
    pairs += [(fading_, fading), (step_, step), (rates_, rates), (spikes_, spikes)]
    copies = [pltpu.make_async_copy(ref, to, sems.at[n]) for n, (ref, to) in enumerate(pairs)]
    for copy in copies:
        copy.start()
    copies[0].wait()
    modulated(place, near, far, context, mine, theirs, u, vectors, down)
    for copy in copies[1:]:
        copy.wait()
    count, extra = asked.shape[1], context.shape[0]
    low = dot(u[...], down[...])
    low = jnp.where(iota(low.shape, 1) < HEAD, low, 0.0)
    k, v = dot(u[...], held[1]), dot(u[...], held[2])
    own = [
        placed_rows(part[:count], place[2], to).astype(BF16)
        for part, to in ((low, moved_low), (k, moved_k), (v, moved_v), (dot(u[:count], held[0]), moved_q))
    ]
    ahead, behind = block_terms(
        own[1], own[2], own[0][:, :HEAD], fading[...], step[...], rates[...], spikes[...], own[3]
    )
    same = same_head(ahead[0].shape)
    size = same.shape[0]
    for n, (factor, offset) in enumerate((ahead[:2], behind[:2])):
        sent[n * size : (n + 1) * size] = jnp.where(same, factor, pltpu.roll(offset, HEAD, 0)).astype(BF16)
    tail = [part[count : count + extra] for part in (k, v, low)]
    sent[2 * size :] = jnp.concatenate(tail + [jnp.zeros_like(tail[0])], axis=0).astype(BF16)
    asked[0], asked[1] = ahead[2].astype(BF16), behind[2].astype(BF16)
    base[...] = ahead[3] + behind[3]


def opened(packed, same):
    packed = packed.astype(F32)
    return jnp.where(same, packed, 0.0), jnp.where(same, pltpu.roll(packed, HEAD, 0), 0.0)


def pair_kernel(place, mine, other, out):
    pairs, _, size = out.shape
    odd = place[0] % 2
    same = same_head((size, size))
    early = jnp.where(odd == 0, mine[...].astype(F32), other[...].astype(F32))
    late = jnp.where(odd == 0, other[...].astype(F32), mine[...].astype(F32))
    both = []
    for first, second, at in ((early, late, 0), (late, early, size)):
        left, right = (opened(part[at : at + size], same) for part in (first, second))
        new = dot(jnp.concatenate(left, axis=0), right[0])
        both.append(jnp.where(same, new[:size], pltpu.roll(new[size:] + right[1], HEAD, 0)).astype(BF16))
    extra = (early.shape[0] - 2 * size) // 4
    tails = [[part[2 * size + n * extra : 2 * size + (n + 1) * extra] for part in (early, late)] for n in range(3)]
    low = tails[2][0] + pltpu.roll(tails[2][1], HEAD, 1)
    tail = jnp.concatenate(tails[0] + tails[1] + [low, jnp.zeros_like(low)], axis=0).astype(BF16)
    for j in range(pairs):
        out[j, :size] = jnp.where(place[0] // 2 < j, both[0], both[1])
        out[j, size:] = tail


def read_kernel(
    place, maps, other, asked, base, fading_, step_, rates_, gains_, emit_,
    keep, give,
    fading, step, rates, gains, emit, sems,
):
    pairs = [(fading_, fading), (step_, step), (rates_, rates), (gains_, gains), (emit_, emit)]
    copies = [pltpu.make_async_copy(ref, to, sems.at[n]) for n, (ref, to) in enumerate(pairs)]
    for copy in copies:
        copy.start()
    peers, _, size = maps.shape
    extra = keep.shape[1]
    same = same_head((size, size))
    me, core = place[0], place[1]
    mine = me // 2
    for copy in copies[:4]:
        copy.wait()
    wide = 2 * extra
    parts = [
        jnp.concatenate([maps[j, size + n * wide : size + (n + 1) * wide].astype(F32) for j in range(peers)], axis=0)
        for n in range(2)
    ]
    low = []
    for j in range(peers):
        packed = maps[j, size + 2 * wide : size + 2 * wide + extra].astype(F32)
        low += [packed, pltpu.roll(packed, HEAD, 1)]
    parts = [part.astype(BF16) for part in (*parts, jnp.concatenate(low, axis=0))]
    context = block_terms(parts[0], parts[1], parts[2][:, :HEAD], fading[...], step[...], rates[...])
    eye = (iota((size, size), 0) == iota((size, size), 1)).astype(F32)
    composed = [jnp.concatenate([eye, jnp.zeros_like(eye)], axis=0) for _ in range(2)]

    def follow(d, packed, reached):
        factor, offset = opened(packed, same)
        new = dot(composed[d], factor)
        new = jnp.concatenate([new[:size], new[size:] + offset], axis=0)
        composed[d] = jnp.where(reached, new, composed[d])

    for n in range(peers - 1):
        follow(0, maps[n, :size], n < mine)
        follow(1, maps[peers - 1 - n, :size], peers - 1 - n > mine)
    follow(0, other[:size], me % 2 == 1)
    follow(1, other[size : 2 * size], me % 2 == 0)
    out = base[...]
    for d in range(2):
        start = jnp.where(same, context[d][1], 0.0)
        state = dot(start, composed[d][:size]) + composed[d][size:]
        out = out + dot(asked[d], state, ((1,), (1,)))
    first = iota(out.shape, 1) < HEAD

    def mean(value):
        left = jnp.sum(jnp.where(first, value, 0.0), -1, keepdims=True)
        right = jnp.sum(jnp.where(first, 0.0, value), -1, keepdims=True)
        return jnp.where(first, left, right) * (1.0 / HEAD)

    out = out - mean(out)
    normed = out * lax.rsqrt(mean(out * out) + EPS_HEAD) * gains[...]
    chips, rows, _ = keep.shape
    split = normed.reshape(chips, 2, rows, size)
    even, odd = split[:, 0].reshape(chips * rows, size), split[:, 1].reshape(chips * rows, size)
    mine = jnp.where(core == 0, even, odd)
    other = jnp.where(core == 0, odd, even)
    left = jnp.concatenate([mine, other], axis=0).astype(BF16)
    copies[4].wait()
    lane = emit.shape[2]
    for s in range(emit.shape[0]):
        part = dot(left, emit[s]).reshape(2, chips, rows, lane).astype(BF16)
        keep[:, :, s * lane : (s + 1) * lane] = part[0]
        give[:, :, s * lane : (s + 1) * lane] = part[1]


def last_kernel(parts, hidden, vectors, out):
    lane = vectors.shape[2]
    for t in range(vectors.shape[0]):
        cols = slice(t * lane, (t + 1) * lane)
        total = parts[0, :, cols].astype(F32)
        for n in range(1, parts.shape[0]):
            total = total + parts[n, :, cols].astype(F32)
        out[:, cols] = (hidden[:, cols].astype(F32) + vectors[t, 4:5, :] * total).astype(BF16)


def exchange(blocks, axis, groups=None):
    return lax.all_to_all(blocks, axis, 0, 0, tiled=True, axis_index_groups=groups)


def swapped(value, axis, bit):
    return lax.ppermute(value, axis, [(i, i ^ bit) for i in range(lax.axis_size(axis))])


def shards(
    hidden_items,
    sample_cond,
    prompt_items,
    prompt_cond,
    adjust_shifting,
    adjust_stretch,
    skip_valve,
    receiver_matrix,
    address_matrix,
    payload_matrix,
    joint_lower_projector,
    fading_raise_matrix,
    step_raise_matrix,
    feature_fading,
    spike_logfade,
    group_standard_factor,
    emit_matrix,
):
    n_sp, n_tp = lax.axis_size("sp"), lax.axis_size("tp")
    me, tp = lax.axis_index("sp"), lax.axis_index("tp")
    rows, width = hidden_items.shape
    extra = prompt_items.shape[0]
    count = rows * n_tp
    lanes = receiver_matrix.shape[1]
    span, chunk = adjust_shifting.shape
    chips = n_tp // 2
    same_core = [[2 * i + c for i in range(chips)] for c in range(2)]
    place = jnp.stack([me, tp % 2, tp]).astype(jnp.int32)

    parts = call(
        partials_kernel,
        ((n_sp, 4, 8, lanes), BF16),
        place,
        sample_cond.reshape(-1, lanes),
        prompt_cond.reshape(-1, lanes),
        joint_lower_projector.T,
        adjust_shifting,
        adjust_stretch,
        skip_valve,
        scalars=1,
        fetched=6,
        room=ALL,
        flops=8 * span * chunk * 6,
        scratch=[
            pltpu.VMEM((2, width // lanes, lanes), BF16),
            pltpu.VMEM(joint_lower_projector.shape[::-1], BF16),
            pltpu.VMEM((3, span, chunk), BF16),
            pltpu.SemaphoreType.DMA((6,)),
        ],
    )
    emit = lax.all_gather(emit_matrix, "sp", axis=0)
    parts = exchange(parts, "sp")

    near, bit = hidden_items[None], n_tp // 2
    while bit > 1:
        far = swapped(near, "tp", bit)
        near = jnp.concatenate([near, far], axis=0)
        bit //= 2
    far = swapped(near, "tp", 1)

    mine = call(sum_kernel, ((chips, n_sp + 3, 8, lanes), BF16), parts)
    mine = exchange(mine, "tp", same_core)
    theirs = swapped(mine, "tp", 1)

    padded = count + -(-extra // 16) * 16
    rates = feature_fading.reshape(1, lanes)
    small = [
        pltpu.VMEM(fading_raise_matrix.shape, BF16),
        pltpu.VMEM(step_raise_matrix.shape, BF16),
        pltpu.VMEM(rates.shape, F32),
    ]
    sent, asked, base, vectors = call(
        block_kernel,
        [
            ((2 * lanes + 4 * extra, lanes), BF16),
            ((2, count, lanes), BF16),
            ((count, lanes), F32),
            ((n_tp, 8, chunk), F32),
        ],
        place,
        mine,
        theirs,
        near.reshape(count // 2, width),
        far.reshape(count // 2, width),
        prompt_items,
        receiver_matrix,
        address_matrix,
        payload_matrix,
        fading_raise_matrix,
        step_raise_matrix,
        rates,
        spike_logfade.T,
        scalars=1,
        fetched=8,
        room=ALL,
        flops=2 * padded * width * lanes * 4,
        scratch=[
            pltpu.VMEM((extra, width), BF16),
            pltpu.VMEM((3, width, lanes), BF16),
            *small,
            pltpu.VMEM(spike_logfade.shape[::-1], F32),
            pltpu.VMEM((padded, width), BF16),
            pltpu.VMEM((width, lanes), BF16),
            *[pltpu.VMEM((n_tp, rows, lanes), F32)] * 4,
            pltpu.SemaphoreType.DMA((8,)),
        ],
    )
    other = swapped(sent, "sp", 1)
    sent = call(
        pair_kernel,
        ((n_sp // 2, lanes + 6 * extra, lanes), BF16),
        place,
        sent,
        other,
        scalars=1,
        flops=2 * 128**3 * 8,
    )
    maps = exchange(sent, "sp", [[2 * i + c for i in range(n_sp // 2)] for c in range(2)])
    keep, give = call(
        read_kernel,
        [((chips, rows, width), BF16)] * 2,
        place,
        maps,
        other,
        asked,
        base,
        fading_raise_matrix,
        step_raise_matrix,
        rates,
        group_standard_factor.reshape(1, lanes),
        emit,
        scalars=1,
        fetched=5,
        room=ALL,
        flops=2 * count * lanes * width,
        scratch=[
            *small,
            pltpu.VMEM((1, lanes), F32),
            pltpu.VMEM((n_sp, *emit_matrix.shape), BF16),
            pltpu.SemaphoreType.DMA((5,)),
        ],
    )
    given = swapped(give, "tp", 1)
    both = (keep.astype(F32) + given.astype(F32)).astype(BF16)
    final = exchange(both, "tp", same_core)
    return call(last_kernel, ((rows, width), BF16), final, hidden_items, vectors)


def solution(mesh):
    placed = (
        P(("grp", "sp", "tp"), None),
        P("grp"),
        P(("grp", "sp"), None),
        P(),
        P("sp", "tp"),
        P("sp", "tp"),
        P("sp", "tp"),
        P(None, "tp"),
        P(None, "tp"),
        P(None, "tp"),
        P("sp", None),
        P(None, "tp"),
        P(None, "tp"),
        P("tp"),
        P(("grp", "sp"), "tp"),
        P("tp"),
        P("tp", "sp"),
    )

    return jax.shard_map(shards, mesh=mesh, in_specs=placed, out_specs=P(("grp", "sp", "tp"), None), check_vma=False)
```

```python
import jax
import jax.numpy as jnp
from jax import lax
from jax.experimental import pallas as pl
from jax.experimental.pallas import tpu as pltpu
from jax.sharding import PartitionSpec as P


HEAD = 64
EPS_ROW = 1e-05
EPS_HEAD = 0.00064
EPS_KEY = 1e-06
RATE_SHIFT = 5.0
NEVER = -1e30
SOME, MOST, ALL, READ = 24 * 1024 * 1024, 52 * 1024 * 1024, 63 * 1024 * 1024, 52 * 1024 * 1024
BF16, F32 = jnp.bfloat16, jnp.float32

VMEM = pl.BlockSpec(memory_space=pltpu.VMEM)
SMEM = pl.BlockSpec(memory_space=pltpu.SMEM)
HBM = pl.BlockSpec(memory_space=pltpu.HBM)


def call(body, outs, *args, flops=0, scalars=0, scratch=(), fetched=0, room=SOME):
    many = isinstance(outs, list)
    shapes = [jax.ShapeDtypeStruct(s, d) for s, d in (outs if many else [outs])]
    got = pl.pallas_call(
        body,
        out_shape=shapes,
        in_specs=[SMEM] * scalars + [VMEM] * (len(args) - scalars - fetched) + [HBM] * fetched,
        out_specs=[VMEM] * len(shapes),
        scratch_shapes=list(scratch),
        compiler_params=pltpu.CompilerParams(vmem_limit_bytes=room),
        cost_estimate=pl.CostEstimate(
            flops=flops, transcendentals=0, bytes_accessed=sum(a.size * a.dtype.itemsize for a in args)
        ),
    )(*args)
    return got if many else got[0]


def dot(left, right, dims=((1,), (0,))):
    return lax.dot_general(
        left.astype(BF16), right.astype(BF16), (dims, ((), ())), preferred_element_type=F32
    )


def iota(shape, dim):
    return lax.broadcasted_iota(jnp.int32, shape, dim)


USED = 5


def packed_lines(total, lanes):
    high = total.astype(BF16).astype(F32)
    rest = total - high
    row = iota((total.shape[0], lanes), 0)
    last = rest[:, lanes:]
    free = total.shape[0] - USED
    return [
        jnp.where(row < USED, high[:, :lanes], pltpu.roll(last, USED, 0)).astype(BF16),
        jnp.where(row < USED, high[:, lanes:], pltpu.roll(last, USED - free, 0)).astype(BF16),
        rest[:, :lanes].astype(BF16),
    ]


def unpacked_lines(first, second, third):
    first, second, third = (part.astype(F32) for part in (first, second, third))
    count = first.shape[0]
    row = iota(first.shape, 0)
    free = count - USED
    last = jnp.where(row < free, pltpu.roll(first, count - USED, 0), pltpu.roll(second, count - USED + free, 0))
    return jnp.concatenate([first + third, second + last], axis=1)


def partials_kernel(place, sample, prompt, lower, shifting, stretch, valve, out, conds, low_rows, held, sems):
    pairs = [(sample, conds.at[0]), (prompt, conds.at[1]), (lower, low_rows)]
    pairs += [(ref, held.at[n]) for n, ref in enumerate((shifting, stretch, valve))]
    copies = [pltpu.make_async_copy(ref, to, sems.at[n]) for n, (ref, to) in enumerate(pairs)]
    for copy in copies:
        copy.start()
    for copy in copies[:3]:
        copy.wait()
    peers, _, rows, _ = out.shape
    chunk = held.shape[2]
    wide = chunk // sample.shape[1]
    line = iota(sample.shape, 0)

    def own(n):
        full = conds[n].astype(F32)
        cut = [
            jnp.sum(jnp.where(line == place[0] * wide + n, full, 0.0), axis=0, keepdims=True) for n in range(wide)
        ]
        return jax.nn.silu(jnp.concatenate(cut, axis=1))

    row = iota((rows, chunk), 0)
    first, second = own(0), own(1)

    def at(k, both):
        left = jnp.where(row == k, first, 0.0)
        return jnp.where(row == k + 1, second, left) if both else left

    upright = low_rows[...].astype(F32).T
    count = upright.shape[0] // rows
    blocks = upright.reshape(count, rows, upright.shape[1])
    number = iota(blocks.shape, 0)
    halves = [
        jnp.sum(jnp.where(number == place[2] + n * (count // 2), blocks, 0.0), axis=0) for n in range(2)
    ]
    piece = jnp.concatenate(halves, axis=1)
    for copy in copies[3:]:
        copy.wait()
    total = dot(at(0, True), held[0]) + dot(at(2, True), held[1]) + dot(at(4, False), held[2])
    for n, block in enumerate(packed_lines(total, out.shape[3]) + [piece.astype(BF16)]):
        for p in range(peers):
            out[p, n] = block


def sum_kernel(parts, out):
    lanes = out.shape[3]
    total = unpacked_lines(parts[0, 0], parts[0, 1], parts[0, 2])
    for k in range(1, parts.shape[0]):
        total = total + unpacked_lines(parts[k, 0], parts[k, 1], parts[k, 2])
    blocks = [parts[k, 3] for k in range(parts.shape[0])] + packed_lines(total, lanes)
    for p in range(out.shape[0]):
        for n, block in enumerate(blocks):
            out[p, n] = block


def by_core(core, own, other):
    return jnp.where(core == 0, own, other), jnp.where(core == 0, other, own)


STEPS = (0, -2, 2, 4, -1, -3, 1, 3)


def placed_rows(value, tp, held):
    count, rows, lanes = held.shape
    for n in range(count):
        core = tp % 2 if n < len(STEPS) else 1 - tp % 2
        chip = (tp // 2 + STEPS[n % len(STEPS)] + count // 2) % (count // 2)
        held[2 * chip + core] = value[n * rows : (n + 1) * rows]
    return held[...].reshape(count * rows, lanes)


def moments(ref, lane):
    width = ref.shape[1]
    total = jnp.zeros((ref.shape[0], lane), F32)
    for c in range(0, width, lane):
        total = total + ref[:, c : c + lane].astype(F32)
    centre = jnp.sum(total, -1, keepdims=True) * (1.0 / width)
    total = jnp.zeros((ref.shape[0], lane), F32)
    for c in range(0, width, lane):
        off = ref[:, c : c + lane].astype(F32) - centre
        total = total + off * off
    spread = jnp.sum(total, -1, keepdims=True) * (1.0 / width)
    return centre, lax.rsqrt(spread + EPS_ROW)


def modulated(place, near, far, context, mine, theirs, u, vectors, down):
    half, width = near.shape
    count, extra = 2 * half, context.shape[0]
    lane, lanes = vectors.shape[2], mine.shape[3]
    stats = [moments(ref, lane) for ref in (near, far, context)]
    first = mine.shape[1] - 3
    for x in range(mine.shape[0]):
        found = [unpacked_lines(ref[x, first], ref[x, first + 1], ref[x, first + 2]) for ref in (mine, theirs)]
        vectors[2 * x], vectors[2 * x + 1] = by_core(place[1], *found)
    pad = jnp.zeros((u.shape[0] - count - extra, lane), F32)
    for t in range(width // lane):
        cols = slice(t * lane, (t + 1) * lane)

        def one(n, ref, i):
            normed = (ref[:, cols].astype(F32) - stats[n][0]) * stats[n][1]
            return normed * (1.0 + vectors[t, 2 + i : 3 + i, :]) + vectors[t, i : i + 1, :]

        u[:half, cols] = one(0, near, 0).astype(BF16)
        u[half:count, cols] = one(1, far, 0).astype(BF16)
        u[count:, cols] = jnp.concatenate([one(2, context, 1), pad], axis=0).astype(BF16)
    for s in range(down.shape[0] // (2 * lanes)):
        even, odd = by_core(place[1], mine[:, s].astype(F32), theirs[:, s].astype(F32))
        piece = jnp.stack([even, odd], axis=1).reshape(lanes, lanes)
        down[2 * s * lanes : (2 * s + 1) * lanes] = piece.astype(BF16)
        down[(2 * s + 1) * lanes : (2 * s + 2) * lanes] = pltpu.roll(piece, HEAD, 1).astype(BF16)


def inverse(mixing, row, col):
    size = row.shape[0]
    eye = (row == col).astype(F32)
    width = 1
    found = None
    while width < size:
        shared = (row // (2 * width)) == (col // (2 * width))
        low_row, low_col = (row // width) % 2 == 1, (col // width) % 2 == 1
        corner = {False: shared & low_row & ~low_col, True: shared & low_col & ~low_row}
        parts = [jnp.where(corner[upper], m, 0.0) for m, upper in mixing]
        if found is None:
            found = [eye - p for p in parts]
        else:
            lefts = [dot(p, f) for p, f in zip(parts, found)]
            found = [f - dot(f, g) for f, g in zip(found, lefts)]
        width *= 2
    return found


def block_terms(k, v, low, fading, step, rates, spikes=None, q=None):
    count, lanes = k.shape
    row, col = iota((count, lanes), 0), iota((count, lanes), 1)
    heads = lanes // HEAD
    owns = [(col // HEAD) == h for h in range(heads)]

    squashed = jnp.tanh(low.astype(F32)).astype(BF16)
    feature = -rates * jax.nn.sigmoid(dot(squashed, fading))
    learned = jax.nn.sigmoid(dot(squashed, step) - RATE_SHIFT)
    key = k.astype(F32)
    norms = jnp.zeros_like(key)
    for own in owns:
        total = jnp.sum(jnp.where(own, key * key, 0.0), -1, keepdims=True)
        norms = jnp.where(own, lax.rsqrt(total + EPS_KEY), norms)
    unit = key * norms
    removal = unit * learned

    upto = (row >= col).astype(F32)

    def running(part):
        return lax.dot_general(
            upto, part, (((1,), (0,)), ((), ())), preferred_element_type=F32, precision=lax.Precision.HIGHEST
        )

    after = running(feature)
    before = after - feature
    grow, shrink = jnp.exp(after), jnp.exp(-after)
    grow_x, shrink_x = jnp.exp(before), jnp.exp(-before)
    end = after[count - 1 : count]
    if spikes is None:
        b_end = b_after = b_before = None
    else:
        across = jnp.zeros((lanes, count), F32)
        for h in range(heads):
            across = jnp.where(iota(across.shape, 0) // HEAD == h, -spikes[h : h + 1], across)
        jump = across.T
        b_after = running(jump)
        b_before = b_after - jump
        b_end = b_after[count - 1 : count]
        across_after, across_before = b_after.T, b_before.T

    def pair(h, upper, strict):
        inside = ((col > row) if strict else (col >= row)) if upper else ((col < row) if strict else (col <= row))
        if spikes is None:
            return inside.astype(F32)
        at = h * HEAD
        down_after, down_before = b_after[:, at : at + 1], b_before[:, at : at + 1]
        side_after, side_before = across_after[at : at + 1], across_before[at : at + 1]
        if upper:
            power = side_before - (down_after if strict else down_before)
        else:
            power = (down_before if strict else down_after) - side_after
        return jnp.where(inside, jnp.exp(jnp.where(inside, power, NEVER)), 0.0)

    def scaled(tensor, power):
        return tensor if spikes is None else tensor * jnp.exp(power)

    probes = (unit * grow_x, unit * shrink)
    removals = (removal * shrink, removal * grow_x)
    keys = (key * shrink, key * grow_x)
    asks = None if q is None else (q.astype(F32) * grow, q.astype(F32) * shrink_x)

    scores = []
    for d in range(2):
        right = jnp.concatenate([removals[d], keys[d]], axis=0)
        for own in owns:
            left = jnp.where(own, probes[d], 0.0)
            if q is not None:
                left = jnp.concatenate([left, jnp.where(own, asks[d], 0.0)], axis=0)
            scores.append(dot(left, right, ((1,), (1,))))
    chains = [(d, h) for d in range(2) for h in range(heads)]
    masks = {(d, h): pair(h, d == 1, True) for d, h in chains}
    mixing = {c: scores[n][:count, :count] * masks[c] for n, c in enumerate(chains)}
    seen = {c: dot(scores[n][:count, count:] * masks[c], v) for n, c in enumerate(chains)}
    solved = dict(zip(chains, inverse([(mixing[c], c[0] == 1) for c in chains], row, col)))

    whole = jnp.exp(end)
    starts = (
        scaled(probes[0], b_before),
        scaled(probes[1] * whole, None if spikes is None else b_end - b_after),
    )

    def gathered(parts):
        total = parts[0]
        for own, part in zip(owns[1:], parts[1:]):
            total = jnp.where(own, part, total)
        return total

    results = []
    for d in range(2):
        x, y = [], []
        for h in range(heads):
            both = dot(solved[d, h], jnp.concatenate([starts[d], seen[d, h]], axis=1))
            x.append(both[:, :lanes])
            y.append(both[:, lanes:])
        x, y = gathered(x), gathered(y)
        if d == 0:
            weigh = whole if spikes is None else whole * jnp.exp(b_end - b_after)
        else:
            weigh = jnp.ones_like(whole) if spikes is None else jnp.exp(b_before)
        last_keys, last_removals = keys[d] * weigh, removals[d] * weigh
        offset = dot(
            jnp.concatenate([v.astype(F32), -y], axis=0),
            jnp.concatenate([last_keys, last_removals], axis=0),
            ((0,), (0,)),
        )
        if q is None:
            results.append((None, offset, None, None))
            continue
        decay = whole if spikes is None else jnp.exp(end + b_end)
        factor = jnp.where(row == col, decay, 0.0) - dot(x, last_removals, ((0,), (0,)))
        if d == 0:
            query = scaled(asks[0], b_after)
        else:
            query = scaled(asks[1] * whole, None if spikes is None else b_end - b_before)
        wx, base = [], []
        for h in range(heads):
            n = chains.index((d, h))
            mask = pair(h, d == 1, False)
            reads = scores[n][count:] * jnp.concatenate([mask, mask], axis=1)
            both = dot(reads[:, :count], jnp.concatenate([x, y], axis=1))
            wx.append(both[:, :lanes])
            base.append(dot(reads[:, count:], v) - both[:, lanes:])
        results.append((factor, offset, query - gathered(wx), gathered(base)))
    return results


def same_head(shape):
    return (iota(shape, 0) // HEAD) == (iota(shape, 1) // HEAD)


def block_kernel(
    place, mine, theirs, near, far, context_, wq, wk, wv, fading_, step_, rates_, spikes_,
    sent, asked, base, vectors,
    context, held, fading, step, rates, spikes, u, down, moved_q, moved_k, moved_v, moved_low, sems,
):
    pairs = [(context_, context)]
    pairs += [(ref, held.at[n]) for n, ref in enumerate((wq, wk, wv))]
    pairs += [(fading_, fading), (step_, step), (rates_, rates), (spikes_, spikes)]
    copies = [pltpu.make_async_copy(ref, to, sems.at[n]) for n, (ref, to) in enumerate(pairs)]
    for copy in copies:
        copy.start()
    copies[0].wait()
    modulated(place, near, far, context, mine, theirs, u, vectors, down)
    for copy in copies[1:]:
        copy.wait()
    wq, wk, wv = (held.at[n] for n in range(3))
    count, extra = asked.shape[1], context.shape[0]
    low = dot(u[...], down[...])
    low = jnp.where(iota(low.shape, 1) < HEAD, low, 0.0)
    k, v = dot(u[...], wk[...]), dot(u[...], wv[...])
    own = [
        placed_rows(part[:count], place[2], to).astype(BF16)
        for part, to in ((low, moved_low), (k, moved_k), (v, moved_v), (dot(u[:count], wq[...]), moved_q))
    ]
    ahead, behind = block_terms(
        own[1], own[2], own[0][:, :HEAD], fading[...], step[...], rates[...], spikes[...], own[3]
    )
    same = same_head(ahead[0].shape)
    size = same.shape[0]
    packed = [
        jnp.where(same, factor, pltpu.roll(offset, HEAD, 0)).astype(BF16)
        for factor, offset in (ahead[:2], behind[:2])
    ]
    tail = [part[count : count + extra] for part in (k, v, low)]
    tail = jnp.concatenate(tail + [jnp.zeros_like(tail[0])], axis=0).astype(BF16)
    for j in range(sent.shape[0]):
        sent[j, :size] = jnp.where(place[0] < j, packed[0], packed[1])
        sent[j, size:] = tail
    asked[0], asked[1] = ahead[2].astype(BF16), behind[2].astype(BF16)
    base[...] = ahead[3] + behind[3]


def opened(packed, same):
    packed = packed.astype(F32)
    return jnp.where(same, packed, 0.0), jnp.where(same, pltpu.roll(packed, HEAD, 0), 0.0)


def read_kernel(
    place, maps, asked, base, fading_, step_, rates_, gains_, emit_,
    keep, give,
    fading, step, rates, gains, emit, sems,
):
    pairs = [(fading_, fading), (step_, step), (rates_, rates), (gains_, gains), (emit_, emit)]
    copies = [pltpu.make_async_copy(ref, to, sems.at[n]) for n, (ref, to) in enumerate(pairs)]
    for copy in copies:
        copy.start()
    for copy in copies[:4]:
        copy.wait()
    peers, _, size = maps.shape
    extra = keep.shape[1]
    same = same_head((size, size))
    me, core = place[0], place[1]
    parts = [
        jnp.concatenate([maps[j, size + n * extra : size + (n + 1) * extra].astype(F32) for j in range(peers)], axis=0)
        for n in range(3)
    ]
    parts = [part.astype(BF16) for part in parts]
    context = block_terms(parts[0], parts[1], parts[2][:, :HEAD], fading[...], step[...], rates[...])
    eye = (iota((size, size), 0) == iota((size, size), 1)).astype(F32)
    composed = [jnp.concatenate([eye, jnp.zeros_like(eye)], axis=0) for _ in range(2)]
    for n in range(peers - 1):
        for d, j, reached in ((0, n, n < me), (1, peers - 1 - n, peers - 1 - n > me)):
            factor, offset = opened(maps[j, :size], same)
            new = dot(composed[d], factor)
            new = jnp.concatenate([new[:size], new[size:] + offset], axis=0)
            composed[d] = jnp.where(reached, new, composed[d])
    out = base[...]
    for d in range(2):
        start = jnp.where(same, context[d][1], 0.0)
        state = dot(start, composed[d][:size]) + composed[d][size:]
        out = out + dot(asked[d], state, ((1,), (1,)))
    first = iota(out.shape, 1) < HEAD

    def mean(value):
        left = jnp.sum(jnp.where(first, value, 0.0), -1, keepdims=True)
        right = jnp.sum(jnp.where(first, 0.0, value), -1, keepdims=True)
        return jnp.where(first, left, right) * (1.0 / HEAD)

    out = out - mean(out)
    normed = out * lax.rsqrt(mean(out * out) + EPS_HEAD) * gains[...]
    chips, rows, _ = keep.shape
    split = normed.reshape(chips, 2, rows, size)
    even, odd = split[:, 0].reshape(chips * rows, size), split[:, 1].reshape(chips * rows, size)
    mine = jnp.where(core == 0, even, odd)
    other = jnp.where(core == 0, odd, even)
    left = jnp.concatenate([mine, other], axis=0).astype(BF16)
    copies[4].wait()
    lane = emit.shape[2]
    for s in range(emit.shape[0]):
        part = dot(left, emit[s]).reshape(2, chips, rows, lane).astype(BF16)
        keep[:, :, s * lane : (s + 1) * lane] = part[0]
        give[:, :, s * lane : (s + 1) * lane] = part[1]


def last_kernel(parts, hidden, vectors, out):
    lane = vectors.shape[2]
    for t in range(vectors.shape[0]):
        cols = slice(t * lane, (t + 1) * lane)
        total = parts[0, :, cols].astype(F32)
        for n in range(1, parts.shape[0]):
            total = total + parts[n, :, cols].astype(F32)
        out[:, cols] = (hidden[:, cols].astype(F32) + vectors[t, 4:5, :] * total).astype(BF16)


def exchange(blocks, axis, groups=None):
    return lax.all_to_all(blocks, axis, 0, 0, tiled=True, axis_index_groups=groups)


def swapped(value, axis, bit):
    return lax.ppermute(value, axis, [(i, i ^ bit) for i in range(lax.axis_size(axis))])


def shards(
    hidden_items,
    sample_cond,
    prompt_items,
    prompt_cond,
    adjust_shifting,
    adjust_stretch,
    skip_valve,
    receiver_matrix,
    address_matrix,
    payload_matrix,
    joint_lower_projector,
    fading_raise_matrix,
    step_raise_matrix,
    feature_fading,
    spike_logfade,
    group_standard_factor,
    emit_matrix,
):
    n_sp, n_tp = lax.axis_size("sp"), lax.axis_size("tp")
    me, tp = lax.axis_index("sp"), lax.axis_index("tp")
    rows, width = hidden_items.shape
    extra = prompt_items.shape[0]
    count = rows * n_tp
    lanes = receiver_matrix.shape[1]
    span, chunk = adjust_shifting.shape
    chips = n_tp // 2
    same_core = [[2 * i + c for i in range(chips)] for c in range(2)]
    place = jnp.stack([me, tp % 2, tp]).astype(jnp.int32)

    parts = call(
        partials_kernel,
        ((n_sp, 4, 8, lanes), BF16),
        place,
        sample_cond.reshape(-1, lanes),
        prompt_cond.reshape(-1, lanes),
        joint_lower_projector.T,
        adjust_shifting,
        adjust_stretch,
        skip_valve,
        scalars=1,
        fetched=6,
        room=ALL,
        flops=8 * span * chunk * 6,
        scratch=[
            pltpu.VMEM((2, width // lanes, lanes), BF16),
            pltpu.VMEM(joint_lower_projector.shape[::-1], BF16),
            pltpu.VMEM((3, span, chunk), BF16),
            pltpu.SemaphoreType.DMA((6,)),
        ],
    )
    emit = lax.all_gather(emit_matrix, "sp", axis=0)
    parts = exchange(parts, "sp")

    def shifted(value, chips_on):
        return lax.ppermute(value, "tp", [(i, (i + 2 * chips_on) % n_tp) for i in range(n_tp)])

    below = shifted(hidden_items, 2)
    above = shifted(hidden_items, -2)
    across = shifted(hidden_items, 4)
    odd_below = shifted(jnp.stack([hidden_items, below]), 1)
    odd_above = shifted(jnp.stack([hidden_items, above]), -1)
    near = jnp.concatenate([jnp.stack([hidden_items, below, above, across]), odd_below, odd_above], axis=0)
    far = swapped(near, "tp", 1)

    mine = call(sum_kernel, ((chips, n_sp + 3, 8, lanes), BF16), parts)
    mine = exchange(mine, "tp", same_core)
    theirs = swapped(mine, "tp", 1)

    padded = count + -(-extra // 16) * 16
    rates = feature_fading.reshape(1, lanes)
    sent, asked, base, vectors = call(
        block_kernel,
        [
            ((n_sp, lanes + 4 * extra, lanes), BF16),
            ((2, count, lanes), BF16),
            ((count, lanes), F32),
            ((n_tp, 8, chunk), F32),
        ],
        place,
        mine,
        theirs,
        near.reshape(count // 2, width),
        far.reshape(count // 2, width),
        prompt_items,
        receiver_matrix,
        address_matrix,
        payload_matrix,
        fading_raise_matrix,
        step_raise_matrix,
        rates,
        spike_logfade.T,
        scalars=1,
        fetched=8,
        room=MOST,
        flops=2 * padded * width * lanes * 4,
        scratch=[
            pltpu.VMEM((extra, width), BF16),
            pltpu.VMEM((3, width, lanes), BF16),
            pltpu.VMEM(fading_raise_matrix.shape, BF16),
            pltpu.VMEM(step_raise_matrix.shape, BF16),
            pltpu.VMEM(rates.shape, F32),
            pltpu.VMEM(spike_logfade.shape[::-1], F32),
            pltpu.VMEM((padded, width), BF16),
            pltpu.VMEM((width, lanes), BF16),
            *[pltpu.VMEM((n_tp, rows, lanes), F32)] * 4,
            pltpu.SemaphoreType.DMA((8,)),
        ],
    )
    maps = exchange(sent, "sp")
    keep, give = call(
        read_kernel,
        [((chips, rows, width), BF16)] * 2,
        place,
        maps,
        asked,
        base,
        fading_raise_matrix,
        step_raise_matrix,
        rates,
        group_standard_factor.reshape(1, lanes),
        emit,
        scalars=1,
        fetched=5,
        room=READ,
        flops=2 * count * lanes * width,
        scratch=[
            pltpu.VMEM(fading_raise_matrix.shape, BF16),
            pltpu.VMEM(step_raise_matrix.shape, BF16),
            pltpu.VMEM(rates.shape, F32),
            pltpu.VMEM((1, lanes), F32),
            pltpu.VMEM((n_sp, *emit_matrix.shape), BF16),
            pltpu.SemaphoreType.DMA((5,)),
        ],
    )
    given = swapped(give, "tp", 1)
    both = (keep.astype(F32) + given.astype(F32)).astype(BF16)
    final = exchange(both, "tp", same_core)
    return call(last_kernel, ((rows, width), BF16), final, hidden_items, vectors)


def solution(mesh):
    placed = (
        P(("grp", "sp", "tp"), None),
        P("grp"),
        P(("grp", "sp"), None),
        P(),
        P("sp", "tp"),
        P("sp", "tp"),
        P("sp", "tp"),
        P(None, "tp"),
        P(None, "tp"),
        P(None, "tp"),
        P("sp", None),
        P(None, "tp"),
        P(None, "tp"),
        P("tp"),
        P(("grp", "sp"), "tp"),
        P("tp"),
        P("tp", "sp"),
    )

    return jax.shard_map(shards, mesh=mesh, in_specs=placed, out_specs=P(("grp", "sp", "tp"), None), check_vma=False)
```

```python
import jax
import jax.numpy as jnp
from jax import lax
from jax.experimental import pallas as pl
from jax.experimental.pallas import tpu as pltpu
from jax.sharding import PartitionSpec as P


HEAD = 64
EPS_ROW = 1e-05
EPS_HEAD = 0.00064
EPS_KEY = 1e-06
RATE_SHIFT = 5.0
NEVER = -1e30
SOME, MOST, ALL, READ = 24 * 1024 * 1024, 52 * 1024 * 1024, 63 * 1024 * 1024, 52 * 1024 * 1024
BF16, F32 = jnp.bfloat16, jnp.float32

VMEM = pl.BlockSpec(memory_space=pltpu.VMEM)
SMEM = pl.BlockSpec(memory_space=pltpu.SMEM)
HBM = pl.BlockSpec(memory_space=pltpu.HBM)


def call(body, outs, *args, flops=0, scalars=0, scratch=(), fetched=0, room=SOME):
    many = isinstance(outs, list)
    shapes = [jax.ShapeDtypeStruct(s, d) for s, d in (outs if many else [outs])]
    got = pl.pallas_call(
        body,
        out_shape=shapes,
        in_specs=[SMEM] * scalars + [VMEM] * (len(args) - scalars - fetched) + [HBM] * fetched,
        out_specs=[VMEM] * len(shapes),
        scratch_shapes=list(scratch),
        compiler_params=pltpu.CompilerParams(vmem_limit_bytes=room),
        cost_estimate=pl.CostEstimate(
            flops=flops, transcendentals=0, bytes_accessed=sum(a.size * a.dtype.itemsize for a in args)
        ),
    )(*args)
    return got if many else got[0]


def dot(left, right, dims=((1,), (0,))):
    return lax.dot_general(
        left.astype(BF16), right.astype(BF16), (dims, ((), ())), preferred_element_type=F32
    )


def iota(shape, dim):
    return lax.broadcasted_iota(jnp.int32, shape, dim)


USED = 5


def packed_lines(total, lanes):
    high = total.astype(BF16).astype(F32)
    rest = total - high
    row = iota((total.shape[0], lanes), 0)
    last = rest[:, lanes:]
    free = total.shape[0] - USED
    return [
        jnp.where(row < USED, high[:, :lanes], pltpu.roll(last, USED, 0)).astype(BF16),
        jnp.where(row < USED, high[:, lanes:], pltpu.roll(last, USED - free, 0)).astype(BF16),
        rest[:, :lanes].astype(BF16),
    ]


def unpacked_lines(first, second, third):
    first, second, third = (part.astype(F32) for part in (first, second, third))
    count = first.shape[0]
    row = iota(first.shape, 0)
    free = count - USED
    last = jnp.where(row < free, pltpu.roll(first, count - USED, 0), pltpu.roll(second, count - USED + free, 0))
    return jnp.concatenate([first + third, second + last], axis=1)


def partials_kernel(place, sample, prompt, lower, shifting, stretch, valve, out, conds, low_rows, held, sems):
    pairs = [(sample, conds.at[0]), (prompt, conds.at[1]), (lower, low_rows)]
    pairs += [(ref, held.at[n]) for n, ref in enumerate((shifting, stretch, valve))]
    copies = [pltpu.make_async_copy(ref, to, sems.at[n]) for n, (ref, to) in enumerate(pairs)]
    for copy in copies:
        copy.start()
    for copy in copies[:3]:
        copy.wait()
    peers, _, rows, _ = out.shape
    chunk = held.shape[2]
    wide = chunk // sample.shape[1]
    line = iota(sample.shape, 0)

    def own(n):
        full = conds[n].astype(F32)
        cut = [
            jnp.sum(jnp.where(line == place[0] * wide + n, full, 0.0), axis=0, keepdims=True) for n in range(wide)
        ]
        return jax.nn.silu(jnp.concatenate(cut, axis=1))

    row = iota((rows, chunk), 0)
    first, second = own(0), own(1)

    def at(k, both):
        left = jnp.where(row == k, first, 0.0)
        return jnp.where(row == k + 1, second, left) if both else left

    upright = low_rows[...].astype(F32).T
    count = upright.shape[0] // rows
    blocks = upright.reshape(count, rows, upright.shape[1])
    number = iota(blocks.shape, 0)
    halves = [
        jnp.sum(jnp.where(number == place[2] + n * (count // 2), blocks, 0.0), axis=0) for n in range(2)
    ]
    piece = jnp.concatenate(halves, axis=1)
    for copy in copies[3:]:
        copy.wait()
    total = dot(at(0, True), held[0]) + dot(at(2, True), held[1]) + dot(at(4, False), held[2])
    for n, block in enumerate(packed_lines(total, out.shape[3]) + [piece.astype(BF16)]):
        for p in range(peers):
            out[p, n] = block


def sum_kernel(parts, out):
    lanes = out.shape[3]
    total = unpacked_lines(parts[0, 0], parts[0, 1], parts[0, 2])
    for k in range(1, parts.shape[0]):
        total = total + unpacked_lines(parts[k, 0], parts[k, 1], parts[k, 2])
    blocks = [parts[k, 3] for k in range(parts.shape[0])] + packed_lines(total, lanes)
    for p in range(out.shape[0]):
        for n, block in enumerate(blocks):
            out[p, n] = block


def by_core(core, own, other):
    return jnp.where(core == 0, own, other), jnp.where(core == 0, other, own)


STEPS = (0, -2, 2, 4, -1, -3, 1, 3)


def placed_rows(value, tp, held):
    count, rows, lanes = held.shape
    for n in range(count):
        core = tp % 2 if n < len(STEPS) else 1 - tp % 2
        chip = (tp // 2 + STEPS[n % len(STEPS)] + count // 2) % (count // 2)
        held[2 * chip + core] = value[n * rows : (n + 1) * rows]
    return held[...].reshape(count * rows, lanes)


def moments(ref, lane):
    width = ref.shape[1]
    total = jnp.zeros((ref.shape[0], lane), F32)
    for c in range(0, width, lane):
        total = total + ref[:, c : c + lane].astype(F32)
    centre = jnp.sum(total, -1, keepdims=True) * (1.0 / width)
    total = jnp.zeros((ref.shape[0], lane), F32)
    for c in range(0, width, lane):
        off = ref[:, c : c + lane].astype(F32) - centre
        total = total + off * off
    spread = jnp.sum(total, -1, keepdims=True) * (1.0 / width)
    return centre, lax.rsqrt(spread + EPS_ROW)


def modulated(place, near, far, context, mine, theirs, u, vectors, down):
    half, width = near.shape
    count, extra = 2 * half, context.shape[0]
    lane, lanes = vectors.shape[2], mine.shape[3]
    stats = [moments(ref, lane) for ref in (near, far, context)]
    first = mine.shape[1] - 3
    for x in range(mine.shape[0]):
        found = [unpacked_lines(ref[x, first], ref[x, first + 1], ref[x, first + 2]) for ref in (mine, theirs)]
        vectors[2 * x], vectors[2 * x + 1] = by_core(place[1], *found)
    pad = jnp.zeros((u.shape[0] - count - extra, lane), F32)
    for t in range(width // lane):
        cols = slice(t * lane, (t + 1) * lane)

        def one(n, ref, i):
            normed = (ref[:, cols].astype(F32) - stats[n][0]) * stats[n][1]
            return normed * (1.0 + vectors[t, 2 + i : 3 + i, :]) + vectors[t, i : i + 1, :]

        u[:half, cols] = one(0, near, 0).astype(BF16)
        u[half:count, cols] = one(1, far, 0).astype(BF16)
        u[count:, cols] = jnp.concatenate([one(2, context, 1), pad], axis=0).astype(BF16)
    for s in range(down.shape[0] // (2 * lanes)):
        even, odd = by_core(place[1], mine[:, s].astype(F32), theirs[:, s].astype(F32))
        piece = jnp.stack([even, odd], axis=1).reshape(lanes, lanes)
        down[2 * s * lanes : (2 * s + 1) * lanes] = piece.astype(BF16)
        down[(2 * s + 1) * lanes : (2 * s + 2) * lanes] = pltpu.roll(piece, HEAD, 1).astype(BF16)


def inverse(mixing, row, col):
    size = row.shape[0]
    eye = (row == col).astype(F32)
    width = 1
    found = None
    while width < size:
        shared = (row // (2 * width)) == (col // (2 * width))
        low_row, low_col = (row // width) % 2 == 1, (col // width) % 2 == 1
        corner = {False: shared & low_row & ~low_col, True: shared & low_col & ~low_row}
        parts = [jnp.where(corner[upper], m, 0.0) for m, upper in mixing]
        if found is None:
            found = [eye - p for p in parts]
        else:
            lefts = [dot(p, f) for p, f in zip(parts, found)]
            found = [f - dot(f, g) for f, g in zip(found, lefts)]
        width *= 2
    return found


def block_terms(k, v, low, fading, step, rates, spikes=None, q=None):
    count, lanes = k.shape
    row, col = iota((count, lanes), 0), iota((count, lanes), 1)
    heads = lanes // HEAD
    owns = [(col // HEAD) == h for h in range(heads)]

    squashed = jnp.tanh(low.astype(F32)).astype(BF16)
    feature = -rates * jax.nn.sigmoid(dot(squashed, fading))
    learned = jax.nn.sigmoid(dot(squashed, step) - RATE_SHIFT)
    key = k.astype(F32)
    norms = jnp.zeros_like(key)
    for own in owns:
        total = jnp.sum(jnp.where(own, key * key, 0.0), -1, keepdims=True)
        norms = jnp.where(own, lax.rsqrt(total + EPS_KEY), norms)
    unit = key * norms
    removal = unit * learned

    upto = (row >= col).astype(F32)

    def running(part):
        return lax.dot_general(
            upto, part, (((1,), (0,)), ((), ())), preferred_element_type=F32, precision=lax.Precision.HIGHEST
        )

    after = running(feature)
    before = after - feature
    grow, shrink = jnp.exp(after), jnp.exp(-after)
    grow_x, shrink_x = jnp.exp(before), jnp.exp(-before)
    end = after[count - 1 : count]
    if spikes is None:
        b_end = b_after = b_before = None
    else:
        across = jnp.zeros((lanes, count), F32)
        for h in range(heads):
            across = jnp.where(iota(across.shape, 0) // HEAD == h, -spikes[h : h + 1], across)
        jump = across.T
        b_after = running(jump)
        b_before = b_after - jump
        b_end = b_after[count - 1 : count]
        across_after, across_before = b_after.T, b_before.T

    def pair(h, upper, strict):
        inside = ((col > row) if strict else (col >= row)) if upper else ((col < row) if strict else (col <= row))
        if spikes is None:
            return inside.astype(F32)
        at = h * HEAD
        down_after, down_before = b_after[:, at : at + 1], b_before[:, at : at + 1]
        side_after, side_before = across_after[at : at + 1], across_before[at : at + 1]
        if upper:
            power = side_before - (down_after if strict else down_before)
        else:
            power = (down_before if strict else down_after) - side_after
        return jnp.where(inside, jnp.exp(jnp.where(inside, power, NEVER)), 0.0)

    def scaled(tensor, power):
        return tensor if spikes is None else tensor * jnp.exp(power)

    probes = (unit * grow_x, unit * shrink)
    removals = (removal * shrink, removal * grow_x)
    keys = (key * shrink, key * grow_x)
    asks = None if q is None else (q.astype(F32) * grow, q.astype(F32) * shrink_x)

    scores = []
    for d in range(2):
        right = jnp.concatenate([removals[d], keys[d]], axis=0)
        for own in owns:
            left = jnp.where(own, probes[d], 0.0)
            if q is not None:
                left = jnp.concatenate([left, jnp.where(own, asks[d], 0.0)], axis=0)
            scores.append(dot(left, right, ((1,), (1,))))
    chains = [(d, h) for d in range(2) for h in range(heads)]
    masks = {(d, h): pair(h, d == 1, True) for d, h in chains}
    mixing = {c: scores[n][:count, :count] * masks[c] for n, c in enumerate(chains)}
    seen = {c: dot(scores[n][:count, count:] * masks[c], v) for n, c in enumerate(chains)}
    solved = dict(zip(chains, inverse([(mixing[c], c[0] == 1) for c in chains], row, col)))

    whole = jnp.exp(end)
    starts = (
        scaled(probes[0], b_before),
        scaled(probes[1] * whole, None if spikes is None else b_end - b_after),
    )

    def gathered(parts):
        total = parts[0]
        for own, part in zip(owns[1:], parts[1:]):
            total = jnp.where(own, part, total)
        return total

    results = []
    for d in range(2):
        x, y = [], []
        for h in range(heads):
            both = dot(solved[d, h], jnp.concatenate([starts[d], seen[d, h]], axis=1))
            x.append(both[:, :lanes])
            y.append(both[:, lanes:])
        x, y = gathered(x), gathered(y)
        if d == 0:
            weigh = whole if spikes is None else whole * jnp.exp(b_end - b_after)
        else:
            weigh = jnp.ones_like(whole) if spikes is None else jnp.exp(b_before)
        last_keys, last_removals = keys[d] * weigh, removals[d] * weigh
        offset = dot(
            jnp.concatenate([v.astype(F32), -y], axis=0),
            jnp.concatenate([last_keys, last_removals], axis=0),
            ((0,), (0,)),
        )
        if q is None:
            results.append((None, offset, None, None))
            continue
        decay = whole if spikes is None else jnp.exp(end + b_end)
        factor = jnp.where(row == col, decay, 0.0) - dot(x, last_removals, ((0,), (0,)))
        if d == 0:
            query = scaled(asks[0], b_after)
        else:
            query = scaled(asks[1] * whole, None if spikes is None else b_end - b_before)
        wx, base = [], []
        for h in range(heads):
            n = chains.index((d, h))
            mask = pair(h, d == 1, False)
            reads = scores[n][count:] * jnp.concatenate([mask, mask], axis=1)
            both = dot(reads[:, :count], jnp.concatenate([x, y], axis=1))
            wx.append(both[:, :lanes])
            base.append(dot(reads[:, count:], v) - both[:, lanes:])
        results.append((factor, offset, query - gathered(wx), gathered(base)))
    return results


def same_head(shape):
    return (iota(shape, 0) // HEAD) == (iota(shape, 1) // HEAD)


def block_kernel(
    place, mine, theirs, near, far, context_, wq, wk, wv, fading_, step_, rates_, spikes_,
    sent, asked, base, vectors,
    context, held, fading, step, rates, spikes, u, moved_q, moved_k, moved_v, moved_low, sems,
):
    lanes = wq.shape[1]
    pairs = [(context_, context)]
    pairs += [(ref, held.at[n // 2, :, pl.ds(n % 2 * lanes, lanes)]) for n, ref in enumerate((wq, wk, wv))]
    pairs += [(fading_, fading), (step_, step), (rates_, rates), (spikes_, spikes)]
    copies = [pltpu.make_async_copy(ref, to, sems.at[n]) for n, (ref, to) in enumerate(pairs)]
    for copy in copies:
        copy.start()
    copies[0].wait()
    modulated(place, near, far, context, mine, theirs, u, vectors, held.at[1, :, pl.ds(lanes, lanes)])
    for copy in copies[1:]:
        copy.wait()
    count, extra = asked.shape[1], context.shape[0]
    first, second = dot(u[...], held[0]), dot(u[...], held[1])
    q, k, v, low = first[:, :lanes], first[:, lanes:], second[:, :lanes], second[:, lanes:]
    low = jnp.where(iota(low.shape, 1) < HEAD, low, 0.0)
    own = [
        placed_rows(part[:count], place[2], to).astype(BF16)
        for part, to in ((low, moved_low), (k, moved_k), (v, moved_v), (q, moved_q))
    ]
    ahead, behind = block_terms(
        own[1], own[2], own[0][:, :HEAD], fading[...], step[...], rates[...], spikes[...], own[3]
    )
    same = same_head(ahead[0].shape)
    size = same.shape[0]
    packed = [
        jnp.where(same, factor, pltpu.roll(offset, HEAD, 0)).astype(BF16)
        for factor, offset in (ahead[:2], behind[:2])
    ]
    tail = [part[count : count + extra].astype(BF16) for part in (k, v, low)]
    for j in range(sent.shape[0]):
        sent[j, :size] = jnp.where(place[0] < j, packed[0], packed[1])
        for n, part in enumerate(tail):
            sent[j, size + n * extra : size + (n + 1) * extra] = part
    asked[0], asked[1] = ahead[2].astype(BF16), behind[2].astype(BF16)
    base[...] = ahead[3] + behind[3]


def opened(packed, same):
    packed = packed.astype(F32)
    return jnp.where(same, packed, 0.0), jnp.where(same, pltpu.roll(packed, HEAD, 0), 0.0)


def read_kernel(
    place, maps, asked, base, fading_, step_, rates_, gains_, emit_,
    keep, give,
    fading, step, rates, gains, emit, sems,
):
    pairs = [(fading_, fading), (step_, step), (rates_, rates), (gains_, gains), (emit_, emit)]
    copies = [pltpu.make_async_copy(ref, to, sems.at[n]) for n, (ref, to) in enumerate(pairs)]
    for copy in copies:
        copy.start()
    for copy in copies[:4]:
        copy.wait()
    peers, _, size = maps.shape
    extra = keep.shape[1]
    same = same_head((size, size))
    me, core = place[0], place[1]
    parts = [
        jnp.concatenate([maps[j, size + n * extra : size + (n + 1) * extra].astype(F32) for j in range(peers)], axis=0)
        for n in range(3)
    ]
    parts = [part.astype(BF16) for part in parts]
    context = block_terms(parts[0], parts[1], parts[2][:, :HEAD], fading[...], step[...], rates[...])
    eye = (iota((size, size), 0) == iota((size, size), 1)).astype(F32)
    composed = [jnp.concatenate([eye, jnp.zeros_like(eye)], axis=0) for _ in range(2)]
    for n in range(peers - 1):
        for d, j, reached in ((0, n, n < me), (1, peers - 1 - n, peers - 1 - n > me)):
            factor, offset = opened(maps[j, :size], same)
            new = dot(composed[d], factor)
            new = jnp.concatenate([new[:size], new[size:] + offset], axis=0)
            composed[d] = jnp.where(reached, new, composed[d])
    out = base[...]
    for d in range(2):
        start = jnp.where(same, context[d][1], 0.0)
        state = dot(start, composed[d][:size]) + composed[d][size:]
        out = out + dot(asked[d], state, ((1,), (1,)))
    first = iota(out.shape, 1) < HEAD

    def mean(value):
        left = jnp.sum(jnp.where(first, value, 0.0), -1, keepdims=True)
        right = jnp.sum(jnp.where(first, 0.0, value), -1, keepdims=True)
        return jnp.where(first, left, right) * (1.0 / HEAD)

    out = out - mean(out)
    normed = out * lax.rsqrt(mean(out * out) + EPS_HEAD) * gains[...]
    chips, rows, _ = keep.shape
    split = normed.reshape(chips, 2, rows, size)
    even, odd = split[:, 0].reshape(chips * rows, size), split[:, 1].reshape(chips * rows, size)
    mine = jnp.where(core == 0, even, odd)
    other = jnp.where(core == 0, odd, even)
    left = jnp.concatenate([mine, other], axis=0).astype(BF16)
    copies[4].wait()
    lane = emit.shape[2]
    for s in range(emit.shape[0]):
        part = dot(left, emit[s]).reshape(2, chips, rows, lane).astype(BF16)
        keep[:, :, s * lane : (s + 1) * lane] = part[0]
        give[:, :, s * lane : (s + 1) * lane] = part[1]


def last_kernel(parts, hidden, vectors, out):
    lane = vectors.shape[2]
    for t in range(vectors.shape[0]):
        cols = slice(t * lane, (t + 1) * lane)
        total = parts[0, :, cols].astype(F32)
        for n in range(1, parts.shape[0]):
            total = total + parts[n, :, cols].astype(F32)
        out[:, cols] = (hidden[:, cols].astype(F32) + vectors[t, 4:5, :] * total).astype(BF16)


def exchange(blocks, axis, groups=None):
    return lax.all_to_all(blocks, axis, 0, 0, tiled=True, axis_index_groups=groups)


def swapped(value, axis, bit):
    return lax.ppermute(value, axis, [(i, i ^ bit) for i in range(lax.axis_size(axis))])


def shards(
    hidden_items,
    sample_cond,
    prompt_items,
    prompt_cond,
    adjust_shifting,
    adjust_stretch,
    skip_valve,
    receiver_matrix,
    address_matrix,
    payload_matrix,
    joint_lower_projector,
    fading_raise_matrix,
    step_raise_matrix,
    feature_fading,
    spike_logfade,
    group_standard_factor,
    emit_matrix,
):
    n_sp, n_tp = lax.axis_size("sp"), lax.axis_size("tp")
    me, tp = lax.axis_index("sp"), lax.axis_index("tp")
    rows, width = hidden_items.shape
    extra = prompt_items.shape[0]
    count = rows * n_tp
    lanes = receiver_matrix.shape[1]
    span, chunk = adjust_shifting.shape
    chips = n_tp // 2
    same_core = [[2 * i + c for i in range(chips)] for c in range(2)]
    place = jnp.stack([me, tp % 2, tp]).astype(jnp.int32)

    parts = call(
        partials_kernel,
        ((n_sp, 4, 8, lanes), BF16),
        place,
        sample_cond.reshape(-1, lanes),
        prompt_cond.reshape(-1, lanes),
        joint_lower_projector.T,
        adjust_shifting,
        adjust_stretch,
        skip_valve,
        scalars=1,
        fetched=6,
        room=ALL,
        flops=8 * span * chunk * 6,
        scratch=[
            pltpu.VMEM((2, width // lanes, lanes), BF16),
            pltpu.VMEM(joint_lower_projector.shape[::-1], BF16),
            pltpu.VMEM((3, span, chunk), BF16),
            pltpu.SemaphoreType.DMA((6,)),
        ],
    )
    emit = lax.all_gather(emit_matrix, "sp", axis=0)
    parts = exchange(parts, "sp")

    def shifted(value, chips_on):
        return lax.ppermute(value, "tp", [(i, (i + 2 * chips_on) % n_tp) for i in range(n_tp)])

    below = shifted(hidden_items, 2)
    above = shifted(hidden_items, -2)
    across = shifted(hidden_items, 4)
    odd_below = shifted(jnp.stack([hidden_items, below]), 1)
    odd_above = shifted(jnp.stack([hidden_items, above]), -1)
    near = jnp.concatenate([jnp.stack([hidden_items, below, above, across]), odd_below, odd_above], axis=0)
    far = swapped(near, "tp", 1)

    mine = call(sum_kernel, ((chips, n_sp + 3, 8, lanes), BF16), parts)
    mine = exchange(mine, "tp", same_core)
    theirs = swapped(mine, "tp", 1)

    padded = count + -(-extra // 16) * 16
    rates = feature_fading.reshape(1, lanes)
    sent, asked, base, vectors = call(
        block_kernel,
        [
            ((n_sp, lanes + 3 * extra, lanes), BF16),
            ((2, count, lanes), BF16),
            ((count, lanes), F32),
            ((n_tp, 8, chunk), F32),
        ],
        place,
        mine,
        theirs,
        near.reshape(count // 2, width),
        far.reshape(count // 2, width),
        prompt_items,
        receiver_matrix,
        address_matrix,
        payload_matrix,
        fading_raise_matrix,
        step_raise_matrix,
        rates,
        spike_logfade.T,
        scalars=1,
        fetched=8,
        room=MOST,
        flops=2 * padded * width * lanes * 4,
        scratch=[
            pltpu.VMEM((extra, width), BF16),
            pltpu.VMEM((2, width, 2 * lanes), BF16),
            pltpu.VMEM(fading_raise_matrix.shape, BF16),
            pltpu.VMEM(step_raise_matrix.shape, BF16),
            pltpu.VMEM(rates.shape, F32),
            pltpu.VMEM(spike_logfade.shape[::-1], F32),
            pltpu.VMEM((padded, width), BF16),
            *[pltpu.VMEM((n_tp, rows, lanes), F32)] * 4,
            pltpu.SemaphoreType.DMA((8,)),
        ],
    )
    maps = exchange(sent, "sp")
    keep, give = call(
        read_kernel,
        [((chips, rows, width), BF16)] * 2,
        place,
        maps,
        asked,
        base,
        fading_raise_matrix,
        step_raise_matrix,
        rates,
        group_standard_factor.reshape(1, lanes),
        emit,
        scalars=1,
        fetched=5,
        room=READ,
        flops=2 * count * lanes * width,
        scratch=[
            pltpu.VMEM(fading_raise_matrix.shape, BF16),
            pltpu.VMEM(step_raise_matrix.shape, BF16),
            pltpu.VMEM(rates.shape, F32),
            pltpu.VMEM((1, lanes), F32),
            pltpu.VMEM((n_sp, *emit_matrix.shape), BF16),
            pltpu.SemaphoreType.DMA((5,)),
        ],
    )
    given = swapped(give, "tp", 1)
    both = (keep.astype(F32) + given.astype(F32)).astype(BF16)
    final = exchange(both, "tp", same_core)
    return call(last_kernel, ((rows, width), BF16), final, hidden_items, vectors)


def solution(mesh):
    placed = (
        P(("grp", "sp", "tp"), None),
        P("grp"),
        P(("grp", "sp"), None),
        P(),
        P("sp", "tp"),
        P("sp", "tp"),
        P("sp", "tp"),
        P(None, "tp"),
        P(None, "tp"),
        P(None, "tp"),
        P("sp", None),
        P(None, "tp"),
        P(None, "tp"),
        P("tp"),
        P(("grp", "sp"), "tp"),
        P("tp"),
        P("tp", "sp"),
    )

    return jax.shard_map(shards, mesh=mesh, in_specs=placed, out_specs=P(("grp", "sp", "tp"), None), check_vma=False)
```

```python
import jax
import jax.numpy as jnp
from jax import lax
from jax.experimental import pallas as pl
from jax.experimental.pallas import tpu as pltpu
from jax.sharding import PartitionSpec as P


HEAD = 64
EPS_ROW = 1e-05
EPS_HEAD = 0.00064
EPS_KEY = 1e-06
RATE_SHIFT = 5.0
NEVER = -1e30
SOME, MOST, ALL, READ = 24 * 1024 * 1024, 52 * 1024 * 1024, 63 * 1024 * 1024, 52 * 1024 * 1024
BF16, F32 = jnp.bfloat16, jnp.float32

VMEM = pl.BlockSpec(memory_space=pltpu.VMEM)
HBM = pl.BlockSpec(memory_space=pltpu.HBM)


def call(body, outs, *args, flops=0, scratch=(), fetched=0, room=SOME):
    many = isinstance(outs, list)
    shapes = [jax.ShapeDtypeStruct(s, d) for s, d in (outs if many else [outs])]
    got = pl.pallas_call(
        body,
        out_shape=shapes,
        in_specs=[VMEM] * (len(args) - fetched) + [HBM] * fetched,
        out_specs=[VMEM] * len(shapes),
        scratch_shapes=list(scratch),
        compiler_params=pltpu.CompilerParams(vmem_limit_bytes=room),
        cost_estimate=pl.CostEstimate(
            flops=flops, transcendentals=0, bytes_accessed=sum(a.size * a.dtype.itemsize for a in args)
        ),
    )(*args)
    return got if many else got[0]


def dot(left, right, dims=((1,), (0,))):
    return lax.dot_general(
        left.astype(BF16), right.astype(BF16), (dims, ((), ())), preferred_element_type=F32
    )


def iota(shape, dim):
    return lax.broadcasted_iota(jnp.int32, shape, dim)


USED = 5


def packed_lines(total, lanes):
    high = total.astype(BF16).astype(F32)
    rest = total - high
    row = iota((total.shape[0], lanes), 0)
    last = rest[:, lanes:]
    free = total.shape[0] - USED
    return [
        jnp.where(row < USED, high[:, :lanes], pltpu.roll(last, USED, 0)).astype(BF16),
        jnp.where(row < USED, high[:, lanes:], pltpu.roll(last, USED - free, 0)).astype(BF16),
        rest[:, :lanes].astype(BF16),
    ]


def unpacked_lines(first, second, third):
    first, second, third = (part.astype(F32) for part in (first, second, third))
    count = first.shape[0]
    row = iota(first.shape, 0)
    free = count - USED
    last = jnp.where(row < free, pltpu.roll(first, count - USED, 0), pltpu.roll(second, count - USED + free, 0))
    return jnp.concatenate([first + third, second + last], axis=1)


def partials_kernel(sample, prompt, lower, shifting, stretch, valve, out, conds, low_rows, held, sems):
    place = here()
    pairs = [(sample, conds.at[0]), (prompt, conds.at[1]), (lower, low_rows)]
    pairs += [(ref, held.at[n]) for n, ref in enumerate((shifting, stretch, valve))]
    copies = [pltpu.make_async_copy(ref, to, sems.at[n]) for n, (ref, to) in enumerate(pairs)]
    for copy in copies:
        copy.start()
    for copy in copies[:3]:
        copy.wait()
    peers, _, rows, _ = out.shape
    chunk = held.shape[2]
    wide = chunk // sample.shape[1]
    line = iota(sample.shape, 0)

    def own(n):
        full = conds[n].astype(F32)
        cut = [
            jnp.sum(jnp.where(line == place[0] * wide + n, full, 0.0), axis=0, keepdims=True) for n in range(wide)
        ]
        return jax.nn.silu(jnp.concatenate(cut, axis=1))

    row = iota((rows, chunk), 0)
    first, second = own(0), own(1)

    def at(k, both):
        left = jnp.where(row == k, first, 0.0)
        return jnp.where(row == k + 1, second, left) if both else left

    upright = low_rows[...].astype(F32).T
    count = upright.shape[0] // rows
    blocks = upright.reshape(count, rows, upright.shape[1])
    number = iota(blocks.shape, 0)
    halves = [
        jnp.sum(jnp.where(number == place[2] + n * (count // 2), blocks, 0.0), axis=0) for n in range(2)
    ]
    piece = jnp.concatenate(halves, axis=1)
    for copy in copies[3:]:
        copy.wait()
    total = dot(at(0, True), held[0]) + dot(at(2, True), held[1]) + dot(at(4, False), held[2])
    for n, block in enumerate(packed_lines(total, out.shape[3]) + [piece.astype(BF16)]):
        for p in range(peers):
            out[p, n] = block


def sum_kernel(parts, out):
    lanes = out.shape[3]
    total = unpacked_lines(parts[0, 0], parts[0, 1], parts[0, 2])
    for k in range(1, parts.shape[0]):
        total = total + unpacked_lines(parts[k, 0], parts[k, 1], parts[k, 2])
    blocks = [parts[k, 3] for k in range(parts.shape[0])] + packed_lines(total, lanes)
    for p in range(out.shape[0]):
        for n, block in enumerate(blocks):
            out[p, n] = block


def here():
    tp = lax.axis_index("tp")
    return lax.axis_index("sp"), tp % 2, tp


def by_core(core, own, other):
    return jnp.where(core == 0, own, other), jnp.where(core == 0, other, own)


STEPS = (0, -2, 2, 4, -1, -3, 1, 3)


def placed_rows(value, tp, held):
    count, rows, lanes = held.shape
    for n in range(count):
        core = tp % 2 if n < len(STEPS) else 1 - tp % 2
        chip = (tp // 2 + STEPS[n % len(STEPS)] + count // 2) % (count // 2)
        held[2 * chip + core] = value[n * rows : (n + 1) * rows]
    return held[...].reshape(count * rows, lanes)


def moments(ref, lane):
    width = ref.shape[1]
    total = jnp.zeros((ref.shape[0], lane), F32)
    for c in range(0, width, lane):
        total = total + ref[:, c : c + lane].astype(F32)
    centre = jnp.sum(total, -1, keepdims=True) * (1.0 / width)
    total = jnp.zeros((ref.shape[0], lane), F32)
    for c in range(0, width, lane):
        off = ref[:, c : c + lane].astype(F32) - centre
        total = total + off * off
    spread = jnp.sum(total, -1, keepdims=True) * (1.0 / width)
    return centre, lax.rsqrt(spread + EPS_ROW)


def modulated(place, near, far, context, mine, theirs, u, vectors, down):
    half, width = near.shape
    count, extra = 2 * half, context.shape[0]
    lane, lanes = vectors.shape[2], mine.shape[3]
    stats = [moments(ref, lane) for ref in (near, far, context)]
    first = mine.shape[1] - 3
    for x in range(mine.shape[0]):
        found = [unpacked_lines(ref[x, first], ref[x, first + 1], ref[x, first + 2]) for ref in (mine, theirs)]
        vectors[2 * x], vectors[2 * x + 1] = by_core(place[1], *found)
    pad = jnp.zeros((u.shape[0] - count - extra, lane), F32)
    for t in range(width // lane):
        cols = slice(t * lane, (t + 1) * lane)

        def one(n, ref, i):
            normed = (ref[:, cols].astype(F32) - stats[n][0]) * stats[n][1]
            return normed * (1.0 + vectors[t, 2 + i : 3 + i, :]) + vectors[t, i : i + 1, :]

        u[:half, cols] = one(0, near, 0).astype(BF16)
        u[half:count, cols] = one(1, far, 0).astype(BF16)
        u[count:, cols] = jnp.concatenate([one(2, context, 1), pad], axis=0).astype(BF16)
    for s in range(down.shape[0] // (2 * lanes)):
        even, odd = by_core(place[1], mine[:, s].astype(F32), theirs[:, s].astype(F32))
        piece = jnp.stack([even, odd], axis=1).reshape(lanes, lanes)
        down[2 * s * lanes : (2 * s + 1) * lanes] = piece.astype(BF16)
        down[(2 * s + 1) * lanes : (2 * s + 2) * lanes] = pltpu.roll(piece, HEAD, 1).astype(BF16)


def inverse(mixing, row, col):
    size = row.shape[0]
    eye = (row == col).astype(F32)
    width = 1
    found = None
    while width < size:
        shared = (row // (2 * width)) == (col // (2 * width))
        low_row, low_col = (row // width) % 2 == 1, (col // width) % 2 == 1
        corner = {False: shared & low_row & ~low_col, True: shared & low_col & ~low_row}
        parts = [jnp.where(corner[upper], m, 0.0) for m, upper in mixing]
        if found is None:
            found = [eye - p for p in parts]
        else:
            lefts = [dot(p, f) for p, f in zip(parts, found)]
            found = [f - dot(f, g) for f, g in zip(found, lefts)]
        width *= 2
    return found


def block_terms(k, v, low, fading, step, rates, spikes=None, q=None):
    count, lanes = k.shape
    row, col = iota((count, lanes), 0), iota((count, lanes), 1)
    heads = lanes // HEAD
    owns = [(col // HEAD) == h for h in range(heads)]

    squashed = jnp.tanh(low.astype(F32)).astype(BF16)
    feature = -rates * jax.nn.sigmoid(dot(squashed, fading))
    learned = jax.nn.sigmoid(dot(squashed, step) - RATE_SHIFT)
    key = k.astype(F32)
    norms = jnp.zeros_like(key)
    for own in owns:
        total = jnp.sum(jnp.where(own, key * key, 0.0), -1, keepdims=True)
        norms = jnp.where(own, lax.rsqrt(total + EPS_KEY), norms)
    unit = key * norms
    removal = unit * learned

    upto = (row >= col).astype(F32)

    def running(part):
        return lax.dot_general(
            upto, part, (((1,), (0,)), ((), ())), preferred_element_type=F32, precision=lax.Precision.HIGHEST
        )

    after = running(feature)
    before = after - feature
    grow, shrink = jnp.exp(after), jnp.exp(-after)
    grow_x, shrink_x = jnp.exp(before), jnp.exp(-before)
    end = after[count - 1 : count]
    if spikes is None:
        b_end = b_after = b_before = None
    else:
        across = jnp.zeros((lanes, count), F32)
        for h in range(heads):
            across = jnp.where(iota(across.shape, 0) // HEAD == h, -spikes[h : h + 1], across)
        jump = across.T
        b_after = running(jump)
        b_before = b_after - jump
        b_end = b_after[count - 1 : count]
        across_after, across_before = b_after.T, b_before.T

    def pair(h, upper, strict):
        inside = ((col > row) if strict else (col >= row)) if upper else ((col < row) if strict else (col <= row))
        if spikes is None:
            return inside.astype(F32)
        at = h * HEAD
        down_after, down_before = b_after[:, at : at + 1], b_before[:, at : at + 1]
        side_after, side_before = across_after[at : at + 1], across_before[at : at + 1]
        if upper:
            power = side_before - (down_after if strict else down_before)
        else:
            power = (down_before if strict else down_after) - side_after
        return jnp.where(inside, jnp.exp(jnp.where(inside, power, NEVER)), 0.0)

    def scaled(tensor, power):
        return tensor if spikes is None else tensor * jnp.exp(power)

    probes = (unit * grow_x, unit * shrink)
    removals = (removal * shrink, removal * grow_x)
    keys = (key * shrink, key * grow_x)
    asks = None if q is None else (q.astype(F32) * grow, q.astype(F32) * shrink_x)

    scores = []
    for d in range(2):
        right = jnp.concatenate([removals[d], keys[d]], axis=0)
        for own in owns:
            left = jnp.where(own, probes[d], 0.0)
            if q is not None:
                left = jnp.concatenate([left, jnp.where(own, asks[d], 0.0)], axis=0)
            scores.append(dot(left, right, ((1,), (1,))))
    chains = [(d, h) for d in range(2) for h in range(heads)]
    masks = {(d, h): pair(h, d == 1, True) for d, h in chains}
    mixing = {c: scores[n][:count, :count] * masks[c] for n, c in enumerate(chains)}
    seen = {c: dot(scores[n][:count, count:] * masks[c], v) for n, c in enumerate(chains)}
    solved = dict(zip(chains, inverse([(mixing[c], c[0] == 1) for c in chains], row, col)))

    whole = jnp.exp(end)
    starts = (
        scaled(probes[0], b_before),
        scaled(probes[1] * whole, None if spikes is None else b_end - b_after),
    )

    def gathered(parts):
        total = parts[0]
        for own, part in zip(owns[1:], parts[1:]):
            total = jnp.where(own, part, total)
        return total

    results = []
    for d in range(2):
        x, y = [], []
        for h in range(heads):
            both = dot(solved[d, h], jnp.concatenate([starts[d], seen[d, h]], axis=1))
            x.append(both[:, :lanes])
            y.append(both[:, lanes:])
        x, y = gathered(x), gathered(y)
        if d == 0:
            weigh = whole if spikes is None else whole * jnp.exp(b_end - b_after)
        else:
            weigh = jnp.ones_like(whole) if spikes is None else jnp.exp(b_before)
        last_keys, last_removals = keys[d] * weigh, removals[d] * weigh
        offset = dot(
            jnp.concatenate([v.astype(F32), -y], axis=0),
            jnp.concatenate([last_keys, last_removals], axis=0),
            ((0,), (0,)),
        )
        if q is None:
            results.append((None, offset, None, None))
            continue
        decay = whole if spikes is None else jnp.exp(end + b_end)
        factor = jnp.where(row == col, decay, 0.0) - dot(x, last_removals, ((0,), (0,)))
        if d == 0:
            query = scaled(asks[0], b_after)
        else:
            query = scaled(asks[1] * whole, None if spikes is None else b_end - b_before)
        wx, base = [], []
        for h in range(heads):
            n = chains.index((d, h))
            mask = pair(h, d == 1, False)
            reads = scores[n][count:] * jnp.concatenate([mask, mask], axis=1)
            both = dot(reads[:, :count], jnp.concatenate([x, y], axis=1))
            wx.append(both[:, :lanes])
            base.append(dot(reads[:, count:], v) - both[:, lanes:])
        results.append((factor, offset, query - gathered(wx), gathered(base)))
    return results


def same_head(shape):
    return (iota(shape, 0) // HEAD) == (iota(shape, 1) // HEAD)


def block_kernel(
    mine, theirs, near, far, context_, wq, wk, wv, fading_, step_, rates_, gains_, spikes_,
    sent, asked, base, vectors, fading, step, lines,
    context, held, spikes, u, moved_q, moved_k, moved_v, moved_low, sems,
):
    place = here()
    lanes = wq.shape[1]
    pairs = [(context_, context)]
    pairs += [(ref, held.at[n // 2, :, pl.ds(n % 2 * lanes, lanes)]) for n, ref in enumerate((wq, wk, wv))]
    pairs += [(fading_, fading), (step_, step), (rates_, lines.at[0:1]), (gains_, lines.at[1:2]), (spikes_, spikes)]
    copies = [pltpu.make_async_copy(ref, to, sems.at[n]) for n, (ref, to) in enumerate(pairs)]
    for copy in copies:
        copy.start()
    copies[0].wait()
    modulated(place, near, far, context, mine, theirs, u, vectors, held.at[1, :, pl.ds(lanes, lanes)])
    for copy in copies[1:]:
        copy.wait()
    count, extra = asked.shape[1], context.shape[0]
    first, second = dot(u[...], held[0]), dot(u[...], held[1])
    q, k, v, low = first[:, :lanes], first[:, lanes:], second[:, :lanes], second[:, lanes:]
    low = jnp.where(iota(low.shape, 1) < HEAD, low, 0.0)
    own = [
        placed_rows(part[:count], place[2], to).astype(BF16)
        for part, to in ((low, moved_low), (k, moved_k), (v, moved_v), (q, moved_q))
    ]
    ahead, behind = block_terms(
        own[1], own[2], own[0][:, :HEAD], fading[...], step[...], lines[0:1], spikes[...], own[3]
    )
    same = same_head(ahead[0].shape)
    size = same.shape[0]
    packed = [
        jnp.where(same, factor, pltpu.roll(offset, HEAD, 0)).astype(BF16)
        for factor, offset in (ahead[:2], behind[:2])
    ]
    tail = [part[count : count + extra].astype(BF16) for part in (k, v, low)]
    for j in range(sent.shape[0]):
        sent[j, :size] = jnp.where(place[0] < j, packed[0], packed[1])
        for n, part in enumerate(tail):
            sent[j, size + n * extra : size + (n + 1) * extra] = part
    asked[0], asked[1] = ahead[2].astype(BF16), behind[2].astype(BF16)
    base[...] = ahead[3] + behind[3]


def opened(packed, same):
    packed = packed.astype(F32)
    return jnp.where(same, packed, 0.0), jnp.where(same, pltpu.roll(packed, HEAD, 0), 0.0)


def read_kernel(maps, asked, base, fading, step, lines, emit_, keep, give, emit, sem):
    copy = pltpu.make_async_copy(emit_, emit, sem)
    copy.start()
    rates, gains = lines[0:1], lines[1:2]
    peers, _, size = maps.shape
    extra = keep.shape[1]
    same = same_head((size, size))
    me, core, _ = here()
    parts = [
        jnp.concatenate([maps[j, size + n * extra : size + (n + 1) * extra].astype(F32) for j in range(peers)], axis=0)
        for n in range(3)
    ]
    parts = [part.astype(BF16) for part in parts]
    context = block_terms(parts[0], parts[1], parts[2][:, :HEAD], fading[...], step[...], rates)
    eye = (iota((size, size), 0) == iota((size, size), 1)).astype(F32)
    composed = [jnp.concatenate([eye, jnp.zeros_like(eye)], axis=0) for _ in range(2)]
    for n in range(peers - 1):
        for d, j, reached in ((0, n, n < me), (1, peers - 1 - n, peers - 1 - n > me)):
            factor, offset = opened(maps[j, :size], same)
            new = dot(composed[d], factor)
            new = jnp.concatenate([new[:size], new[size:] + offset], axis=0)
            composed[d] = jnp.where(reached, new, composed[d])
    out = base[...]
    for d in range(2):
        start = jnp.where(same, context[d][1], 0.0)
        state = dot(start, composed[d][:size]) + composed[d][size:]
        out = out + dot(asked[d], state, ((1,), (1,)))
    first = iota(out.shape, 1) < HEAD

    def mean(value):
        left = jnp.sum(jnp.where(first, value, 0.0), -1, keepdims=True)
        right = jnp.sum(jnp.where(first, 0.0, value), -1, keepdims=True)
        return jnp.where(first, left, right) * (1.0 / HEAD)

    out = out - mean(out)
    normed = out * lax.rsqrt(mean(out * out) + EPS_HEAD) * gains
    chips, rows, _ = keep.shape
    split = normed.reshape(chips, 2, rows, size)
    even, odd = split[:, 0].reshape(chips * rows, size), split[:, 1].reshape(chips * rows, size)
    mine = jnp.where(core == 0, even, odd)
    other = jnp.where(core == 0, odd, even)
    left = jnp.concatenate([mine, other], axis=0).astype(BF16)
    copy.wait()
    lane = emit.shape[2]
    for s in range(emit.shape[0]):
        part = dot(left, emit[s]).reshape(2, chips, rows, lane).astype(BF16)
        keep[:, :, s * lane : (s + 1) * lane] = part[0]
        give[:, :, s * lane : (s + 1) * lane] = part[1]


def last_kernel(parts, hidden, vectors, out):
    lane = vectors.shape[2]
    for t in range(vectors.shape[0]):
        cols = slice(t * lane, (t + 1) * lane)
        total = parts[0, :, cols].astype(F32)
        for n in range(1, parts.shape[0]):
            total = total + parts[n, :, cols].astype(F32)
        out[:, cols] = (hidden[:, cols].astype(F32) + vectors[t, 4:5, :] * total).astype(BF16)


def exchange(blocks, axis, groups=None):
    return lax.all_to_all(blocks, axis, 0, 0, tiled=True, axis_index_groups=groups)


def swapped(value, axis, bit):
    return lax.ppermute(value, axis, [(i, i ^ bit) for i in range(lax.axis_size(axis))])


def shards(
    hidden_items,
    sample_cond,
    prompt_items,
    prompt_cond,
    adjust_shifting,
    adjust_stretch,
    skip_valve,
    receiver_matrix,
    address_matrix,
    payload_matrix,
    joint_lower_projector,
    fading_raise_matrix,
    step_raise_matrix,
    feature_fading,
    spike_logfade,
    group_standard_factor,
    emit_matrix,
):
    n_sp, n_tp = lax.axis_size("sp"), lax.axis_size("tp")
    rows, width = hidden_items.shape
    extra = prompt_items.shape[0]
    count = rows * n_tp
    lanes = receiver_matrix.shape[1]
    span, chunk = adjust_shifting.shape
    chips = n_tp // 2
    same_core = [[2 * i + c for i in range(chips)] for c in range(2)]

    parts = call(
        partials_kernel,
        ((n_sp, 4, 8, lanes), BF16),
        sample_cond.reshape(-1, lanes),
        prompt_cond.reshape(-1, lanes),
        joint_lower_projector.T,
        adjust_shifting,
        adjust_stretch,
        skip_valve,
        fetched=6,
        room=ALL,
        flops=8 * span * chunk * 6,
        scratch=[
            pltpu.VMEM((2, width // lanes, lanes), BF16),
            pltpu.VMEM(joint_lower_projector.shape[::-1], BF16),
            pltpu.VMEM((3, span, chunk), BF16),
            pltpu.SemaphoreType.DMA((6,)),
        ],
    )
    emit = lax.all_gather(emit_matrix, "sp", axis=0)
    parts = exchange(parts, "sp")

    def shifted(value, chips_on):
        return lax.ppermute(value, "tp", [(i, (i + 2 * chips_on) % n_tp) for i in range(n_tp)])

    below = shifted(hidden_items, 2)
    above = shifted(hidden_items, -2)
    across = shifted(above, -2)
    odd_below = shifted(jnp.stack([hidden_items, below]), 1)
    odd_above = shifted(jnp.stack([hidden_items, above]), -1)
    near = jnp.concatenate([jnp.stack([hidden_items, below, above, across]), odd_below, odd_above], axis=0)
    far = swapped(near, "tp", 1)

    mine = call(sum_kernel, ((chips, n_sp + 3, 8, lanes), BF16), parts)
    mine = exchange(mine, "tp", same_core)
    theirs = swapped(mine, "tp", 1)

    padded = count + -(-extra // 16) * 16
    sent, asked, base, vectors, *small = call(
        block_kernel,
        [
            ((n_sp, lanes + 3 * extra, lanes), BF16),
            ((2, count, lanes), BF16),
            ((count, lanes), F32),
            ((n_tp, 8, chunk), F32),
            (fading_raise_matrix.shape, BF16),
            (step_raise_matrix.shape, BF16),
            ((2, lanes), F32),
        ],
        mine,
        theirs,
        near.reshape(count // 2, width),
        far.reshape(count // 2, width),
        prompt_items,
        receiver_matrix,
        address_matrix,
        payload_matrix,
        fading_raise_matrix,
        step_raise_matrix,
        feature_fading.reshape(1, lanes),
        group_standard_factor.reshape(1, lanes),
        spike_logfade.T,
        fetched=9,
        room=MOST,
        flops=2 * padded * width * lanes * 4,
        scratch=[
            pltpu.VMEM((extra, width), BF16),
            pltpu.VMEM((2, width, 2 * lanes), BF16),
            pltpu.VMEM(spike_logfade.shape[::-1], F32),
            pltpu.VMEM((padded, width), BF16),
            *[pltpu.VMEM((n_tp, rows, lanes), F32)] * 4,
            pltpu.SemaphoreType.DMA((9,)),
        ],
    )
    maps = exchange(sent, "sp")
    keep, give = call(
        read_kernel,
        [((chips, rows, width), BF16)] * 2,
        maps,
        asked,
        base,
        *small,
        emit,
        fetched=1,
        room=READ,
        flops=2 * count * lanes * width,
        scratch=[
            pltpu.VMEM((n_sp, *emit_matrix.shape), BF16),
            pltpu.SemaphoreType.DMA,
        ],
    )
    given = swapped(give, "tp", 1)
    both = (keep.astype(F32) + given.astype(F32)).astype(BF16)
    final = exchange(both, "tp", same_core)
    return call(last_kernel, ((rows, width), BF16), final, hidden_items, vectors)


def solution(mesh):
    placed = (
        P(("grp", "sp", "tp"), None),
        P("grp"),
        P(("grp", "sp"), None),
        P(),
        P("sp", "tp"),
        P("sp", "tp"),
        P("sp", "tp"),
        P(None, "tp"),
        P(None, "tp"),
        P(None, "tp"),
        P("sp", None),
        P(None, "tp"),
        P(None, "tp"),
        P("tp"),
        P(("grp", "sp"), "tp"),
        P("tp"),
        P("tp", "sp"),
    )

    return jax.shard_map(shards, mesh=mesh, in_specs=placed, out_specs=P(("grp", "sp", "tp"), None), check_vma=False)
```

```python
import jax
import jax.numpy as jnp
from jax import lax
from jax.experimental import pallas as pl
from jax.experimental.pallas import tpu as pltpu
from jax.sharding import PartitionSpec as P


HEAD = 64
EPS_ROW = 1e-05
EPS_HEAD = 0.00064
EPS_KEY = 1e-06
RATE_SHIFT = 5.0
NEVER = -1e30
SOME, MOST, ALL, READ = 24 * 1024 * 1024, 52 * 1024 * 1024, 63 * 1024 * 1024, 52 * 1024 * 1024
BF16, F32 = jnp.bfloat16, jnp.float32

VMEM = pl.BlockSpec(memory_space=pltpu.VMEM)
HBM = pl.BlockSpec(memory_space=pltpu.HBM)


def call(body, outs, *args, flops=0, scratch=(), fetched=0, room=SOME):
    many = isinstance(outs, list)
    shapes = [jax.ShapeDtypeStruct(s, d) for s, d in (outs if many else [outs])]
    got = pl.pallas_call(
        body,
        out_shape=shapes,
        in_specs=[VMEM] * (len(args) - fetched) + [HBM] * fetched,
        out_specs=[VMEM] * len(shapes),
        scratch_shapes=list(scratch),
        compiler_params=pltpu.CompilerParams(vmem_limit_bytes=room),
        cost_estimate=pl.CostEstimate(
            flops=flops, transcendentals=0, bytes_accessed=sum(a.size * a.dtype.itemsize for a in args)
        ),
    )(*args)
    return got if many else got[0]


def dot(left, right, dims=((1,), (0,))):
    return lax.dot_general(
        left.astype(BF16), right.astype(BF16), (dims, ((), ())), preferred_element_type=F32
    )


def iota(shape, dim):
    return lax.broadcasted_iota(jnp.int32, shape, dim)


USED = 5


def packed_lines(total, lanes):
    high = total.astype(BF16).astype(F32)
    rest = total - high
    row = iota((total.shape[0], lanes), 0)
    last = rest[:, lanes:]
    free = total.shape[0] - USED
    return [
        jnp.where(row < USED, high[:, :lanes], pltpu.roll(last, USED, 0)).astype(BF16),
        jnp.where(row < USED, high[:, lanes:], pltpu.roll(last, USED - free, 0)).astype(BF16),
        rest[:, :lanes].astype(BF16),
    ]


def unpacked_lines(first, second, third):
    first, second, third = (part.astype(F32) for part in (first, second, third))
    count = first.shape[0]
    row = iota(first.shape, 0)
    free = count - USED
    last = jnp.where(row < free, pltpu.roll(first, count - USED, 0), pltpu.roll(second, count - USED + free, 0))
    return jnp.concatenate([first + third, second + last], axis=1)


def partials_kernel(sample, prompt, lower, shifting, stretch, valve, out, conds, low_rows, held, sems):
    place = here()
    pairs = [(sample, conds.at[0]), (prompt, conds.at[1]), (lower, low_rows)]
    pairs += [(ref, held.at[n]) for n, ref in enumerate((shifting, stretch, valve))]
    copies = [pltpu.make_async_copy(ref, to, sems.at[n]) for n, (ref, to) in enumerate(pairs)]
    for copy in copies:
        copy.start()
    for copy in copies[:3]:
        copy.wait()
    peers, _, rows, _ = out.shape
    chunk = held.shape[2]
    wide = chunk // sample.shape[1]
    line = iota(sample.shape, 0)

    def own(n):
        full = conds[n].astype(F32)
        cut = [
            jnp.sum(jnp.where(line == place[0] * wide + n, full, 0.0), axis=0, keepdims=True) for n in range(wide)
        ]
        return jax.nn.silu(jnp.concatenate(cut, axis=1))

    row = iota((rows, chunk), 0)
    first, second = own(0), own(1)

    def at(k, both):
        left = jnp.where(row == k, first, 0.0)
        return jnp.where(row == k + 1, second, left) if both else left

    upright = low_rows[...].astype(F32).T
    count = upright.shape[0] // rows
    blocks = upright.reshape(count, rows, upright.shape[1])
    number = iota(blocks.shape, 0)
    halves = [
        jnp.sum(jnp.where(number == place[2] + n * (count // 2), blocks, 0.0), axis=0) for n in range(2)
    ]
    piece = jnp.concatenate(halves, axis=1)
    for copy in copies[3:]:
        copy.wait()
    total = dot(at(0, True), held[0]) + dot(at(2, True), held[1]) + dot(at(4, False), held[2])
    for n, block in enumerate(packed_lines(total, out.shape[3]) + [piece.astype(BF16)]):
        for p in range(peers):
            out[p, n] = block


def sum_kernel(parts, out):
    lanes = out.shape[3]
    total = unpacked_lines(parts[0, 0], parts[0, 1], parts[0, 2])
    for k in range(1, parts.shape[0]):
        total = total + unpacked_lines(parts[k, 0], parts[k, 1], parts[k, 2])
    blocks = [parts[k, 3] for k in range(parts.shape[0])] + packed_lines(total, lanes)
    for p in range(out.shape[0]):
        for n, block in enumerate(blocks):
            out[p, n] = block


def here():
    tp = lax.axis_index("tp")
    return lax.axis_index("sp"), tp % 2, tp


def by_core(core, own, other):
    return jnp.where(core == 0, own, other), jnp.where(core == 0, other, own)


STEPS = (0, -2, 2, 4, -1, -3, 1, 3)


def placed_rows(value, tp, held):
    count, rows, lanes = held.shape
    for n in range(count):
        core = tp % 2 if n < len(STEPS) else 1 - tp % 2
        chip = (tp // 2 + STEPS[n % len(STEPS)] + count // 2) % (count // 2)
        held[2 * chip + core] = value[n * rows : (n + 1) * rows]
    return held[...].reshape(count * rows, lanes)


def moments(ref, lane):
    width = ref.shape[1]
    total = jnp.zeros((ref.shape[0], lane), F32)
    for c in range(0, width, lane):
        total = total + ref[:, c : c + lane].astype(F32)
    centre = jnp.sum(total, -1, keepdims=True) * (1.0 / width)
    total = jnp.zeros((ref.shape[0], lane), F32)
    for c in range(0, width, lane):
        off = ref[:, c : c + lane].astype(F32) - centre
        total = total + off * off
    spread = jnp.sum(total, -1, keepdims=True) * (1.0 / width)
    return centre, lax.rsqrt(spread + EPS_ROW)


def modulated(place, near, far, context, mine, theirs, u, vectors, down):
    half, width = near.shape
    count, extra = 2 * half, context.shape[0]
    lane, lanes = vectors.shape[2], mine.shape[3]
    stats = [moments(ref, lane) for ref in (near, far, context)]
    first = mine.shape[1] - 3
    for x in range(mine.shape[0]):
        found = [unpacked_lines(ref[x, first], ref[x, first + 1], ref[x, first + 2]) for ref in (mine, theirs)]
        vectors[2 * x], vectors[2 * x + 1] = by_core(place[1], *found)
    pad = jnp.zeros((u.shape[0] - count - extra, lane), F32)
    for t in range(width // lane):
        cols = slice(t * lane, (t + 1) * lane)

        def one(n, ref, i):
            normed = (ref[:, cols].astype(F32) - stats[n][0]) * stats[n][1]
            return normed * (1.0 + vectors[t, 2 + i : 3 + i, :]) + vectors[t, i : i + 1, :]

        u[:half, cols] = one(0, near, 0).astype(BF16)
        u[half:count, cols] = one(1, far, 0).astype(BF16)
        u[count:, cols] = jnp.concatenate([one(2, context, 1), pad], axis=0).astype(BF16)
    for s in range(down.shape[0] // (2 * lanes)):
        even, odd = by_core(place[1], mine[:, s].astype(F32), theirs[:, s].astype(F32))
        piece = jnp.stack([even, odd], axis=1).reshape(lanes, lanes)
        down[2 * s * lanes : (2 * s + 1) * lanes] = piece.astype(BF16)
        down[(2 * s + 1) * lanes : (2 * s + 2) * lanes] = pltpu.roll(piece, HEAD, 1).astype(BF16)


def inverse(mixing, row, col, between):
    size = row.shape[0]
    eye = (row == col).astype(F32)
    width = 1
    found = None
    while width < size:
        shared = (row // (2 * width)) == (col // (2 * width))
        low_row, low_col = (row // width) % 2 == 1, (col // width) % 2 == 1
        corner = {False: shared & low_row & ~low_col, True: shared & low_col & ~low_row}
        parts = [jnp.where(corner[upper], m, 0.0) for m, upper in mixing]
        if found is None:
            found = [eye - p for p in parts]
        else:
            lefts = [dot(p, f) for p, f in zip(parts, found)]
            next(between, None)
            found = [f - dot(f, g) for f, g in zip(found, lefts)]
            next(between, None)
        width *= 2
    return found


def block_terms(k, v, low, fading, step, rates, spikes=None, q=None, between=iter(())):
    count, lanes = k.shape
    row, col = iota((count, lanes), 0), iota((count, lanes), 1)
    heads = lanes // HEAD
    owns = [(col // HEAD) == h for h in range(heads)]

    squashed = jnp.tanh(low.astype(F32)).astype(BF16)
    feature = -rates * jax.nn.sigmoid(dot(squashed, fading))
    learned = jax.nn.sigmoid(dot(squashed, step) - RATE_SHIFT)
    key = k.astype(F32)
    norms = jnp.zeros_like(key)
    for own in owns:
        total = jnp.sum(jnp.where(own, key * key, 0.0), -1, keepdims=True)
        norms = jnp.where(own, lax.rsqrt(total + EPS_KEY), norms)
    unit = key * norms
    removal = unit * learned

    upto = (row >= col).astype(F32)

    def running(part):
        return lax.dot_general(
            upto, part, (((1,), (0,)), ((), ())), preferred_element_type=F32, precision=lax.Precision.HIGHEST
        )

    after = running(feature)
    before = after - feature
    grow, shrink = jnp.exp(after), jnp.exp(-after)
    grow_x, shrink_x = jnp.exp(before), jnp.exp(-before)
    end = after[count - 1 : count]
    if spikes is None:
        b_end = b_after = b_before = None
    else:
        across = jnp.zeros((lanes, count), F32)
        for h in range(heads):
            across = jnp.where(iota(across.shape, 0) // HEAD == h, -spikes[h : h + 1], across)
        jump = across.T
        b_after = running(jump)
        b_before = b_after - jump
        b_end = b_after[count - 1 : count]
        across_after, across_before = b_after.T, b_before.T

    def pair(h, upper, strict):
        inside = ((col > row) if strict else (col >= row)) if upper else ((col < row) if strict else (col <= row))
        if spikes is None:
            return inside.astype(F32)
        at = h * HEAD
        down_after, down_before = b_after[:, at : at + 1], b_before[:, at : at + 1]
        side_after, side_before = across_after[at : at + 1], across_before[at : at + 1]
        if upper:
            power = side_before - (down_after if strict else down_before)
        else:
            power = (down_before if strict else down_after) - side_after
        return jnp.where(inside, jnp.exp(jnp.where(inside, power, NEVER)), 0.0)

    def scaled(tensor, power):
        return tensor if spikes is None else tensor * jnp.exp(power)

    probes = (unit * grow_x, unit * shrink)
    removals = (removal * shrink, removal * grow_x)
    keys = (key * shrink, key * grow_x)
    asks = None if q is None else (q.astype(F32) * grow, q.astype(F32) * shrink_x)

    scores = []
    for d in range(2):
        right = jnp.concatenate([removals[d], keys[d]], axis=0)
        for own in owns:
            left = jnp.where(own, probes[d], 0.0)
            if q is not None:
                left = jnp.concatenate([left, jnp.where(own, asks[d], 0.0)], axis=0)
            scores.append(dot(left, right, ((1,), (1,))))
    chains = [(d, h) for d in range(2) for h in range(heads)]
    masks = {(d, h): pair(h, d == 1, True) for d, h in chains}
    mixing = {c: scores[n][:count, :count] * masks[c] for n, c in enumerate(chains)}
    seen = {c: dot(scores[n][:count, count:] * masks[c], v) for n, c in enumerate(chains)}
    solved = dict(zip(chains, inverse([(mixing[c], c[0] == 1) for c in chains], row, col, between)))

    whole = jnp.exp(end)
    starts = (
        scaled(probes[0], b_before),
        scaled(probes[1] * whole, None if spikes is None else b_end - b_after),
    )

    def gathered(parts):
        total = parts[0]
        for own, part in zip(owns[1:], parts[1:]):
            total = jnp.where(own, part, total)
        return total

    results = []
    for d in range(2):
        x, y = [], []
        for h in range(heads):
            both = dot(solved[d, h], jnp.concatenate([starts[d], seen[d, h]], axis=1))
            x.append(both[:, :lanes])
            y.append(both[:, lanes:])
        x, y = gathered(x), gathered(y)
        if d == 0:
            weigh = whole if spikes is None else whole * jnp.exp(b_end - b_after)
        else:
            weigh = jnp.ones_like(whole) if spikes is None else jnp.exp(b_before)
        last_keys, last_removals = keys[d] * weigh, removals[d] * weigh
        offset = dot(
            jnp.concatenate([v.astype(F32), -y], axis=0),
            jnp.concatenate([last_keys, last_removals], axis=0),
            ((0,), (0,)),
        )
        if q is None:
            results.append((None, offset, None, None))
            continue
        decay = whole if spikes is None else jnp.exp(end + b_end)
        factor = jnp.where(row == col, decay, 0.0) - dot(x, last_removals, ((0,), (0,)))
        if d == 0:
            query = scaled(asks[0], b_after)
        else:
            query = scaled(asks[1] * whole, None if spikes is None else b_end - b_before)
        wx, base = [], []
        for h in range(heads):
            n = chains.index((d, h))
            mask = pair(h, d == 1, False)
            reads = scores[n][count:] * jnp.concatenate([mask, mask], axis=1)
            both = dot(reads[:, :count], jnp.concatenate([x, y], axis=1))
            wx.append(both[:, :lanes])
            base.append(dot(reads[:, count:], v) - both[:, lanes:])
        results.append((factor, offset, query - gathered(wx), gathered(base)))
    return results


def same_head(shape):
    return (iota(shape, 0) // HEAD) == (iota(shape, 1) // HEAD)


def block_kernel(
    mine, theirs, near_, far_, context_, wq, wk, wv, fading_, step_, rates_, gains_, spikes_,
    sent, asked, base, vectors, fading, step, lines,
    near, far, context, held, spikes, u, moved_q, moved_k, moved_v, moved_low, sems,
):
    place = here()
    lanes = wq.shape[1]
    pairs = [(near_, near), (far_, far), (context_, context)]
    pairs += [(ref, held.at[n]) for n, ref in enumerate((wq, wk, wv))]
    pairs += [(fading_, fading), (step_, step), (rates_, lines.at[0:1]), (gains_, lines.at[1:2]), (spikes_, spikes)]
    copies = [pltpu.make_async_copy(ref, to, sems.at[n]) for n, (ref, to) in enumerate(pairs)]
    for copy in copies:
        copy.start()
    for copy in copies[:3]:
        copy.wait()
    modulated(place, near, far, context, mine, theirs, u, vectors, held.at[3])
    for copy in copies[3:]:
        copy.wait()
    count, extra = asked.shape[1], context.shape[0]
    first, second = (dot(u[...], jnp.concatenate([held[n], held[n + 1]], axis=1)) for n in (0, 2))
    q, k, v, low = first[:, :lanes], first[:, lanes:], second[:, :lanes], second[:, lanes:]
    low = jnp.where(iota(low.shape, 1) < HEAD, low, 0.0)
    own = [
        placed_rows(part[:count], place[2], to).astype(BF16)
        for part, to in ((low, moved_low), (k, moved_k), (v, moved_v), (q, moved_q))
    ]
    ahead, behind = block_terms(
        own[1], own[2], own[0][:, :HEAD], fading[...], step[...], lines[0:1], spikes[...], own[3]
    )
    same = same_head(ahead[0].shape)
    size = same.shape[0]
    packed = [
        jnp.where(same, factor, pltpu.roll(offset, HEAD, 0)).astype(BF16)
        for factor, offset in (ahead[:2], behind[:2])
    ]
    tail = [part[count : count + extra].astype(BF16) for part in (k, v, low)]
    for j in range(sent.shape[0]):
        sent[j, :size] = jnp.where(place[0] < j, packed[0], packed[1])
        for n, part in enumerate(tail):
            sent[j, size + n * extra : size + (n + 1) * extra] = part
    asked[0], asked[1] = ahead[2].astype(BF16), behind[2].astype(BF16)
    base[...] = ahead[3] + behind[3]


def opened(packed, same):
    packed = packed.astype(F32)
    return jnp.where(same, packed, 0.0), jnp.where(same, pltpu.roll(packed, HEAD, 0), 0.0)


def read_kernel(maps, asked, base, fading, step, lines, emit_, keep, give, emit, sem):
    copy = pltpu.make_async_copy(emit_, emit, sem)
    copy.start()
    rates, gains = lines[0:1], lines[1:2]
    peers, _, size = maps.shape
    extra = keep.shape[1]
    same = same_head((size, size))
    me, core, _ = here()
    parts = [
        jnp.concatenate([maps[j, size + n * extra : size + (n + 1) * extra].astype(F32) for j in range(peers)], axis=0)
        for n in range(3)
    ]
    parts = [part.astype(BF16) for part in parts]
    eye = (iota((size, size), 0) == iota((size, size), 1)).astype(F32)
    composed = [jnp.concatenate([eye, jnp.zeros_like(eye)], axis=0) for _ in range(2)]

    def composing():
        for n in range(peers - 1):
            for d, j, reached in ((0, n, n < me), (1, peers - 1 - n, peers - 1 - n > me)):
                factor, offset = opened(maps[j, :size], same)
                new = dot(composed[d], factor)
                new = jnp.concatenate([new[:size], new[size:] + offset], axis=0)
                composed[d] = jnp.where(reached, new, composed[d])
            yield

    steps = composing()
    context = block_terms(
        parts[0], parts[1], parts[2][:, :HEAD], fading[...], step[...], rates, between=steps
    )
    for _ in steps:
        pass
    out = base[...]
    for d in range(2):
        start = jnp.where(same, context[d][1], 0.0)
        state = dot(start, composed[d][:size]) + composed[d][size:]
        out = out + dot(asked[d], state, ((1,), (1,)))
    first = iota(out.shape, 1) < HEAD

    def mean(value):
        left = jnp.sum(jnp.where(first, value, 0.0), -1, keepdims=True)
        right = jnp.sum(jnp.where(first, 0.0, value), -1, keepdims=True)
        return jnp.where(first, left, right) * (1.0 / HEAD)

    out = out - mean(out)
    normed = out * lax.rsqrt(mean(out * out) + EPS_HEAD) * gains
    chips, rows, _ = keep.shape
    split = normed.reshape(chips, 2, rows, size)
    even, odd = split[:, 0].reshape(chips * rows, size), split[:, 1].reshape(chips * rows, size)
    mine = jnp.where(core == 0, even, odd)
    other = jnp.where(core == 0, odd, even)
    left = jnp.concatenate([mine, other], axis=0).astype(BF16)
    copy.wait()
    lane = emit.shape[2]
    for s in range(emit.shape[0]):
        part = dot(left, emit[s]).reshape(2, chips, rows, lane).astype(BF16)
        keep[:, :, s * lane : (s + 1) * lane] = part[0]
        give[:, :, s * lane : (s + 1) * lane] = part[1]


def last_kernel(parts, hidden, vectors, out):
    lane = vectors.shape[2]
    for t in range(vectors.shape[0]):
        cols = slice(t * lane, (t + 1) * lane)
        total = parts[0, :, cols].astype(F32)
        for n in range(1, parts.shape[0]):
            total = total + parts[n, :, cols].astype(F32)
        out[:, cols] = (hidden[:, cols].astype(F32) + vectors[t, 4:5, :] * total).astype(BF16)


def exchange(blocks, axis, groups=None):
    return lax.all_to_all(blocks, axis, 0, 0, tiled=True, axis_index_groups=groups)


def swapped(value, axis, bit):
    return lax.ppermute(value, axis, [(i, i ^ bit) for i in range(lax.axis_size(axis))])


def shards(
    hidden_items,
    sample_cond,
    prompt_items,
    prompt_cond,
    adjust_shifting,
    adjust_stretch,
    skip_valve,
    receiver_matrix,
    address_matrix,
    payload_matrix,
    joint_lower_projector,
    fading_raise_matrix,
    step_raise_matrix,
    feature_fading,
    spike_logfade,
    group_standard_factor,
    emit_matrix,
):
    n_sp, n_tp = lax.axis_size("sp"), lax.axis_size("tp")
    rows, width = hidden_items.shape
    extra = prompt_items.shape[0]
    count = rows * n_tp
    lanes = receiver_matrix.shape[1]
    span, chunk = adjust_shifting.shape
    chips = n_tp // 2
    same_core = [[2 * i + c for i in range(chips)] for c in range(2)]

    parts = call(
        partials_kernel,
        ((n_sp, 4, 8, lanes), BF16),
        sample_cond.reshape(-1, lanes),
        prompt_cond.reshape(-1, lanes),
        joint_lower_projector.T,
        adjust_shifting,
        adjust_stretch,
        skip_valve,
        fetched=6,
        room=ALL,
        flops=8 * span * chunk * 6,
        scratch=[
            pltpu.VMEM((2, width // lanes, lanes), BF16),
            pltpu.VMEM(joint_lower_projector.shape[::-1], BF16),
            pltpu.VMEM((3, span, chunk), BF16),
            pltpu.SemaphoreType.DMA((6,)),
        ],
    )
    emit = lax.all_gather(emit_matrix, "sp", axis=0)
    parts = exchange(parts, "sp")

    def shifted(value, chips_on):
        return lax.ppermute(value, "tp", [(i, (i + 2 * chips_on) % n_tp) for i in range(n_tp)])

    below = shifted(hidden_items, 2)
    above = shifted(hidden_items, -2)
    across = shifted(above, -2)
    odd_below = shifted(jnp.stack([hidden_items, below]), 1)
    odd_above = shifted(jnp.stack([hidden_items, above]), -1)
    near = jnp.concatenate([jnp.stack([hidden_items, below, above, across]), odd_below, odd_above], axis=0)
    far = swapped(near, "tp", 1)

    mine = call(sum_kernel, ((chips, n_sp + 3, 8, lanes), BF16), parts)
    mine = exchange(mine, "tp", same_core)
    theirs = swapped(mine, "tp", 1)

    padded = count + -(-extra // 16) * 16
    sent, asked, base, vectors, *small = call(
        block_kernel,
        [
            ((n_sp, lanes + 3 * extra, lanes), BF16),
            ((2, count, lanes), BF16),
            ((count, lanes), F32),
            ((n_tp, 8, chunk), F32),
            (fading_raise_matrix.shape, BF16),
            (step_raise_matrix.shape, BF16),
            ((2, lanes), F32),
        ],
        mine,
        theirs,
        near.reshape(count // 2, width),
        far.reshape(count // 2, width),
        prompt_items,
        receiver_matrix,
        address_matrix,
        payload_matrix,
        fading_raise_matrix,
        step_raise_matrix,
        feature_fading.reshape(1, lanes),
        group_standard_factor.reshape(1, lanes),
        spike_logfade.T,
        fetched=11,
        room=MOST,
        flops=2 * padded * width * lanes * 4,
        scratch=[
            *[pltpu.VMEM((count // 2, width), BF16)] * 2,
            pltpu.VMEM((extra, width), BF16),
            pltpu.VMEM((4, width, lanes), BF16),
            pltpu.VMEM(spike_logfade.shape[::-1], F32),
            pltpu.VMEM((padded, width), BF16),
            *[pltpu.VMEM((n_tp, rows, lanes), F32)] * 4,
            pltpu.SemaphoreType.DMA((11,)),
        ],
    )
    maps = exchange(sent, "sp")
    keep, give = call(
        read_kernel,
        [((chips, rows, width), BF16)] * 2,
        maps,
        asked,
        base,
        *small,
        emit,
        fetched=1,
        room=READ,
        flops=2 * count * lanes * width,
        scratch=[
            pltpu.VMEM((n_sp, *emit_matrix.shape), BF16),
            pltpu.SemaphoreType.DMA,
        ],
    )
    given = swapped(give, "tp", 1)
    both = (keep.astype(F32) + given.astype(F32)).astype(BF16)
    final = exchange(both, "tp", same_core)
    return call(last_kernel, ((rows, width), BF16), final, hidden_items, vectors)


def solution(mesh):
    placed = (
        P(("grp", "sp", "tp"), None),
        P("grp"),
        P(("grp", "sp"), None),
        P(),
        P("sp", "tp"),
        P("sp", "tp"),
        P("sp", "tp"),
        P(None, "tp"),
        P(None, "tp"),
        P(None, "tp"),
        P("sp", None),
        P(None, "tp"),
        P(None, "tp"),
        P("tp"),
        P(("grp", "sp"), "tp"),
        P("tp"),
        P("tp", "sp"),
    )

    return jax.shard_map(shards, mesh=mesh, in_specs=placed, out_specs=P(("grp", "sp", "tp"), None), check_vma=False)
```
